32 devices in a mesh: sp: 8 (over z, x), tp: 4 (over y, core).
Axes of the slice: x: 2, y: 2, z: 4, core: 2. Of those that a mesh axis runs over, the one named last changes fastest.
Arguments:
- tokens: bfloat16 [4096, 2048], P('sp', 'tp'), may hold values from -72 to 72
- w_query: bfloat16 [2048, 1024], P('sp', 'tp'), may hold values from -0.125 to 0.125
- w_key: bfloat16 [2048, 256], P('sp', 'tp'), may hold values from -0.125 to 0.125
- w_value: bfloat16 [2048, 256], P('sp', 'tp'), may hold values from -0.125 to 0.125
- w_pool_in: bfloat16 [2048, 1024], P('sp', 'tp'), may hold values from -0.125 to 0.125
- sink: float32 [16], P('tp'), may hold values from 3 to 7
- w_pool: bfloat16 [4, 256, 256], P('tp'), may hold values from -0.375 to 0.375
- pool_scale: float32 [1024], P('tp'), may hold values from 0.1 to 1.9
- w_out_attn: bfloat16 [1024, 2048], P('tp', 'sp'), may hold values from -0.5 to 0.5
- w_out_pool: bfloat16 [1024, 2048], P('tp', 'sp'), may hold values from -0.125 to 0.125
- out_gain: float32 [2048], P('tp'), may hold values from 0.1 to 1.9
Outputs:
- mixed: bfloat16 [4096, 2048], P('sp', 'tp')
The draws below stay inside these ranges and needn't reach their ends.
All inputs are finite; a program needn't handle non-finite values.
Results may differ from the reference program's by a relative error of at most 0.012.
The reference program's roundings to bfloat16 on the way count: a program that leaves them out, or rounds other values in their place, can miss the bound.
Values may be sent and summed in bfloat16 or wider, within the bound.
A program may use at most 64 MiB of HBM per device.

```python
import jax
import jax.numpy as jnp
from jax import lax

D = 2048
HEADS = 16
KV_HEADS = 4
HEAD_DIM = 64
POOL_GROUPS = 4
GROUP_DIM = 256
WINDOW = 128
SEQ = 4096
ATTN_WIDTH = 1024
KV_WIDTH = 256
POOL_WIDTH = 1024
N_TP = 4


def draw_tokens(key, part):
    base = jnp.clip(jax.random.normal(key, (SEQ, D), jnp.float32), -6.0, 6.0)
    return base.astype(jnp.bfloat16)


def levels(stream_key, dims, pieces, smallest, top_value):
    level = 1.0
    for position, shards_of in pieces:
        heights = jax.random.uniform(jax.random.fold_in(jax.random.fold_in(stream_key, 6), position), (shards_of,), jnp.float32, smallest / len(pieces), top_value / len(pieces))
        level = level * jnp.repeat(jnp.exp(heights), dims[position] // shards_of).reshape((-1,) + (1,) * (len(dims) - 1 - position))
    return level


def centred(rng, shape, deviation, bound, shards=(), kind=jnp.bfloat16):
    entries = jax.random.normal(rng, shape, jnp.float32) * deviation
    if len(shards) > 0:
        entries = levels(rng, shape, shards, -0.22, 0.18) * entries
    return jnp.clip(entries, min=-bound, max=bound).astype(kind)


def setup_inputs(seed: int = 0) -> dict:
    splits = jax.random.split(jax.random.key(seed), 12)
    return {
        "tokens": draw_tokens(jax.random.fold_in(splits[11], 71), 0),
        "w_query": centred(splits[1], (D, ATTN_WIDTH), D ** -0.5, 0.125, ((0, 8), (1, 4))),
        "w_key": centred(splits[2], (D, KV_WIDTH), D ** -0.5, 0.125, ((0, 8), (1, 4))),
        "w_value": centred(splits[3], (D, KV_WIDTH), D ** -0.5, 0.125, ((0, 8), (1, 4))),
        "w_pool_in": centred(splits[4], (D, POOL_WIDTH), D ** -0.5, 0.125, ((0, 8), (1, 4))),
        "sink": jnp.clip(3.0 + 4.0 * jax.random.uniform(splits[5], (HEADS,), jnp.float32) ** levels(splits[5], (HEADS,), ((0, 4),), -0.2, 0.2), 3.0, 7.0),
        "w_pool": centred(splits[6], (POOL_GROUPS, GROUP_DIM, GROUP_DIM), GROUP_DIM ** -0.5, 0.375, ((0, 4),)),
        "pool_scale": jnp.clip(1.0 + 0.18 * jax.random.normal(splits[7], (POOL_WIDTH,), jnp.float32), 0.1, 1.9),
        "w_out_attn": centred(splits[8], (ATTN_WIDTH, D), (ATTN_WIDTH // 8) ** -0.5, 0.5, ((0, 4), (1, 8))),
        "w_out_pool": centred(splits[9], (POOL_WIDTH, D), (ATTN_WIDTH + POOL_WIDTH) ** -0.5, 0.125, ((0, 4), (1, 8))),
        "out_gain": jnp.clip(1.0 + 0.18 * jax.random.normal(splits[10], (D,), jnp.float32), 0.1, 1.9),
    }


epsilon = 1e-05
masked_score = -1e+30

def attend_head(query_one, key_one, value_one, sink_one):
    seq_len = query_one.shape[0]
    group = query_one.shape[1]
    block_count = seq_len // WINDOW
    query_blocks = query_one.reshape(block_count, WINDOW, group, HEAD_DIM).astype(jnp.float32)

    def banded(source):
        padded = jnp.pad(source, ((WINDOW, WINDOW), (0, 0))).reshape(block_count + 2, WINDOW, HEAD_DIM)
        return jnp.concatenate([padded[:-2], padded[1:-1], padded[2:]], axis=1).astype(jnp.float32)
    key_band = banded(key_one)
    value_band = banded(value_one)
    scores = jnp.einsum('nqgd,nsd->ngqs', query_blocks, key_band) * HEAD_DIM ** (-0.5)
    starts = jnp.arange(block_count, dtype=jnp.int32) * WINDOW
    query_pos = starts[:, None] + jnp.arange(WINDOW, dtype=jnp.int32)[None, :]
    key_pos = starts[:, None] + jnp.arange(3 * WINDOW, dtype=jnp.int32)[None, :] - WINDOW
    distance = key_pos[:, None, :] - query_pos[:, :, None]
    inside = (key_pos >= 0) & (key_pos < seq_len)
    keep = (jnp.abs(distance) <= WINDOW) & inside[:, None, :]
    scores = jnp.where(keep[:, None], scores, masked_score)
    sink_logit = sink_one.astype(jnp.float32)[None, :, None, None]
    top = jnp.maximum(lax.optimization_barrier(jnp.max(scores, axis=-1, keepdims=True)), sink_logit)
    raised = jnp.exp(scores - top)
    total = lax.optimization_barrier(jnp.sum(raised, axis=-1, keepdims=True)) + jnp.exp(sink_logit - top)
    probs = (raised / total).astype(jnp.bfloat16)
    attended = jnp.einsum('ngqs,nsd->nqgd', probs.astype(jnp.float32), value_band)
    return attended.astype(jnp.bfloat16).reshape(seq_len, group * HEAD_DIM)

def reference(tokens, w_query, w_key, w_value, w_pool_in, sink, w_pool, pool_scale, w_out_attn, w_out_pool, out_gain):
    seq_len = tokens.shape[0]
    group = HEADS // KV_HEADS
    query = jnp.dot(tokens, w_query, preferred_element_type=jnp.float32).astype(jnp.bfloat16)
    keys = jnp.dot(tokens, w_key, preferred_element_type=jnp.float32).astype(jnp.bfloat16)
    values = jnp.dot(tokens, w_value, preferred_element_type=jnp.float32).astype(jnp.bfloat16)
    chan = jnp.dot(tokens, w_pool_in, preferred_element_type=jnp.float32).astype(jnp.bfloat16)
    query_heads = query.reshape(seq_len, KV_HEADS, group, HEAD_DIM).transpose(1, 0, 2, 3)
    key_heads = keys.reshape(seq_len, KV_HEADS, HEAD_DIM).transpose(1, 0, 2)
    value_heads = values.reshape(seq_len, KV_HEADS, HEAD_DIM).transpose(1, 0, 2)
    sink_heads = sink.reshape(KV_HEADS, group)
    attended = lax.map(lambda parts: attend_head(*parts), (query_heads, key_heads, value_heads, sink_heads))
    attended = attended.transpose(1, 0, 2).reshape(seq_len, HEADS * HEAD_DIM)
    chan_float = chan.astype(jnp.float32)
    running = jnp.concatenate([jnp.zeros((1, POOL_WIDTH), jnp.float32), jnp.cumsum(chan_float, axis=0)], axis=0)
    positions = jnp.arange(seq_len, dtype=jnp.int32)
    outputs = []
    for level in range(POOL_GROUPS):
        half = 2 ** level
        lower = jnp.clip(positions - half, 0, seq_len)
        upper = jnp.clip(positions + half, 0, seq_len)
        columns = slice(level * GROUP_DIM, (level + 1) * GROUP_DIM)
        band = running[:, columns]
        count = (upper - lower).astype(jnp.float32)
        spread = ((band[upper] - band[lower]) / count[:, None] - chan_float[:, columns]).astype(jnp.bfloat16)
        outputs.append(jnp.dot(spread, w_pool[level], preferred_element_type=jnp.float32))
    pooled = (jnp.concatenate(outputs, axis=1) * pool_scale).astype(jnp.bfloat16)
    attn_share = ATTN_WIDTH // N_TP
    pool_share = POOL_WIDTH // N_TP
    mix = jnp.zeros((seq_len, D), jnp.float32)
    for device in range(N_TP):
        attn_cols = slice(device * attn_share, (device + 1) * attn_share)
        pool_cols = slice(device * pool_share, (device + 1) * pool_share)
        partial_sum = jnp.dot(attended[:, attn_cols], w_out_attn[attn_cols], preferred_element_type=jnp.float32)
        partial_sum = partial_sum + jnp.dot(pooled[:, pool_cols], w_out_pool[pool_cols], preferred_element_type=jnp.float32)
        mix = mix + partial_sum.astype(jnp.bfloat16).astype(jnp.float32)
    row_mean = lax.optimization_barrier(jnp.sum(mix, axis=1)) / D
    variance = lax.optimization_barrier(jnp.sum(mix * mix, axis=1)) / D - row_mean * row_mean
    normed = (mix - row_mean[:, None]) * lax.rsqrt(variance + epsilon)[:, None] * out_gain
    return normed.astype(jnp.bfloat16)
```

```python
import functools

import jax
import jax.numpy as jnp
from jax import lax
from jax.experimental import pallas as pl
from jax.experimental.pallas import tpu as pltpu
from jax.sharding import PartitionSpec as P

HEAD_DIM = 64
POOL_GROUPS = 4
WINDOW = 128


epsilon = 1e-05
masked_score = -1e30


def padded(cells, sides, width):
    for axis, dim in sides:
        count = lax.axis_size(axis)
        ends = count - 1
        head = lax.slice_in_dim(cells, 0, width, axis=dim)
        tail = lax.slice_in_dim(cells, cells.shape[dim] - width, cells.shape[dim], axis=dim)
        cells = jnp.concatenate(
            [
                lax.ppermute(tail, axis, [(i, (i + 1) % count) for i in range(ends)]),
                cells,
                lax.ppermute(head, axis, [((i + 1) % count, i) for i in range(ends)]),
            ],
            axis=dim,
        )
    return cells


def make_projector(gathered, pieces):
    piece_query, piece_key, piece_value, piece_chan = pieces
    joined = jnp.concatenate([piece_key, piece_value], axis=1)
    return (
        jnp.dot(gathered, piece_query, preferred_element_type=jnp.float32),
        jnp.dot(gathered, joined, preferred_element_type=jnp.float32),
        jnp.dot(gathered, piece_chan, preferred_element_type=jnp.float32),
    )


def attend_local(query, keys_ext, sinks, offset, seq_len, key_cols):
    tok_rows, query_cols = query.shape
    kv_local = key_cols // HEAD_DIM
    group = query_cols // key_cols
    block_count = tok_rows // WINDOW
    stacked = keys_ext.reshape(block_count + 2, WINDOW, 2 * key_cols)
    banded = jnp.concatenate([stacked[:-2], stacked[1:-1], stacked[2:]], axis=1)
    key_band = banded[:, :, :key_cols].reshape(block_count, 3 * WINDOW, kv_local, HEAD_DIM)
    value_band = banded[:, :, key_cols:].reshape(block_count, 3 * WINDOW, kv_local, HEAD_DIM)
    query_blocks = query.reshape(block_count, WINDOW, kv_local, group, HEAD_DIM)
    scores = jnp.einsum(
        "nqkgd,nskd->nkgqs", query_blocks, key_band, preferred_element_type=jnp.float32
    ) * HEAD_DIM ** (-0.5)
    starts = offset + jnp.arange(block_count, dtype=jnp.int32) * WINDOW
    query_pos = starts[:, None] + jnp.arange(WINDOW, dtype=jnp.int32)[None, :]
    key_pos = starts[:, None] + jnp.arange(3 * WINDOW, dtype=jnp.int32)[None, :] - WINDOW
    distance = key_pos[:, None, :] - query_pos[:, :, None]
    inside = (key_pos >= 0) & (key_pos < seq_len)
    keep = (jnp.abs(distance) <= WINDOW) & inside[:, None, :]
    scores = jnp.where(keep[:, None, None], scores, masked_score)
    sink_logit = sinks.reshape(kv_local, group)[None, :, :, None, None]
    top = jnp.maximum(jnp.max(scores, axis=-1, keepdims=True), sink_logit)
    raised = jnp.exp(scores - top)
    total = jnp.sum(raised, axis=-1, keepdims=True) + jnp.exp(sink_logit - top)
    probs = (raised / total).astype(jnp.bfloat16)
    attended = jnp.einsum(
        "nkgqs,nskd->nqkgd", probs, value_band, preferred_element_type=jnp.float32
    )
    return attended.astype(jnp.bfloat16).reshape(tok_rows, query_cols)


def local(
    tokens,
    w_query,
    w_key,
    w_value,
    w_pool_in,
    sink,
    w_pool,
    pool_scale,
    w_out_attn,
    w_out_pool,
    out_gain,
):
    tok_rows = tokens.shape[0]
    seq_len = tok_rows * lax.axis_size("sp")
    offset = lax.axis_index("sp") * tok_rows
    out_both = jnp.concatenate([w_out_attn, w_out_pool], axis=0)
    gathered = lax.all_gather(tokens, "tp", axis=1, tiled=True)
    key_cols = w_key.shape[1]
    chan_cols = w_pool_in.shape[1]
    query_sum, joined_sum, chan_sum = make_projector(
        gathered,
        (
            lax.all_gather(w_query, "sp", axis=0, tiled=True),
            lax.all_gather(w_key, "sp", axis=0, tiled=True),
            lax.all_gather(w_value, "sp", axis=0, tiled=True),
            lax.all_gather(w_pool_in, "sp", axis=0, tiled=True),
        ),
    )
    query = query_sum.astype(jnp.bfloat16)
    key_value = joined_sum.astype(jnp.bfloat16)
    chan = chan_sum.astype(jnp.bfloat16)
    keys_ext = padded(key_value, (("sp", 0),), WINDOW)
    attended = attend_local(query, keys_ext, sink, offset, seq_len, key_cols)
    rim_rows = 2 ** (POOL_GROUPS - 1)
    chan_ext = padded(chan, (("sp", 0),), rim_rows)
    running = jnp.concatenate(
        [jnp.zeros((1, chan_cols), jnp.float32), jnp.cumsum(chan_ext.astype(jnp.float32), axis=0)],
        axis=0,
    )
    chan_float = chan.astype(jnp.float32)
    positions = offset + jnp.arange(tok_rows, dtype=jnp.int32)
    group_count = w_pool.shape[0]
    level = lax.axis_index("tp") * group_count + 0
    half = jnp.left_shift(jnp.int32(1), level)
    upper = lax.dynamic_slice_in_dim(running, rim_rows + half, tok_rows, 0)
    lower = lax.dynamic_slice_in_dim(running, rim_rows - half, tok_rows, 0)
    count = (
        jnp.clip(positions + half, 0, seq_len) - jnp.clip(positions - half, 0, seq_len)
    ).astype(jnp.float32)
    spread = ((upper - lower) / count[:, None] - chan_float).astype(jnp.bfloat16)
    outputs = jnp.dot(spread, w_pool[0], preferred_element_type=jnp.float32)
    pooled = (outputs * pool_scale).astype(jnp.bfloat16)
    hidden = jnp.concatenate([attended, pooled], axis=1)
    terms = jnp.dot(
        hidden,
        lax.all_gather(out_both, "sp", axis=1, tiled=True),
        preferred_element_type=jnp.float32,
    )
    share_width = out_gain.shape[0]
    model_width = share_width * lax.axis_size("tp")
    share = lax.psum_scatter(
        terms.astype(jnp.bfloat16), "tp", scatter_dimension=1, tiled=True
    ).astype(jnp.float32)
    row_total, row_square = lax.psum((jnp.sum(share, axis=1), jnp.sum(share * share, axis=1)), "tp")
    row_mean = row_total / model_width
    variance = row_square / model_width - row_mean * row_mean
    normed = (share - row_mean[:, None]) * lax.rsqrt(variance + epsilon)[:, None] * out_gain
    return normed.astype(jnp.bfloat16)


MESH = pl.DeviceIdType.MESH
RIM = 16
QUARTERS = 4


def mixer_kernel(
    n,
    tp,
    tok_ref,
    wq_ref,
    wk_ref,
    wv_ref,
    wc_ref,
    sink_ref,
    wp_ref,
    ps_ref,
    woa_ref,
    wop_ref,
    gain_ref,
    out_ref,
    win,
    wout,
    tok,
    acc,
    query,
    kv,
    chan,
    hidden,
    part,
    mated,
    landed,
    own,
    stats,
    pair_in,
    sinks,
    wpool,
    scales,
    gains,
    win_send,
    win_recv,
    wout_send,
    wout_recv,
    tok_send,
    tok_recv,
    rim_send,
    rim_recv,
    part_send,
    mate_recv,
    part_recv,
    load,
    stat_send,
    stat_recv,
):
    f32, bf16 = jnp.float32, jnp.bfloat16
    me, t = lax.axis_index("sp"), lax.axis_index("tp")
    rows = tok_ref.shape[0]
    seq_len = rows * n
    half_n = n // 2
    column = me % 2
    pos = (me // 2) * (1 - column) + column * (n - 1 - me // 2)

    def at(p):
        p = lax.rem(p + n, n)
        back = p // half_n
        return (1 - back) * (2 * p) + back * (2 * (n - 1 - p) + 1)

    ring = (at(pos + 1), at(pos - 1))
    after, before = lax.rem(me + 1, n), lax.rem(me + n - 1, n)
    mate = t + 1 - 2 * lax.rem(t, 2)
    across = lax.rem(t + 2, tp)
    per = n // tp

    def rdma(src, dst, send, recv, sp, tpi):
        return pltpu.make_async_remote_copy(
            src_ref=src,
            dst_ref=dst,
            send_sem=send,
            recv_sem=recv,
            device_id={"sp": sp, "tp": tpi},
            device_id_type=MESH,
        )

    qc, kc = wq_ref.shape[1], wk_ref.shape[0]
    cc = wc_ref.shape[1]
    depth = wq_ref.shape[0]
    quarter = depth // QUARTERS
    wide = woa_ref.shape[1]
    half = wide // 2
    barrier = pltpu.get_barrier_semaphore()
    peers = [(s, t) for s in ring] + [(s, t) for s in (before, after)]
    peers += [(me, lax.rem(t + i, tp)) for i in range(1, tp)]
    for s, p in peers:
        pl.semaphore_signal(barrier, inc=1, device_id={"sp": s, "tp": p}, device_id_type=MESH)

    loads = []

    def fetch(src, dst):
        copy = pltpu.make_async_copy(src, dst, load.at[len(loads)])
        copy.start()
        loads.append(copy)
        return copy

    pairs = [fetch(wk_ref, pair_in.at[pl.ds(0, kc)]), fetch(wv_ref, pair_in.at[pl.ds(kc, kc)])]
    first = []
    for h in range(QUARTERS):
        rows_in = pl.ds(h * quarter, quarter)
        first.append(fetch(wq_ref.at[rows_in], win.at[me, h, :, pl.ds(0, qc)]))
        first.append(fetch(wc_ref.at[rows_in], win.at[me, h, :, pl.ds(qc + 2 * kc, cc)]))
    own_tok = [fetch(tok_ref.at[:, pl.ds(b * depth, depth)], tok.at[t * per + b]) for b in range(per)]
    later = []
    for h in range(2):
        later.append(fetch(woa_ref.at[:, pl.ds(h * half, half)], wout.at[me, h, 0]))
        later.append(fetch(wop_ref.at[:, pl.ds(h * half, half)], wout.at[me, h, 1]))
    later.append(fetch(sink_ref, sinks))
    later.append(fetch(wp_ref, wpool))
    later.append(fetch(ps_ref, scales))
    later.append(fetch(gain_ref, gains))
    for copy in pairs:
        copy.wait()
    pair = jnp.transpose(pair_in[...].astype(f32)).astype(bf16)
    for h in range(QUARTERS):
        win[me, h, :, qc : qc + 2 * kc] = pair[h * quarter : (h + 1) * quarter]
    for copy in first:
        copy.wait()
    pl.semaphore_wait(barrier, len(peers))

    def ring_copy(buf, send, recv, way, k, hop):
        sign = -1 if way == 0 else 1
        q = k % QUARTERS if way == 0 else QUARTERS - 1 - k % QUARTERS
        o = at(pos + sign * (k // QUARTERS + hop))
        slot = buf.at[o, q] if buf is win else buf.at[o, q // 2, q % 2]
        return rdma(slot, slot, send.at[way, k], recv.at[way, k], ring[way], t)

    def w_in(way, k, hop):
        return ring_copy(win, win_send, win_recv, way, k, hop)

    def w_out(way, k, hop):
        return ring_copy(wout, wout_send, wout_recv, way, k, hop)

    def tok_copy(owner, b, i, dst):
        slot = tok.at[owner * per + b]
        return rdma(slot, slot, tok_send.at[i], tok_recv.at[i], me, dst)

    count = QUARTERS * (n - 1) // 2
    last = count - 1
    for k in range(QUARTERS):
        for way in range(2):
            w_in(way, k, 0).start()
    for copy in own_tok:
        copy.wait()
    for b in range(per):
        tok_copy(t, b, b, across).start()
    for b in range(per):
        tok_copy(t, b, per + b, mate).start()
    for copy in later:
        copy.wait()

    origin = [at(pos)]
    for d in range(1, half_n):
        origin += [at(pos - d), at(pos + d)]
    origin.append(at(pos + half_n))

    def project(i, first=False):
        o = origin[i]
        w = win[o].reshape(depth, qc + 2 * kc + cc)
        term = jnp.dot(tok[o], w, preferred_element_type=f32)
        if first:
            acc[...] = term
        else:
            acc[...] += term

    def relay(copy, k):
        for way in range(2):
            copy(way, k, 1).wait_recv()
            if k + QUARTERS <= last:
                copy(way, k + QUARTERS, 0).start()

    def start_out(k):
        for way in range(2):
            w_out(way, k, 0).start()

    done_blocks = 0
    for k in range(count):
        relay(w_in, k)
        if k in (last - 3, last - 2):
            start_out(k - (last - 3))
        if k in (3, 6):
            b = 0 if k == 3 else 1
            tok_copy(across, b, b, across).wait_recv()
            tok_copy(across, b, 2 * per + b, mate).start()
        if k == 8:
            for b in range(per):
                tok_copy(mate, b, per + b, mate).wait_recv()
                tok_copy(lax.rem(mate + 2, tp), b, 2 * per + b, mate).wait_recv()
        if k >= 8:
            ready = n if k == last else 1 + 2 * ((k + 1) // QUARTERS)
            upto = ready if k == last else min(ready, done_blocks + 2)
            while done_blocks < upto:
                project(done_blocks, done_blocks == 0)
                done_blocks += 1

    kv[WINDOW : WINDOW + rows, :] = acc[:, qc : qc + 2 * kc].astype(bf16)
    chan[RIM : RIM + rows, :] = acc[:, qc + 2 * kc :].astype(bf16)

    def rim(buf, width, down, i):
        if down:
            return rdma(buf.at[pl.ds(rows, width)], buf.at[pl.ds(0, width)], rim_send.at[i], rim_recv.at[i], after, t)
        return rdma(
            buf.at[pl.ds(width, width)], buf.at[pl.ds(rows + width, width)], rim_send.at[i], rim_recv.at[i], before, t
        )

    rims = [rim(kv, WINDOW, True, 0), rim(kv, WINDOW, False, 1), rim(chan, RIM, True, 2), rim(chan, RIM, False, 3)]
    for c in rims:
        c.start()
    start_out(2)
    start_out(3)
    query[...] = acc[:, 0:qc].astype(bf16)

    group = qc // kc

    def attend(b):
        band = kv[b * WINDOW : (b + 3) * WINDOW, :]
        q = query[b * WINDOW : (b + 1) * WINDOW, :]
        stacked = jnp.concatenate([q[:, g * HEAD_DIM : (g + 1) * HEAD_DIM] for g in range(group)], axis=0)
        scores = lax.dot_general(
            stacked, band[:, :HEAD_DIM], (((1,), (1,)), ((), ())), preferred_element_type=f32
        ) * HEAD_DIM ** (-0.5)
        scores = scores.reshape(group, WINDOW, 3 * WINDOW)
        r = lax.broadcasted_iota(jnp.int32, (WINDOW, 3 * WINDOW), 0)
        c = lax.broadcasted_iota(jnp.int32, (WINDOW, 3 * WINDOW), 1)
        keep = (c >= r) & (c <= r + 2 * WINDOW)
        key_pos = c + (me * rows + b * WINDOW - WINDOW)
        keep = keep & (key_pos >= 0) & (key_pos < seq_len)
        outs = []
        for g in range(group):
            s = jnp.where(keep, scores[g], masked_score)
            logit = sinks[0:1, g : g + 1]
            top = jnp.maximum(jnp.max(s, axis=1, keepdims=True), logit)
            raised = jnp.exp(s - top)
            total = jnp.sum(raised, axis=1, keepdims=True) + jnp.exp(logit - top)
            outs.append((raised * (1.0 / total)).astype(bf16))
        got = jnp.dot(jnp.concatenate(outs, axis=0), band, preferred_element_type=f32)
        got = got[:, HEAD_DIM : 2 * HEAD_DIM].astype(bf16)
        hidden[b * WINDOW : (b + 1) * WINDOW, 0:qc] = jnp.concatenate(
            [got[g * WINDOW : (g + 1) * WINDOW] for g in range(group)], axis=1
        )

    def pool():
        length = rows + 2 * RIM
        e = chan[...].astype(f32)
        p = lax.broadcasted_iota(jnp.int32, (length, 1), 0) + (me * rows - RIM)
        e = jnp.where((p >= 0) & (p < seq_len), e, 0.0)
        sums = e + pltpu.roll(e, 1, 0)
        pick = sums
        for level in range(1, POOL_GROUPS):
            step = 2 ** (level - 1)
            sums = pltpu.roll(sums, step, 0) + pltpu.roll(sums, length - step, 0)
            pick = jnp.where(t == level, sums, pick)
        half_width = 1
        for level in range(1, POOL_GROUPS):
            half_width = jnp.where(t == level, 2**level, half_width)
        number = (jnp.clip(p + half_width, 0, seq_len) - jnp.clip(p - half_width, 0, seq_len)).astype(f32)
        spread = (pick[RIM : RIM + rows] / number[RIM : RIM + rows] - e[RIM : RIM + rows]).astype(bf16)
        got = jnp.dot(spread, wpool[0], preferred_element_type=f32)
        hidden[:, qc:] = (got * scales[...]).astype(bf16)

    def to_mate(o, h):
        return rdma(part.at[o, h], mated.at[o, h], part_send.at[o, h], mate_recv.at[o, h], me, mate)

    def to_owner(o, h):
        s = lax.rem(o, per)
        return rdma(part.at[o, h], landed.at[s, h], part_send.at[o, h], part_recv.at[s, h], me, across)

    pieces = [(0, 0), (0, 1)]
    for k in range(1, count, 2):
        d, h = k // QUARTERS, (k % QUARTERS) // 2
        pieces += [(min(2 * d + 1, n - 1), h), (min(2 * d + 2, n - 1), 1 - h)]

    def emit(i):
        o, h = origin[pieces[i][0]], pieces[i][1]
        got = jnp.dot(hidden[...], wout[o, h].reshape(qc + cc, half), preferred_element_type=f32)
        part[o, h] = got.astype(bf16)

        @pl.when(lax.rem(o // per, 2) != lax.rem(t, 2))
        def _():
            to_mate(o, h).start()

    def combine(i):
        o, h = origin[pieces[i][0]], pieces[i][1]

        @pl.when(o // per == t)
        def _():
            to_mate(o, h).wait_recv()
            own[lax.rem(o, per), h] = part[o, h].astype(f32) + mated[o, h].astype(f32)

        @pl.when(o // per == across)
        def _():
            to_mate(o, h).wait_recv()
            part[o, h] = (part[o, h].astype(f32) + mated[o, h].astype(f32)).astype(bf16)
            to_owner(o, h).start()

    blocks = rows // WINDOW
    inner = list(range(1, blocks - 1))
    emitted = combined = 0
    for k in range(count):
        relay(w_out, k)
        if k < 2:
            for b in inner[k :: 2]:
                attend(b)
        elif k == 2:
            for c in rims:
                c.wait()
            attend(0)
        elif k == 3:
            attend(blocks - 1)
        elif k == 4:
            pool()
        else:
            here = 2 + 2 * ((k + 1) // 2)
            goal = here if k == last else min(here, emitted + 3)
            behind = emitted
            while emitted < goal:
                emit(emitted)
                emitted += 1
            while combined < (emitted if k == last else behind):
                combine(combined)
                combined += 1

    share = []
    for s in range(per):
        for h in range(2):
            to_owner(t * per + s, h).wait_recv()
            share.append(own[s, h] + landed[s, h].astype(f32))
    mix = jnp.concatenate(share, axis=1)
    acc[:, 0 : mix.shape[1]] = mix
    one = jnp.sum(mix, axis=1, keepdims=True)
    two = jnp.sum(mix * mix, axis=1, keepdims=True)
    lane = lax.broadcasted_iota(jnp.int32, (rows, 128), 1)
    both = jnp.where(lane == 0, one, jnp.where(lane == 1, two, 0.0))
    stats[t] = jnp.transpose(both)[0:8]

    def stat_copy(j):
        return rdma(stats.at[t], stats.at[t], stat_send.at[j], stat_recv.at[t], me, lax.rem(t + j, tp))

    for j in range(1, tp):
        stat_copy(j).start()
    for o in range(n):

        @pl.when(o // per != t)
        def _():
            for h in range(2):
                to_mate(o, h).wait_send()

    for k in range(count):
        for way in range(2):
            w_in(way, k, 0).wait_send()
            w_out(way, k, 0).wait_send()
    for b in range(per):
        tok_copy(t, b, b, across).wait_send()
        tok_copy(t, b, per + b, mate).wait_send()
        tok_copy(across, b, 2 * per + b, mate).wait_send()
    for j in range(1, tp):
        src = lax.rem(t + j, tp)
        rdma(stats.at[src], stats.at[src], stat_send.at[j], stat_recv.at[src], me, src).wait_recv()
    totals = stats[0]
    for i in range(1, tp):
        totals = totals + stats[i]
    tall = jnp.concatenate([totals, jnp.zeros((120, rows), f32)], axis=0)
    back = jnp.transpose(tall)
    width = gain_ref.shape[1] * tp
    row_mean = back[:, 0:1] / width
    variance = back[:, 1:2] / width - row_mean * row_mean
    scale = lax.rsqrt(variance + epsilon)
    out_ref[...] = ((acc[:, 0 : gain_ref.shape[1]] - row_mean) * scale * gains[...]).astype(bf16)
    for j in range(1, tp):
        stat_copy(j).wait_send()


def fused(n, tp, tokens, w_query, w_key, w_value, w_pool_in, sink, w_pool, pool_scale, w_out_attn, w_out_pool, out_gain):
    rows, share = tokens.shape
    depth, qc = w_query.shape
    kc, cc = w_key.shape[1], w_pool_in.shape[1]
    wide = w_out_attn.shape[1]
    half = wide // 2
    per = n // tp
    count = QUARTERS * (n - 1) // 2
    bf16, f32 = jnp.bfloat16, jnp.float32
    dma = pltpu.SemaphoreType.DMA
    return pl.pallas_call(
        functools.partial(mixer_kernel, n, tp),
        out_shape=jax.ShapeDtypeStruct((rows, share), bf16),
        in_specs=[pl.BlockSpec(memory_space=pltpu.HBM)] * 11,
        out_specs=pl.BlockSpec(memory_space=pltpu.VMEM),
        scratch_shapes=[
            pltpu.VMEM((n, QUARTERS, depth // QUARTERS, qc + 2 * kc + cc), bf16),
            pltpu.VMEM((n, 2, 2, qc, half), bf16),
            pltpu.VMEM((n, rows, depth), bf16),
            pltpu.VMEM((rows, qc + 2 * kc + cc), f32),
            pltpu.VMEM((rows, qc), bf16),
            pltpu.VMEM((rows + 2 * WINDOW, 2 * kc), bf16),
            pltpu.VMEM((rows + 2 * RIM, cc), bf16),
            pltpu.VMEM((rows, qc + cc), bf16),
            pltpu.VMEM((n, 2, rows, half), bf16),
            pltpu.VMEM((n, 2, rows, half), bf16),
            pltpu.VMEM((per, 2, rows, half), bf16),
            pltpu.VMEM((per, 2, rows, half), f32),
            pltpu.VMEM((tp, 8, rows), f32),
            pltpu.VMEM((2 * kc, depth), bf16),
            pltpu.VMEM((1, sink.shape[0]), f32),
            pltpu.VMEM(w_pool.shape, bf16),
            pltpu.VMEM((1, cc), f32),
            pltpu.VMEM((1, share), f32),
            dma((2, count)),
            dma((2, count)),
            dma((2, count)),
            dma((2, count)),
            dma((3 * per,)),
            dma((3 * per,)),
            dma((4,)),
            dma((4,)),
            dma((n, 2)),
            dma((n, 2)),
            dma((per, 2)),
            dma((2 * QUARTERS + per + 10,)),
            dma((tp,)),
            dma((tp,)),
        ],
        compiler_params=pltpu.CompilerParams(
            collective_id=0, has_side_effects=True, vmem_limit_bytes=32 * 1024 * 1024
        ),
        name="mixer",
    )(
        pltpu.with_memory_space_constraint(tokens, pltpu.HBM),
        pltpu.with_memory_space_constraint(w_query, pltpu.HBM),
        pltpu.with_memory_space_constraint(w_key.T, pltpu.HBM),
        pltpu.with_memory_space_constraint(w_value.T, pltpu.HBM),
        pltpu.with_memory_space_constraint(w_pool_in, pltpu.HBM),
        pltpu.with_memory_space_constraint(sink.reshape(1, -1), pltpu.HBM),
        pltpu.with_memory_space_constraint(w_pool, pltpu.HBM),
        pltpu.with_memory_space_constraint(pool_scale.reshape(1, -1), pltpu.HBM),
        pltpu.with_memory_space_constraint(w_out_attn, pltpu.HBM),
        pltpu.with_memory_space_constraint(w_out_pool, pltpu.HBM),
        pltpu.with_memory_space_constraint(out_gain.reshape(1, -1), pltpu.HBM),
    )


def fits(n, tp, tokens, w_query, w_key, w_pool, w_out_attn):
    return (
        tp == 4
        and n == 2 * tp
        and w_query.shape[0] % 64 == 0
        and w_query.shape[1] % 128 == 0
        and w_key.shape[1] == HEAD_DIM
        and w_pool.shape[0] == 1
        and w_out_attn.shape[1] % 256 == 0
        and w_out_attn.shape[0] == w_query.shape[1]
        and tokens.shape[0] >= 2 * WINDOW
    )


def mixed_rows(*args):
    n, tp = lax.axis_size("sp"), lax.axis_size("tp")
    if fits(n, tp, args[0], args[1], args[2], args[6], args[8]):
        return fused(n, tp, *args)
    return local(*args)


def solution(mesh):
    return jax.shard_map(
        mixed_rows,
        mesh=mesh,
        in_specs=(
            P("sp", "tp"),
            P("sp", "tp"),
            P("sp", "tp"),
            P("sp", "tp"),
            P("sp", "tp"),
            P("tp"),
            P("tp", None, None),
            P("tp"),
            P("tp", "sp"),
            P("tp", "sp"),
            P("tp"),
        ),
        out_specs=P("sp", "tp"),
        check_vma=False,
    )
```

```python
import functools

import jax
import jax.numpy as jnp
from jax import lax
from jax.experimental import pallas as pl
from jax.experimental.pallas import tpu as pltpu
from jax.sharding import PartitionSpec as P

HEAD_DIM = 64
POOL_GROUPS = 4
WINDOW = 128


epsilon = 1e-05
masked_score = -1e30


def padded(cells, sides, width):
    for axis, dim in sides:
        count = lax.axis_size(axis)
        ends = count - 1
        head = lax.slice_in_dim(cells, 0, width, axis=dim)
        tail = lax.slice_in_dim(cells, cells.shape[dim] - width, cells.shape[dim], axis=dim)
        cells = jnp.concatenate(
            [
                lax.ppermute(tail, axis, [(i, (i + 1) % count) for i in range(ends)]),
                cells,
                lax.ppermute(head, axis, [((i + 1) % count, i) for i in range(ends)]),
            ],
            axis=dim,
        )
    return cells


def make_projector(gathered, pieces):
    piece_query, piece_key, piece_value, piece_chan = pieces
    joined = jnp.concatenate([piece_key, piece_value], axis=1)
    return (
        jnp.dot(gathered, piece_query, preferred_element_type=jnp.float32),
        jnp.dot(gathered, joined, preferred_element_type=jnp.float32),
        jnp.dot(gathered, piece_chan, preferred_element_type=jnp.float32),
    )


def attend_local(query, keys_ext, sinks, offset, seq_len, key_cols):
    tok_rows, query_cols = query.shape
    kv_local = key_cols // HEAD_DIM
    group = query_cols // key_cols
    block_count = tok_rows // WINDOW
    stacked = keys_ext.reshape(block_count + 2, WINDOW, 2 * key_cols)
    banded = jnp.concatenate([stacked[:-2], stacked[1:-1], stacked[2:]], axis=1)
    key_band = banded[:, :, :key_cols].reshape(block_count, 3 * WINDOW, kv_local, HEAD_DIM)
    value_band = banded[:, :, key_cols:].reshape(block_count, 3 * WINDOW, kv_local, HEAD_DIM)
    query_blocks = query.reshape(block_count, WINDOW, kv_local, group, HEAD_DIM)
    scores = jnp.einsum(
        "nqkgd,nskd->nkgqs", query_blocks, key_band, preferred_element_type=jnp.float32
    ) * HEAD_DIM ** (-0.5)
    starts = offset + jnp.arange(block_count, dtype=jnp.int32) * WINDOW
    query_pos = starts[:, None] + jnp.arange(WINDOW, dtype=jnp.int32)[None, :]
    key_pos = starts[:, None] + jnp.arange(3 * WINDOW, dtype=jnp.int32)[None, :] - WINDOW
    distance = key_pos[:, None, :] - query_pos[:, :, None]
    inside = (key_pos >= 0) & (key_pos < seq_len)
    keep = (jnp.abs(distance) <= WINDOW) & inside[:, None, :]
    scores = jnp.where(keep[:, None, None], scores, masked_score)
    sink_logit = sinks.reshape(kv_local, group)[None, :, :, None, None]
    top = jnp.maximum(jnp.max(scores, axis=-1, keepdims=True), sink_logit)
    raised = jnp.exp(scores - top)
    total = jnp.sum(raised, axis=-1, keepdims=True) + jnp.exp(sink_logit - top)
    probs = (raised / total).astype(jnp.bfloat16)
    attended = jnp.einsum(
        "nkgqs,nskd->nqkgd", probs, value_band, preferred_element_type=jnp.float32
    )
    return attended.astype(jnp.bfloat16).reshape(tok_rows, query_cols)


def local(
    tokens,
    w_query,
    w_key,
    w_value,
    w_pool_in,
    sink,
    w_pool,
    pool_scale,
    w_out_attn,
    w_out_pool,
    out_gain,
):
    tok_rows = tokens.shape[0]
    seq_len = tok_rows * lax.axis_size("sp")
    offset = lax.axis_index("sp") * tok_rows
    out_both = jnp.concatenate([w_out_attn, w_out_pool], axis=0)
    gathered = lax.all_gather(tokens, "tp", axis=1, tiled=True)
    key_cols = w_key.shape[1]
    chan_cols = w_pool_in.shape[1]
    query_sum, joined_sum, chan_sum = make_projector(
        gathered,
        (
            lax.all_gather(w_query, "sp", axis=0, tiled=True),
            lax.all_gather(w_key, "sp", axis=0, tiled=True),
            lax.all_gather(w_value, "sp", axis=0, tiled=True),
            lax.all_gather(w_pool_in, "sp", axis=0, tiled=True),
        ),
    )
    query = query_sum.astype(jnp.bfloat16)
    key_value = joined_sum.astype(jnp.bfloat16)
    chan = chan_sum.astype(jnp.bfloat16)
    keys_ext = padded(key_value, (("sp", 0),), WINDOW)
    attended = attend_local(query, keys_ext, sink, offset, seq_len, key_cols)
    rim_rows = 2 ** (POOL_GROUPS - 1)
    chan_ext = padded(chan, (("sp", 0),), rim_rows)
    running = jnp.concatenate(
        [jnp.zeros((1, chan_cols), jnp.float32), jnp.cumsum(chan_ext.astype(jnp.float32), axis=0)],
        axis=0,
    )
    chan_float = chan.astype(jnp.float32)
    positions = offset + jnp.arange(tok_rows, dtype=jnp.int32)
    group_count = w_pool.shape[0]
    level = lax.axis_index("tp") * group_count + 0
    half = jnp.left_shift(jnp.int32(1), level)
    upper = lax.dynamic_slice_in_dim(running, rim_rows + half, tok_rows, 0)
    lower = lax.dynamic_slice_in_dim(running, rim_rows - half, tok_rows, 0)
    count = (
        jnp.clip(positions + half, 0, seq_len) - jnp.clip(positions - half, 0, seq_len)
    ).astype(jnp.float32)
    spread = ((upper - lower) / count[:, None] - chan_float).astype(jnp.bfloat16)
    outputs = jnp.dot(spread, w_pool[0], preferred_element_type=jnp.float32)
    pooled = (outputs * pool_scale).astype(jnp.bfloat16)
    hidden = jnp.concatenate([attended, pooled], axis=1)
    terms = jnp.dot(
        hidden,
        lax.all_gather(out_both, "sp", axis=1, tiled=True),
        preferred_element_type=jnp.float32,
    )
    share_width = out_gain.shape[0]
    model_width = share_width * lax.axis_size("tp")
    share = lax.psum_scatter(
        terms.astype(jnp.bfloat16), "tp", scatter_dimension=1, tiled=True
    ).astype(jnp.float32)
    row_total, row_square = lax.psum((jnp.sum(share, axis=1), jnp.sum(share * share, axis=1)), "tp")
    row_mean = row_total / model_width
    variance = row_square / model_width - row_mean * row_mean
    normed = (share - row_mean[:, None]) * lax.rsqrt(variance + epsilon)[:, None] * out_gain
    return normed.astype(jnp.bfloat16)


MESH = pl.DeviceIdType.MESH
RIM = 16
QUARTERS = 4
SENDS = 8


def mixer_kernel(
    n,
    tp,
    tok_ref,
    wq_ref,
    wk_ref,
    wv_ref,
    wc_ref,
    sink_ref,
    wp_ref,
    ps_ref,
    woa_ref,
    wop_ref,
    gain_ref,
    out_ref,
    win,
    wout,
    tok,
    acc,
    query,
    kv,
    chan,
    hidden,
    part,
    mated,
    landed,
    own,
    stats,
    pair_in,
    sinks,
    wpool,
    scales,
    gains,
    ring_send,
    ring_recv,
    tok_send,
    tok_recv,
    rim_send,
    rim_recv,
    part_send,
    mate_recv,
    part_recv,
    load,
    stat_send,
    stat_recv,
):
    f32, bf16 = jnp.float32, jnp.bfloat16
    me, t = lax.axis_index("sp"), lax.axis_index("tp")
    rows = tok_ref.shape[0]
    seq_len = rows * n
    half_n = n // 2
    column = me % 2
    pos = (me // 2) * (1 - column) + column * (n - 1 - me // 2)

    def at(p):
        p = lax.rem(p + n, n)
        back = p // half_n
        return (1 - back) * (2 * p) + back * (2 * (n - 1 - p) + 1)

    ring = (at(pos + 1), at(pos - 1))
    after, before = lax.rem(me + 1, n), lax.rem(me + n - 1, n)
    mate = t + 1 - 2 * lax.rem(t, 2)
    across = lax.rem(t + 2, tp)
    per = n // tp

    def rdma(src, dst, send, recv, sp, tpi):
        return pltpu.make_async_remote_copy(
            src_ref=src,
            dst_ref=dst,
            send_sem=send,
            recv_sem=recv,
            device_id={"sp": sp, "tp": tpi},
            device_id_type=MESH,
        )

    qc, kc = wq_ref.shape[2], wk_ref.shape[0]
    cc = wc_ref.shape[2]
    depth = QUARTERS * wq_ref.shape[1]
    quarter = depth // QUARTERS
    wide = woa_ref.shape[1]
    half = wide // 2
    barrier = pltpu.get_barrier_semaphore()
    peers = [(s, t) for s in ring] + [(s, t) for s in (before, after)]
    peers += [(me, lax.rem(t + i, tp)) for i in range(1, tp)]
    for s, p in peers:
        pl.semaphore_signal(barrier, inc=1, device_id={"sp": s, "tp": p}, device_id_type=MESH)

    loads = []

    def fetch(src, dst):
        copy = pltpu.make_async_copy(src, dst, load.at[len(loads)])
        copy.start()
        loads.append(copy)
        return copy

    pairs = [fetch(wk_ref, pair_in.at[pl.ds(0, kc)]), fetch(wv_ref, pair_in.at[pl.ds(kc, kc)])]
    first = [
        fetch(wq_ref, win.at[me, :, :, pl.ds(0, qc)]),
        fetch(wc_ref, win.at[me, :, :, pl.ds(qc + 2 * kc, cc)]),
    ]
    own_tok = [fetch(tok_ref.at[:, pl.ds(b * depth, depth)], tok.at[t * per + b]) for b in range(per)]
    later = []
    for h in range(2):
        later.append(fetch(woa_ref.at[:, pl.ds(h * half, half)], wout.at[me, h, 0]))
        later.append(fetch(wop_ref.at[:, pl.ds(h * half, half)], wout.at[me, h, 1]))
    later.append(fetch(sink_ref, sinks))
    later.append(fetch(wp_ref, wpool))
    later.append(fetch(ps_ref, scales))
    later.append(fetch(gain_ref, gains))
    for copy in pairs:
        copy.wait()
    pair = jnp.transpose(pair_in[...].astype(f32)).astype(bf16)
    for h in range(QUARTERS):
        win[me, h, :, qc : qc + 2 * kc] = pair[h * quarter : (h + 1) * quarter]
    for copy in first:
        copy.wait()
    pl.semaphore_wait(barrier, len(peers))

    count = QUARTERS * (n - 1) // 2
    last = count - 1

    def ring_copy(buf, way, k, hop, turn):
        sign = -1 if way == 0 else 1
        q = k % QUARTERS if way == 0 else QUARTERS - 1 - k % QUARTERS
        o = at(pos + sign * (k // QUARTERS + hop))
        slot = buf.at[o, q] if buf is win else buf.at[o, q // 2, q % 2]
        return rdma(slot, slot, ring_send.at[way, turn % SENDS], ring_recv.at[way, k], ring[way], t)

    def w_in(way, k, hop):
        return ring_copy(win, way, k, hop, k)

    def w_out(way, k, hop):
        return ring_copy(wout, way, k, hop, count + k)

    def launched(way, turn):
        return w_in(way, turn, 0) if turn < count else w_out(way, turn - count, 0)

    def launch(way, turn):
        if turn >= SENDS:
            launched(way, turn - SENDS).wait_send()
        launched(way, turn).start()

    def tok_copy(owner, b, i, dst):
        slot = tok.at[owner * per + b]
        return rdma(slot, slot, tok_send.at[i], tok_recv.at[i], me, dst)

    for k in range(QUARTERS):
        for way in range(2):
            launch(way, k)
    for copy in own_tok:
        copy.wait()
    for b in range(per):
        tok_copy(t, b, b, across).start()
    for b in range(per):
        tok_copy(t, b, per + b, mate).start()
    for copy in later:
        copy.wait()

    origin = [at(pos)]
    for d in range(1, half_n):
        origin += [at(pos - d), at(pos + d)]
    origin.append(at(pos + half_n))

    def project(i, first=False):
        o = origin[i]
        w = win[o].reshape(depth, qc + 2 * kc + cc)
        term = jnp.dot(tok[o], w, preferred_element_type=f32)
        if first:
            acc[...] = term
        else:
            acc[...] += term

    def relay(copy, k):
        for way in range(2):
            copy(way, k, 1).wait_recv()
            if k + QUARTERS <= last:
                launch(way, k + QUARTERS + (0 if copy is w_in else count))

    def start_out(k):
        for way in range(2):
            launch(way, count + k)

    done_blocks = 0
    for k in range(count):
        relay(w_in, k)
        if last - 3 <= k < last:
            start_out(k - (last - 3))
        if k in (3, 6):
            b = 0 if k == 3 else 1
            tok_copy(across, b, b, across).wait_recv()
            tok_copy(across, b, 2 * per + b, mate).start()
        if k == 8:
            for b in range(per):
                tok_copy(mate, b, per + b, mate).wait_recv()
                tok_copy(lax.rem(mate + 2, tp), b, 2 * per + b, mate).wait_recv()
        if k >= 8:
            ready = n if k == last else 1 + 2 * ((k + 1) // QUARTERS)
            upto = ready if k == last else min(ready, done_blocks + 2)
            while done_blocks < upto:
                project(done_blocks, done_blocks == 0)
                done_blocks += 1

    kv[WINDOW : WINDOW + rows, :] = acc[:, qc : qc + 2 * kc].astype(bf16)
    chan[RIM : RIM + rows, :] = acc[:, qc + 2 * kc :].astype(bf16)

    def rim(buf, width, down, i):
        if down:
            return rdma(buf.at[pl.ds(rows, width)], buf.at[pl.ds(0, width)], rim_send.at[i], rim_recv.at[i], after, t)
        return rdma(
            buf.at[pl.ds(width, width)], buf.at[pl.ds(rows + width, width)], rim_send.at[i], rim_recv.at[i], before, t
        )

    rims = [rim(kv, WINDOW, True, 0), rim(kv, WINDOW, False, 1), rim(chan, RIM, True, 2), rim(chan, RIM, False, 3)]
    for c in rims:
        c.start()
    start_out(3)
    query[...] = acc[:, 0:qc].astype(bf16)

    group = qc // kc

    def attend(b):
        band = kv[b * WINDOW : (b + 3) * WINDOW, :]
        q = query[b * WINDOW : (b + 1) * WINDOW, :]
        stacked = jnp.concatenate([q[:, g * HEAD_DIM : (g + 1) * HEAD_DIM] for g in range(group)], axis=0)
        scores = lax.dot_general(
            stacked, band[:, :HEAD_DIM], (((1,), (1,)), ((), ())), preferred_element_type=f32
        ) * HEAD_DIM ** (-0.5)
        scores = scores.reshape(group, WINDOW, 3 * WINDOW)
        r = lax.broadcasted_iota(jnp.int32, (WINDOW, 3 * WINDOW), 0)
        c = lax.broadcasted_iota(jnp.int32, (WINDOW, 3 * WINDOW), 1)
        keep = (c >= r) & (c <= r + 2 * WINDOW)
        key_pos = c + (me * rows + b * WINDOW - WINDOW)
        keep = keep & (key_pos >= 0) & (key_pos < seq_len)
        outs = []
        for g in range(group):
            s = jnp.where(keep, scores[g], masked_score)
            logit = sinks[0:1, g : g + 1]
            top = jnp.maximum(jnp.max(s, axis=1, keepdims=True), logit)
            raised = jnp.exp(s - top)
            total = jnp.sum(raised, axis=1, keepdims=True) + jnp.exp(logit - top)
            outs.append((raised * (1.0 / total)).astype(bf16))
        got = jnp.dot(jnp.concatenate(outs, axis=0), band, preferred_element_type=f32)
        got = got[:, HEAD_DIM : 2 * HEAD_DIM].astype(bf16)
        hidden[b * WINDOW : (b + 1) * WINDOW, 0:qc] = jnp.concatenate(
            [got[g * WINDOW : (g + 1) * WINDOW] for g in range(group)], axis=1
        )

    def pool():
        length = rows + 2 * RIM
        e = chan[...].astype(f32)
        p = lax.broadcasted_iota(jnp.int32, (length, 1), 0) + (me * rows - RIM)
        e = jnp.where((p >= 0) & (p < seq_len), e, 0.0)
        sums = e + pltpu.roll(e, 1, 0)
        pick = sums
        for level in range(1, POOL_GROUPS):
            step = 2 ** (level - 1)
            sums = pltpu.roll(sums, step, 0) + pltpu.roll(sums, length - step, 0)
            pick = jnp.where(t == level, sums, pick)
        half_width = 1
        for level in range(1, POOL_GROUPS):
            half_width = jnp.where(t == level, 2**level, half_width)
        number = (jnp.clip(p + half_width, 0, seq_len) - jnp.clip(p - half_width, 0, seq_len)).astype(f32)
        spread = (pick[RIM : RIM + rows] / number[RIM : RIM + rows] - e[RIM : RIM + rows]).astype(bf16)
        got = jnp.dot(spread, wpool[0], preferred_element_type=f32)
        hidden[:, qc:] = (got * scales[...]).astype(bf16)

    def to_mate(o, h):
        return rdma(part.at[o, h], mated.at[o, h], part_send.at[o, h], mate_recv.at[o, h], me, mate)

    def to_owner(o, h):
        s = lax.rem(o, per)
        return rdma(part.at[o, h], landed.at[s, h], part_send.at[o, h], part_recv.at[s, h], me, across)

    pieces = [(0, 0), (0, 1)]
    for k in range(1, count, 2):
        d, h = k // QUARTERS, (k % QUARTERS) // 2
        pieces += [(min(2 * d + 1, n - 1), h), (min(2 * d + 2, n - 1), 1 - h)]

    def emit(ids):
        places = [(origin[pieces[i][0]], pieces[i][1]) for i in ids]
        side = jnp.concatenate([wout[o, h].reshape(qc + cc, half) for o, h in places], axis=1)
        got = jnp.dot(hidden[...], side, preferred_element_type=f32).astype(bf16)
        for j, (o, h) in enumerate(places):
            part[o, h] = got[:, j * half : (j + 1) * half]
        for o, h in places:

            @pl.when(lax.rem(o // per, 2) != lax.rem(t, 2))
            def _(o=o, h=h):
                to_mate(o, h).start()

    def combine(i):
        o, h = origin[pieces[i][0]], pieces[i][1]

        @pl.when(o // per == t)
        def _():
            to_mate(o, h).wait_recv()
            own[lax.rem(o, per), h] = part[o, h].astype(f32) + mated[o, h].astype(f32)

        @pl.when(o // per == across)
        def _():
            to_mate(o, h).wait_recv()
            part[o, h] = (part[o, h].astype(f32) + mated[o, h].astype(f32)).astype(bf16)
            to_owner(o, h).start()

    blocks = rows // WINDOW
    inner = list(range(1, blocks - 1))
    emits = {6: range(0, 8), 7: range(8, 10), 9: range(10, 12), 11: range(12, 14), 13: range(14, 16)}
    combines = {8: range(0, 8), 9: range(8, 10), 11: range(10, 12), 12: range(12, 14), 13: range(14, 16)}
    for k in range(count):
        relay(w_out, k)
        if k < 2:
            for b in inner[k :: 2]:
                attend(b)
        elif k == 3:
            for c in rims:
                c.wait()
            attend(0)
        elif k == 4:
            attend(blocks - 1)
        elif k == 5:
            pool()
        if k in emits:
            emit(emits[k])
        for i in combines.get(k, ()):
            combine(i)

    share = []
    for s in range(per):
        for h in range(2):
            to_owner(t * per + s, h).wait_recv()
            share.append(own[s, h] + landed[s, h].astype(f32))
    mix = jnp.concatenate(share, axis=1)
    acc[:, 0 : mix.shape[1]] = mix
    one = jnp.sum(mix, axis=1, keepdims=True)
    two = jnp.sum(mix * mix, axis=1, keepdims=True)
    lane = lax.broadcasted_iota(jnp.int32, (rows, 128), 1)
    both = jnp.where(lane == 0, one, jnp.where(lane == 1, two, 0.0))
    stats[t] = jnp.transpose(both)[0:8]

    def stat_copy(j):
        return rdma(stats.at[t], stats.at[t], stat_send.at[j], stat_recv.at[t], me, lax.rem(t + j, tp))

    for j in range(1, tp):
        stat_copy(j).start()
    for o in range(n):

        @pl.when(o // per != t)
        def _():
            for h in range(2):
                to_mate(o, h).wait_send()

    for turn in range(2 * count - SENDS, 2 * count):
        for way in range(2):
            launched(way, turn).wait_send()
    for b in range(per):
        tok_copy(t, b, b, across).wait_send()
        tok_copy(t, b, per + b, mate).wait_send()
        tok_copy(across, b, 2 * per + b, mate).wait_send()
    for j in range(1, tp):
        src = lax.rem(t + j, tp)
        rdma(stats.at[src], stats.at[src], stat_send.at[j], stat_recv.at[src], me, src).wait_recv()
    totals = stats[0]
    for i in range(1, tp):
        totals = totals + stats[i]
    tall = jnp.concatenate([totals, jnp.zeros((120, rows), f32)], axis=0)
    back = jnp.transpose(tall)
    width = gain_ref.shape[1] * tp
    row_mean = back[:, 0:1] / width
    variance = back[:, 1:2] / width - row_mean * row_mean
    scale = lax.rsqrt(variance + epsilon)
    out_ref[...] = ((acc[:, 0 : gain_ref.shape[1]] - row_mean) * scale * gains[...]).astype(bf16)
    for j in range(1, tp):
        stat_copy(j).wait_send()


def fused(n, tp, tokens, w_query, w_key, w_value, w_pool_in, sink, w_pool, pool_scale, w_out_attn, w_out_pool, out_gain):
    rows, share = tokens.shape
    depth, qc = w_query.shape
    kc, cc = w_key.shape[1], w_pool_in.shape[1]
    wide = w_out_attn.shape[1]
    half = wide // 2
    per = n // tp
    count = QUARTERS * (n - 1) // 2
    bf16, f32 = jnp.bfloat16, jnp.float32
    dma = pltpu.SemaphoreType.DMA
    return pl.pallas_call(
        functools.partial(mixer_kernel, n, tp),
        out_shape=jax.ShapeDtypeStruct((rows, share), bf16),
        in_specs=[pl.BlockSpec(memory_space=pltpu.HBM)] * 11,
        out_specs=pl.BlockSpec(memory_space=pltpu.VMEM),
        scratch_shapes=[
            pltpu.VMEM((n, QUARTERS, depth // QUARTERS, qc + 2 * kc + cc), bf16),
            pltpu.VMEM((n, 2, 2, qc, half), bf16),
            pltpu.VMEM((n, rows, depth), bf16),
            pltpu.VMEM((rows, qc + 2 * kc + cc), f32),
            pltpu.VMEM((rows, qc), bf16),
            pltpu.VMEM((rows + 2 * WINDOW, 2 * kc), bf16),
            pltpu.VMEM((rows + 2 * RIM, cc), bf16),
            pltpu.VMEM((rows, qc + cc), bf16),
            pltpu.VMEM((n, 2, rows, half), bf16),
            pltpu.VMEM((n, 2, rows, half), bf16),
            pltpu.VMEM((per, 2, rows, half), bf16),
            pltpu.VMEM((per, 2, rows, half), f32),
            pltpu.VMEM((tp, 8, rows), f32),
            pltpu.VMEM((2 * kc, depth), bf16),
            pltpu.VMEM((1, sink.shape[0]), f32),
            pltpu.VMEM(w_pool.shape, bf16),
            pltpu.VMEM((1, cc), f32),
            pltpu.VMEM((1, share), f32),
            dma((2, SENDS)),
            dma((2, count)),
            dma((3 * per,)),
            dma((3 * per,)),
            dma((4,)),
            dma((4,)),
            dma((n, 2)),
            dma((n, 2)),
            dma((per, 2)),
            dma((per + 12,)),
            dma((tp,)),
            dma((tp,)),
        ],
        compiler_params=pltpu.CompilerParams(
            collective_id=0, has_side_effects=True, vmem_limit_bytes=32 * 1024 * 1024
        ),
        name="mixer",
    )(
        pltpu.with_memory_space_constraint(tokens, pltpu.HBM),
        pltpu.with_memory_space_constraint(w_query.reshape(QUARTERS, -1, qc), pltpu.HBM),
        pltpu.with_memory_space_constraint(w_key.T, pltpu.HBM),
        pltpu.with_memory_space_constraint(w_value.T, pltpu.HBM),
        pltpu.with_memory_space_constraint(w_pool_in.reshape(QUARTERS, -1, cc), pltpu.HBM),
        pltpu.with_memory_space_constraint(sink.reshape(1, -1), pltpu.HBM),
        pltpu.with_memory_space_constraint(w_pool, pltpu.HBM),
        pltpu.with_memory_space_constraint(pool_scale.reshape(1, -1), pltpu.HBM),
        pltpu.with_memory_space_constraint(w_out_attn, pltpu.HBM),
        pltpu.with_memory_space_constraint(w_out_pool, pltpu.HBM),
        pltpu.with_memory_space_constraint(out_gain.reshape(1, -1), pltpu.HBM),
    )


def fits(n, tp, tokens, w_query, w_key, w_pool, w_out_attn):
    return (
        tp == 4
        and n == 2 * tp
        and w_query.shape[0] % 64 == 0
        and w_query.shape[1] % 128 == 0
        and w_key.shape[1] == HEAD_DIM
        and w_pool.shape[0] == 1
        and w_out_attn.shape[1] % 256 == 0
        and w_out_attn.shape[0] == w_query.shape[1]
        and tokens.shape[0] >= 2 * WINDOW
    )


def mixed_rows(*args):
    n, tp = lax.axis_size("sp"), lax.axis_size("tp")
    if fits(n, tp, args[0], args[1], args[2], args[6], args[8]):
        return fused(n, tp, *args)
    return local(*args)


def solution(mesh):
    return jax.shard_map(
        mixed_rows,
        mesh=mesh,
        in_specs=(
            P("sp", "tp"),
            P("sp", "tp"),
            P("sp", "tp"),
            P("sp", "tp"),
            P("sp", "tp"),
            P("tp"),
            P("tp", None, None),
            P("tp"),
            P("tp", "sp"),
            P("tp", "sp"),
            P("tp"),
        ),
        out_specs=P("sp", "tp"),
        check_vma=False,
    )
```

```python
import functools

import jax
import jax.numpy as jnp
from jax import lax
from jax.experimental import pallas as pl
from jax.experimental.pallas import tpu as pltpu
from jax.sharding import PartitionSpec as P

HEAD_DIM = 64
POOL_GROUPS = 4
WINDOW = 128


epsilon = 1e-05
masked_score = -1e30


def padded(cells, sides, width):
    for axis, dim in sides:
        count = lax.axis_size(axis)
        ends = count - 1
        head = lax.slice_in_dim(cells, 0, width, axis=dim)
        tail = lax.slice_in_dim(cells, cells.shape[dim] - width, cells.shape[dim], axis=dim)
        cells = jnp.concatenate(
            [
                lax.ppermute(tail, axis, [(i, (i + 1) % count) for i in range(ends)]),
                cells,
                lax.ppermute(head, axis, [((i + 1) % count, i) for i in range(ends)]),
            ],
            axis=dim,
        )
    return cells


def make_projector(gathered, pieces):
    piece_query, piece_key, piece_value, piece_chan = pieces
    joined = jnp.concatenate([piece_key, piece_value], axis=1)
    return (
        jnp.dot(gathered, piece_query, preferred_element_type=jnp.float32),
        jnp.dot(gathered, joined, preferred_element_type=jnp.float32),
        jnp.dot(gathered, piece_chan, preferred_element_type=jnp.float32),
    )


def attend_local(query, keys_ext, sinks, offset, seq_len, key_cols):
    tok_rows, query_cols = query.shape
    kv_local = key_cols // HEAD_DIM
    group = query_cols // key_cols
    block_count = tok_rows // WINDOW
    stacked = keys_ext.reshape(block_count + 2, WINDOW, 2 * key_cols)
    banded = jnp.concatenate([stacked[:-2], stacked[1:-1], stacked[2:]], axis=1)
    key_band = banded[:, :, :key_cols].reshape(block_count, 3 * WINDOW, kv_local, HEAD_DIM)
    value_band = banded[:, :, key_cols:].reshape(block_count, 3 * WINDOW, kv_local, HEAD_DIM)
    query_blocks = query.reshape(block_count, WINDOW, kv_local, group, HEAD_DIM)
    scores = jnp.einsum(
        "nqkgd,nskd->nkgqs", query_blocks, key_band, preferred_element_type=jnp.float32
    ) * HEAD_DIM ** (-0.5)
    starts = offset + jnp.arange(block_count, dtype=jnp.int32) * WINDOW
    query_pos = starts[:, None] + jnp.arange(WINDOW, dtype=jnp.int32)[None, :]
    key_pos = starts[:, None] + jnp.arange(3 * WINDOW, dtype=jnp.int32)[None, :] - WINDOW
    distance = key_pos[:, None, :] - query_pos[:, :, None]
    inside = (key_pos >= 0) & (key_pos < seq_len)
    keep = (jnp.abs(distance) <= WINDOW) & inside[:, None, :]
    scores = jnp.where(keep[:, None, None], scores, masked_score)
    sink_logit = sinks.reshape(kv_local, group)[None, :, :, None, None]
    top = jnp.maximum(jnp.max(scores, axis=-1, keepdims=True), sink_logit)
    raised = jnp.exp(scores - top)
    total = jnp.sum(raised, axis=-1, keepdims=True) + jnp.exp(sink_logit - top)
    probs = (raised / total).astype(jnp.bfloat16)
    attended = jnp.einsum(
        "nkgqs,nskd->nqkgd", probs, value_band, preferred_element_type=jnp.float32
    )
    return attended.astype(jnp.bfloat16).reshape(tok_rows, query_cols)


def local(
    tokens,
    w_query,
    w_key,
    w_value,
    w_pool_in,
    sink,
    w_pool,
    pool_scale,
    w_out_attn,
    w_out_pool,
    out_gain,
):
    tok_rows = tokens.shape[0]
    seq_len = tok_rows * lax.axis_size("sp")
    offset = lax.axis_index("sp") * tok_rows
    out_both = jnp.concatenate([w_out_attn, w_out_pool], axis=0)
    gathered = lax.all_gather(tokens, "tp", axis=1, tiled=True)
    key_cols = w_key.shape[1]
    chan_cols = w_pool_in.shape[1]
    query_sum, joined_sum, chan_sum = make_projector(
        gathered,
        (
            lax.all_gather(w_query, "sp", axis=0, tiled=True),
            lax.all_gather(w_key, "sp", axis=0, tiled=True),
            lax.all_gather(w_value, "sp", axis=0, tiled=True),
            lax.all_gather(w_pool_in, "sp", axis=0, tiled=True),
        ),
    )
    query = query_sum.astype(jnp.bfloat16)
    key_value = joined_sum.astype(jnp.bfloat16)
    chan = chan_sum.astype(jnp.bfloat16)
    keys_ext = padded(key_value, (("sp", 0),), WINDOW)
    attended = attend_local(query, keys_ext, sink, offset, seq_len, key_cols)
    rim_rows = 2 ** (POOL_GROUPS - 1)
    chan_ext = padded(chan, (("sp", 0),), rim_rows)
    running = jnp.concatenate(
        [jnp.zeros((1, chan_cols), jnp.float32), jnp.cumsum(chan_ext.astype(jnp.float32), axis=0)],
        axis=0,
    )
    chan_float = chan.astype(jnp.float32)
    positions = offset + jnp.arange(tok_rows, dtype=jnp.int32)
    group_count = w_pool.shape[0]
    level = lax.axis_index("tp") * group_count + 0
    half = jnp.left_shift(jnp.int32(1), level)
    upper = lax.dynamic_slice_in_dim(running, rim_rows + half, tok_rows, 0)
    lower = lax.dynamic_slice_in_dim(running, rim_rows - half, tok_rows, 0)
    count = (
        jnp.clip(positions + half, 0, seq_len) - jnp.clip(positions - half, 0, seq_len)
    ).astype(jnp.float32)
    spread = ((upper - lower) / count[:, None] - chan_float).astype(jnp.bfloat16)
    outputs = jnp.dot(spread, w_pool[0], preferred_element_type=jnp.float32)
    pooled = (outputs * pool_scale).astype(jnp.bfloat16)
    hidden = jnp.concatenate([attended, pooled], axis=1)
    terms = jnp.dot(
        hidden,
        lax.all_gather(out_both, "sp", axis=1, tiled=True),
        preferred_element_type=jnp.float32,
    )
    share_width = out_gain.shape[0]
    model_width = share_width * lax.axis_size("tp")
    share = lax.psum_scatter(
        terms.astype(jnp.bfloat16), "tp", scatter_dimension=1, tiled=True
    ).astype(jnp.float32)
    row_total, row_square = lax.psum((jnp.sum(share, axis=1), jnp.sum(share * share, axis=1)), "tp")
    row_mean = row_total / model_width
    variance = row_square / model_width - row_mean * row_mean
    normed = (share - row_mean[:, None]) * lax.rsqrt(variance + epsilon)[:, None] * out_gain
    return normed.astype(jnp.bfloat16)


MESH = pl.DeviceIdType.MESH
RIM = 16
QUARTERS = 4
SENDS = 8


def mixer_kernel(
    n,
    tp,
    tok_ref,
    wq_ref,
    wk_ref,
    wv_ref,
    wc_ref,
    sink_ref,
    wp_ref,
    ps_ref,
    woa_ref,
    wop_ref,
    gain_ref,
    out_ref,
    win,
    wout,
    tok,
    acc,
    query,
    kv,
    chan,
    hidden,
    part,
    mated,
    landed,
    own,
    stats,
    late,
    echo,
    sums,
    pair_in,
    sinks,
    wpool,
    scales,
    gains,
    ring_send,
    ring_recv,
    tok_send,
    tok_recv,
    rim_send,
    rim_recv,
    mate_send,
    mate_recv,
    part_send,
    part_recv,
    echo_send,
    echo_recv,
    load,
    stat_send,
    stat_recv,
    late_send,
    late_recv,
):
    f32, bf16 = jnp.float32, jnp.bfloat16
    me, t = lax.axis_index("sp"), lax.axis_index("tp")
    rows = tok_ref.shape[0]
    seq_len = rows * n
    half_n = n // 2
    column = me % 2
    pos = (me // 2) * (1 - column) + column * (n - 1 - me // 2)

    def at(p):
        p = lax.rem(p + n, n)
        back = p // half_n
        return (1 - back) * (2 * p) + back * (2 * (n - 1 - p) + 1)

    ring = (at(pos + 1), at(pos - 1))
    after, before = lax.rem(me + 1, n), lax.rem(me + n - 1, n)
    mate = t + 1 - 2 * lax.rem(t, 2)
    across = lax.rem(t + 2, tp)
    per = n // tp

    def rdma(src, dst, send, recv, sp, tpi):
        return pltpu.make_async_remote_copy(
            src_ref=src,
            dst_ref=dst,
            send_sem=send,
            recv_sem=recv,
            device_id={"sp": sp, "tp": tpi},
            device_id_type=MESH,
        )

    qc, kc = wq_ref.shape[2], wk_ref.shape[0]
    cc = wc_ref.shape[2]
    depth = QUARTERS * wq_ref.shape[1]
    quarter = depth // QUARTERS
    wide = woa_ref.shape[1]
    half = wide // 2
    barrier = pltpu.get_barrier_semaphore()
    peers = [(s, t) for s in ring] + [(s, t) for s in (before, after)]
    peers += [(me, lax.rem(t + i, tp)) for i in range(1, tp)]
    for s, p in peers:
        pl.semaphore_signal(barrier, inc=1, device_id={"sp": s, "tp": p}, device_id_type=MESH)

    loads = []

    def fetch(src, dst):
        copy = pltpu.make_async_copy(src, dst, load.at[len(loads)])
        copy.start()
        loads.append(copy)
        return copy

    pairs = [fetch(wk_ref, pair_in.at[pl.ds(0, kc)]), fetch(wv_ref, pair_in.at[pl.ds(kc, kc)])]
    first = [
        fetch(wq_ref, win.at[me, :, :, pl.ds(0, qc)]),
        fetch(wc_ref, win.at[me, :, :, pl.ds(qc + 2 * kc, cc)]),
    ]
    own_tok = [fetch(tok_ref.at[:, pl.ds(b * depth, depth)], tok.at[t * per + b]) for b in range(per)]
    later = []
    for h in range(2):
        later.append(fetch(woa_ref.at[:, pl.ds(h * half, half)], wout.at[me, h, 0]))
        later.append(fetch(wop_ref.at[:, pl.ds(h * half, half)], wout.at[me, h, 1]))
    later.append(fetch(sink_ref, sinks))
    later.append(fetch(wp_ref, wpool))
    later.append(fetch(ps_ref, scales))
    later.append(fetch(gain_ref, gains))
    for copy in pairs:
        copy.wait()
    pair = jnp.transpose(pair_in[...].astype(f32)).astype(bf16)
    for h in range(QUARTERS):
        win[me, h, :, qc : qc + 2 * kc] = pair[h * quarter : (h + 1) * quarter]
    for copy in first:
        copy.wait()
    pl.semaphore_wait(barrier, len(peers))

    count = QUARTERS * (n - 1) // 2
    last = count - 1

    def ring_copy(buf, way, k, hop, turn):
        sign = -1 if way == 0 else 1
        q = k % QUARTERS if way == 0 else QUARTERS - 1 - k % QUARTERS
        o = at(pos + sign * (k // QUARTERS + hop))
        slot = buf.at[o, q] if buf is win else buf.at[o, q // 2, q % 2]
        return rdma(slot, slot, ring_send.at[way, turn % SENDS], ring_recv.at[way, k], ring[way], t)

    def w_in(way, k, hop):
        return ring_copy(win, way, k, hop, k)

    def w_out(way, k, hop):
        return ring_copy(wout, way, k, hop, count + k)

    def launched(way, turn):
        return w_in(way, turn, 0) if turn < count else w_out(way, turn - count, 0)

    def launch(way, turn):
        if turn >= SENDS:
            launched(way, turn - SENDS).wait_send()
        launched(way, turn).start()

    def tok_copy(owner, b, i, dst):
        slot = tok.at[owner * per + b]
        return rdma(slot, slot, tok_send.at[i], tok_recv.at[i], me, dst)

    for k in range(QUARTERS):
        for way in range(2):
            launch(way, k)
    for copy in own_tok:
        copy.wait()
    for b in range(per):
        tok_copy(t, b, b, across).start()
    for b in range(per):
        tok_copy(t, b, per + b, mate).start()

    for copy in later:
        copy.wait()

    origin = [at(pos)]
    for d in range(1, half_n):
        origin += [at(pos - d), at(pos + d)]
    origin.append(at(pos + half_n))

    def project(i, first=False):
        o = origin[i]
        w = win[o].reshape(depth, qc + 2 * kc + cc)
        term = jnp.dot(tok[o], w, preferred_element_type=f32)
        if first:
            acc[...] = term
        else:
            acc[...] += term

    def relay(copy, k):
        for way in range(2):
            copy(way, k, 1).wait_recv()
            if k + QUARTERS <= last:
                launch(way, k + QUARTERS + (0 if copy is w_in else count))

    def start_out(k):
        for way in range(2):
            launch(way, count + k)

    done_blocks = 0
    for k in range(count):
        relay(w_in, k)
        if last - 3 <= k < last:
            start_out(k - (last - 3))
        if k in (3, 6):
            b = 0 if k == 3 else 1
            tok_copy(across, b, b, across).wait_recv()
            tok_copy(across, b, 2 * per + b, mate).start()
        if k == 8:
            for b in range(per):
                tok_copy(mate, b, per + b, mate).wait_recv()
                tok_copy(lax.rem(mate + 2, tp), b, 2 * per + b, mate).wait_recv()
        if k >= 8:
            ready = n if k == last else 1 + 2 * ((k + 1) // QUARTERS)
            upto = ready if k == last else min(ready, done_blocks + 2)
            while done_blocks < upto:
                project(done_blocks, done_blocks == 0)
                done_blocks += 1

    kv[WINDOW : WINDOW + rows, :] = acc[:, qc : qc + 2 * kc].astype(bf16)
    chan[RIM : RIM + rows, :] = acc[:, qc + 2 * kc :].astype(bf16)

    def rim(buf, width, down, i):
        if down:
            return rdma(buf.at[pl.ds(rows, width)], buf.at[pl.ds(0, width)], rim_send.at[i], rim_recv.at[i], after, t)
        return rdma(
            buf.at[pl.ds(width, width)], buf.at[pl.ds(rows + width, width)], rim_send.at[i], rim_recv.at[i], before, t
        )

    rims = [rim(kv, WINDOW, True, 0), rim(kv, WINDOW, False, 1), rim(chan, RIM, True, 2), rim(chan, RIM, False, 3)]
    for c in rims:
        c.start()
    start_out(3)
    query[...] = acc[:, 0:qc].astype(bf16)

    group = qc // kc

    def attend(b):
        band = kv[b * WINDOW : (b + 3) * WINDOW, :]
        q = query[b * WINDOW : (b + 1) * WINDOW, :]
        stacked = jnp.concatenate([q[:, g * HEAD_DIM : (g + 1) * HEAD_DIM] for g in range(group)], axis=0)
        scores = lax.dot_general(
            stacked, band[:, :HEAD_DIM], (((1,), (1,)), ((), ())), preferred_element_type=f32
        ) * HEAD_DIM ** (-0.5)
        scores = scores.reshape(group, WINDOW, 3 * WINDOW)
        r = lax.broadcasted_iota(jnp.int32, (WINDOW, 3 * WINDOW), 0)
        c = lax.broadcasted_iota(jnp.int32, (WINDOW, 3 * WINDOW), 1)
        keep = (c >= r) & (c <= r + 2 * WINDOW)
        key_pos = c + (me * rows + b * WINDOW - WINDOW)
        keep = keep & (key_pos >= 0) & (key_pos < seq_len)
        outs = []
        for g in range(group):
            s = jnp.where(keep, scores[g], masked_score)
            logit = sinks[0:1, g : g + 1]
            top = jnp.maximum(jnp.max(s, axis=1, keepdims=True), logit)
            raised = jnp.exp(s - top)
            total = jnp.sum(raised, axis=1, keepdims=True) + jnp.exp(logit - top)
            outs.append((raised * (1.0 / total)).astype(bf16))
        got = jnp.dot(jnp.concatenate(outs, axis=0), band, preferred_element_type=f32)
        got = got[:, HEAD_DIM : 2 * HEAD_DIM].astype(bf16)
        hidden[place(b) : place(b) + WINDOW, 0:qc] = jnp.concatenate(
            [got[g * WINDOW : (g + 1) * WINDOW] for g in range(group)], axis=1
        )

    blocks = rows // WINDOW
    order = list(range(1, blocks - 1)) + [0, blocks - 1]
    early = (blocks - 2) * WINDOW

    def place(b):
        return order.index(b) * WINDOW

    half_width = 1
    for level in range(1, POOL_GROUPS):
        half_width = jnp.where(t == level, 2**level, half_width)

    def spread_of(start, size):
        length = size + 2 * RIM
        e = chan[start : start + length].astype(f32)
        p = lax.broadcasted_iota(jnp.int32, (length, 1), 0) + (me * rows + start - RIM)
        e = jnp.where((p >= 0) & (p < seq_len), e, 0.0)
        total = e + pltpu.roll(e, 1, 0)
        pick = total
        for level in range(1, POOL_GROUPS):
            step = 2 ** (level - 1)
            total = pltpu.roll(total, step, 0) + pltpu.roll(total, length - step, 0)
            pick = jnp.where(t == level, total, pick)
        number = (jnp.clip(p + half_width, 0, seq_len) - jnp.clip(p - half_width, 0, seq_len)).astype(f32)
        return (pick[RIM : RIM + size] / number[RIM : RIM + size] - e[RIM : RIM + size]).astype(bf16)

    def pooled_of(spread):
        return (jnp.dot(spread, wpool[0], preferred_element_type=f32) * scales[...]).astype(bf16)

    def pool_inner():
        got = pooled_of(spread_of(RIM, rows - 2 * RIM))
        for b in range(blocks):
            low, high = max(b * WINDOW, RIM), min((b + 1) * WINDOW, rows - RIM)
            base = place(b) - b * WINDOW
            hidden[base + low : base + high, qc:] = got[low - RIM : high - RIM]

    def pool_edges():
        got = pooled_of(jnp.concatenate([spread_of(0, RIM), spread_of(rows - RIM, RIM)], axis=0))
        hidden[place(0) : place(0) + RIM, qc:] = got[0:RIM]
        end = place(blocks - 1) + WINDOW
        hidden[end - RIM : end, qc:] = got[RIM:]

    near = 3
    spans = (pl.ds(0, early), pl.ds(early, rows - early))

    def unit(buf, o, u, split):
        return buf.at[o, :, spans[u]] if split else buf.at[o, u]

    def to_mate(o, u, split):
        i = (o // (2 * per)) * per + lax.rem(o, per)
        return rdma(
            unit(part, o, u, split), unit(mated, o, u, split), mate_send.at[i, u], mate_recv.at[i, u], me, mate
        )

    def to_owner(o, u, split):
        i = lax.rem(o, per)
        return rdma(
            unit(part, o, u, split), unit(landed, i, u, split), part_send.at[i, u], part_recv.at[i, u], me, across
        )

    final = origin[n - 1]
    holder = final // per

    def to_echo(h):
        return rdma(part.at[final, h], echo.at[h], echo_send.at[h], echo_recv.at[h], me, across)

    def to_late():
        return rdma(late, late, late_send.at[0], late_recv.at[0], me, mate)

    pieces = [(0, 0), (0, 1)]
    for k in range(1, count, 2):
        d, h = k // QUARTERS, (k % QUARTERS) // 2
        pieces += [(min(2 * d + 1, n - 1), h), (min(2 * d + 2, n - 1), 1 - h)]

    def emit(places, span, split):
        side = jnp.concatenate([wout[origin[i], h].reshape(qc + cc, half) for i, h in places], axis=1)
        got = jnp.dot(hidden[span, :], side, preferred_element_type=f32).astype(bf16)
        for j, (i, h) in enumerate(places):
            part[origin[i], h, span] = got[:, j * half : (j + 1) * half]
        sent = [(i, spans.index(span)) for i, h in places if h == 0] if split else places
        for i, u in sent:
            o = origin[i]

            @pl.when(lax.rem(o // per, 2) != lax.rem(t, 2))
            def _(o=o, u=u):
                to_mate(o, u, split).start()

    def emit_near(u):
        emit([(i, h) for i in range(near) for h in range(2)], spans[u], True)

    def emit_far(ids):
        emit([pieces[i] for i in ids], pl.ds(0, rows), False)

    def combine(i, u, split):
        o = origin[i]
        where = (slice(None), spans[u]) if split else (u,)

        @pl.when(o // per == t)
        def _():
            to_mate(o, u, split).wait_recv()
            both = part[(o,) + where].astype(f32) + mated[(o,) + where].astype(f32)
            own[(lax.rem(o, per),) + where] = both
            if i == n - 1:
                part[(o,) + where] = both.astype(bf16)
                to_echo(u).start()

        @pl.when(o // per == across)
        def _():
            to_mate(o, u, split).wait_recv()
            both = part[(o,) + where].astype(f32) + mated[(o,) + where].astype(f32)
            part[(o,) + where] = both.astype(bf16)
            to_owner(o, u, split).start()

    def combine_near(u):
        for i in range(near):
            combine(i, u, True)

    def combine_far(ids):
        for i in ids:
            combine(pieces[i][0], pieces[i][1], False)

    def pack(one, two):
        one = jnp.sum(one, axis=1, keepdims=True)
        two = jnp.sum(two, axis=1, keepdims=True)
        lane = lax.broadcasted_iota(jnp.int32, (rows, 128), 1)
        return jnp.transpose(jnp.where(lane == 0, one, jnp.where(lane == 1, two, 0.0)))[0:8]

    sums[...] = jnp.zeros_like(sums)
    emits = {5: (6, 8), 7: (8, 10), 9: (10, 12), 11: (12, 14), 13: (14, 16)}
    combines = {7: (6, 8), 8: (8, 10), 10: (10, 12), 12: (12, 14), 13: (14, 16)}
    for k in range(count):
        relay(w_out, k)
        if k < 2:
            for b in order[: blocks - 2][k::2]:
                attend(b)
        elif k == 2:
            pool_inner()
        elif k == 3:
            emit_near(0)
            for c in rims:
                c.wait()
            attend(0)
        elif k == 4:
            attend(blocks - 1)
            combine_near(0)
            pool_edges()
            emit_near(1)
        elif k == 6:
            combine_near(1)
        if k in emits:
            emit_far(range(*emits[k]))
        combine_far(range(*combines.get(k, (0, 0))))

    def stat_copy(j):
        return rdma(stats.at[t], stats.at[t], stat_send.at[j], stat_recv.at[t], me, lax.rem(t + j, tp))

    for i in range(n - 1):
        o = origin[i]

        @pl.when(o // per == t)
        def _(o=o, i=i):
            for u in range(2):
                to_owner(o, u, i < near).wait_recv()

    for i in range(per):
        o = t * per + i

        @pl.when(o != final)
        def _(o=o, i=i):
            one = two = 0.0
            for h in range(2):
                mix = own[i, h] + landed[i, h].astype(f32)
                acc[:, (2 * i + h) * half : (2 * i + h + 1) * half] = mix
                one, two = one + mix, two + mix * mix
            sums[0] += one
            sums[1] += two

    stats[t] = pack(sums[0], sums[1])
    for j in range(1, tp):
        stat_copy(j).start()

    @pl.when(holder == t)
    def _():
        one = two = 0.0
        for h in range(2):
            i = lax.rem(final, per)
            to_owner(final, h, False).wait_recv()
            mix = own[i, h] + landed[i, h].astype(f32)
            acc[:, pl.ds(pl.multiple_of((2 * i + h) * half, 128), half)] = mix
            one, two = one + mix, two + mix * mix
        late[...] = pack(one, two)
        to_late().start()

    @pl.when(holder == across)
    def _():
        one = two = 0.0
        for h in range(2):
            to_echo(h).wait_recv()
            mix = part[final, h].astype(f32) + echo[h].astype(f32)
            one, two = one + mix, two + mix * mix
        late[...] = pack(one, two)
        to_late().start()

    for i in range(n):
        o = origin[i]

        @pl.when(lax.rem(o // per, 2) != lax.rem(t, 2))
        def _(o=o, i=i):
            for u in range(2):
                to_mate(o, u, i < near).wait_send()

        @pl.when(o // per == across)
        def _(o=o, i=i):
            for u in range(2):
                to_owner(o, u, i < near).wait_send()

    @pl.when(holder == t)
    def _():
        for h in range(2):
            to_echo(h).wait_send()

    for turn in range(2 * count - SENDS, 2 * count):
        for way in range(2):
            launched(way, turn).wait_send()
    for b in range(per):
        tok_copy(t, b, b, across).wait_send()
        tok_copy(t, b, per + b, mate).wait_send()
        tok_copy(across, b, 2 * per + b, mate).wait_send()
    for j in range(1, tp):
        src = lax.rem(t + j, tp)
        rdma(stats.at[src], stats.at[src], stat_send.at[j], stat_recv.at[src], me, src).wait_recv()
    paired = lax.rem(holder, 2) == lax.rem(t, 2)

    @pl.when(jnp.logical_not(paired))
    def _():
        to_late().wait_recv()

    totals = late[...] + stats[0]
    for i in range(1, tp):
        totals = totals + stats[i]
    tall = jnp.concatenate([totals, jnp.zeros((120, rows), f32)], axis=0)
    back = jnp.transpose(tall)
    width = gain_ref.shape[1] * tp
    row_mean = back[:, 0:1] / width
    variance = back[:, 1:2] / width - row_mean * row_mean
    scale = lax.rsqrt(variance + epsilon)
    normed = ((acc[:, 0 : gain_ref.shape[1]] - row_mean) * scale * gains[...]).astype(bf16)
    for b in range(blocks):
        out_ref[b * WINDOW : (b + 1) * WINDOW, :] = normed[place(b) : place(b) + WINDOW]
    for j in range(1, tp):
        stat_copy(j).wait_send()

    @pl.when(paired)
    def _():
        to_late().wait_send()


def fused(n, tp, tokens, w_query, w_key, w_value, w_pool_in, sink, w_pool, pool_scale, w_out_attn, w_out_pool, out_gain):
    rows, share = tokens.shape
    depth, qc = w_query.shape
    kc, cc = w_key.shape[1], w_pool_in.shape[1]
    wide = w_out_attn.shape[1]
    half = wide // 2
    per = n // tp
    count = QUARTERS * (n - 1) // 2
    bf16, f32 = jnp.bfloat16, jnp.float32
    dma = pltpu.SemaphoreType.DMA
    return pl.pallas_call(
        functools.partial(mixer_kernel, n, tp),
        out_shape=jax.ShapeDtypeStruct((rows, share), bf16),
        in_specs=[pl.BlockSpec(memory_space=pltpu.HBM)] * 11,
        out_specs=pl.BlockSpec(memory_space=pltpu.VMEM),
        scratch_shapes=[
            pltpu.VMEM((n, QUARTERS, depth // QUARTERS, qc + 2 * kc + cc), bf16),
            pltpu.VMEM((n, 2, 2, qc, half), bf16),
            pltpu.VMEM((n, rows, depth), bf16),
            pltpu.VMEM((rows, qc + 2 * kc + cc), f32),
            pltpu.VMEM((rows, qc), bf16),
            pltpu.VMEM((rows + 2 * WINDOW, 2 * kc), bf16),
            pltpu.VMEM((rows + 2 * RIM, cc), bf16),
            pltpu.VMEM((rows, qc + cc), bf16),
            pltpu.VMEM((n, 2, rows, half), bf16),
            pltpu.VMEM((n, 2, rows, half), bf16),
            pltpu.VMEM((per, 2, rows, half), bf16),
            pltpu.VMEM((per, 2, rows, half), f32),
            pltpu.VMEM((tp, 8, rows), f32),
            pltpu.VMEM((8, rows), f32),
            pltpu.VMEM((2, rows, half), bf16),
            pltpu.VMEM((2, rows, half), f32),
            pltpu.VMEM((2 * kc, depth), bf16),
            pltpu.VMEM((1, sink.shape[0]), f32),
            pltpu.VMEM(w_pool.shape, bf16),
            pltpu.VMEM((1, cc), f32),
            pltpu.VMEM((1, share), f32),
            dma((2, SENDS)),
            dma((2, count)),
            dma((3 * per,)),
            dma((3 * per,)),
            dma((4,)),
            dma((4,)),
            dma((n // 2, 2)),
            dma((n // 2, 2)),
            dma((per, 2)),
            dma((per, 2)),
            dma((2,)),
            dma((2,)),
            dma((per + 12,)),
            dma((tp,)),
            dma((tp,)),
            dma((1,)),
            dma((1,)),
        ],
        compiler_params=pltpu.CompilerParams(
            collective_id=0, has_side_effects=True, vmem_limit_bytes=32 * 1024 * 1024
        ),
        name="mixer",
    )(
        pltpu.with_memory_space_constraint(tokens, pltpu.HBM),
        pltpu.with_memory_space_constraint(w_query.reshape(QUARTERS, -1, qc), pltpu.HBM),
        pltpu.with_memory_space_constraint(w_key.T, pltpu.HBM),
        pltpu.with_memory_space_constraint(w_value.T, pltpu.HBM),
        pltpu.with_memory_space_constraint(w_pool_in.reshape(QUARTERS, -1, cc), pltpu.HBM),
        pltpu.with_memory_space_constraint(sink.reshape(1, -1), pltpu.HBM),
        pltpu.with_memory_space_constraint(w_pool, pltpu.HBM),
        pltpu.with_memory_space_constraint(pool_scale.reshape(1, -1), pltpu.HBM),
        pltpu.with_memory_space_constraint(w_out_attn, pltpu.HBM),
        pltpu.with_memory_space_constraint(w_out_pool, pltpu.HBM),
        pltpu.with_memory_space_constraint(out_gain.reshape(1, -1), pltpu.HBM),
    )


def fits(n, tp, tokens, w_query, w_key, w_pool, w_out_attn):
    return (
        tp == 4
        and n == 2 * tp
        and w_query.shape[0] % 64 == 0
        and w_query.shape[1] % 128 == 0
        and w_key.shape[1] == HEAD_DIM
        and w_pool.shape[0] == 1
        and w_out_attn.shape[1] % 256 == 0
        and w_out_attn.shape[0] == w_query.shape[1]
        and tokens.shape[0] >= 3 * WINDOW
    )


def mixed_rows(*args):
    n, tp = lax.axis_size("sp"), lax.axis_size("tp")
    if fits(n, tp, args[0], args[1], args[2], args[6], args[8]):
        return fused(n, tp, *args)
    return local(*args)


def solution(mesh):
    return jax.shard_map(
        mixed_rows,
        mesh=mesh,
        in_specs=(
            P("sp", "tp"),
            P("sp", "tp"),
            P("sp", "tp"),
            P("sp", "tp"),
            P("sp", "tp"),
            P("tp"),
            P("tp", None, None),
            P("tp"),
            P("tp", "sp"),
            P("tp", "sp"),
            P("tp"),
        ),
        out_specs=P("sp", "tp"),
        check_vma=False,
    )
```

```python
import functools

import jax
import jax.numpy as jnp
from jax import lax
from jax.experimental import pallas as pl
from jax.experimental.pallas import tpu as pltpu
from jax.sharding import PartitionSpec as P

HEAD_DIM = 64
POOL_GROUPS = 4
WINDOW = 128


epsilon = 1e-05
masked_score = -1e30


def padded(cells, sides, width):
    for axis, dim in sides:
        count = lax.axis_size(axis)
        ends = count - 1
        head = lax.slice_in_dim(cells, 0, width, axis=dim)
        tail = lax.slice_in_dim(cells, cells.shape[dim] - width, cells.shape[dim], axis=dim)
        cells = jnp.concatenate(
            [
                lax.ppermute(tail, axis, [(i, (i + 1) % count) for i in range(ends)]),
                cells,
                lax.ppermute(head, axis, [((i + 1) % count, i) for i in range(ends)]),
            ],
            axis=dim,
        )
    return cells


def make_projector(gathered, pieces):
    piece_query, piece_key, piece_value, piece_chan = pieces
    joined = jnp.concatenate([piece_key, piece_value], axis=1)
    return (
        jnp.dot(gathered, piece_query, preferred_element_type=jnp.float32),
        jnp.dot(gathered, joined, preferred_element_type=jnp.float32),
        jnp.dot(gathered, piece_chan, preferred_element_type=jnp.float32),
    )


def attend_local(query, keys_ext, sinks, offset, seq_len, key_cols):
    tok_rows, query_cols = query.shape
    kv_local = key_cols // HEAD_DIM
    group = query_cols // key_cols
    block_count = tok_rows // WINDOW
    stacked = keys_ext.reshape(block_count + 2, WINDOW, 2 * key_cols)
    banded = jnp.concatenate([stacked[:-2], stacked[1:-1], stacked[2:]], axis=1)
    key_band = banded[:, :, :key_cols].reshape(block_count, 3 * WINDOW, kv_local, HEAD_DIM)
    value_band = banded[:, :, key_cols:].reshape(block_count, 3 * WINDOW, kv_local, HEAD_DIM)
    query_blocks = query.reshape(block_count, WINDOW, kv_local, group, HEAD_DIM)
    scores = jnp.einsum(
        "nqkgd,nskd->nkgqs", query_blocks, key_band, preferred_element_type=jnp.float32
    ) * HEAD_DIM ** (-0.5)
    starts = offset + jnp.arange(block_count, dtype=jnp.int32) * WINDOW
    query_pos = starts[:, None] + jnp.arange(WINDOW, dtype=jnp.int32)[None, :]
    key_pos = starts[:, None] + jnp.arange(3 * WINDOW, dtype=jnp.int32)[None, :] - WINDOW
    distance = key_pos[:, None, :] - query_pos[:, :, None]
    inside = (key_pos >= 0) & (key_pos < seq_len)
    keep = (jnp.abs(distance) <= WINDOW) & inside[:, None, :]
    scores = jnp.where(keep[:, None, None], scores, masked_score)
    sink_logit = sinks.reshape(kv_local, group)[None, :, :, None, None]
    top = jnp.maximum(jnp.max(scores, axis=-1, keepdims=True), sink_logit)
    raised = jnp.exp(scores - top)
    total = jnp.sum(raised, axis=-1, keepdims=True) + jnp.exp(sink_logit - top)
    probs = (raised / total).astype(jnp.bfloat16)
    attended = jnp.einsum(
        "nkgqs,nskd->nqkgd", probs, value_band, preferred_element_type=jnp.float32
    )
    return attended.astype(jnp.bfloat16).reshape(tok_rows, query_cols)


def local(
    tokens,
    w_query,
    w_key,
    w_value,
    w_pool_in,
    sink,
    w_pool,
    pool_scale,
    w_out_attn,
    w_out_pool,
    out_gain,
):
    tok_rows = tokens.shape[0]
    seq_len = tok_rows * lax.axis_size("sp")
    offset = lax.axis_index("sp") * tok_rows
    out_both = jnp.concatenate([w_out_attn, w_out_pool], axis=0)
    gathered = lax.all_gather(tokens, "tp", axis=1, tiled=True)
    key_cols = w_key.shape[1]
    chan_cols = w_pool_in.shape[1]
    query_sum, joined_sum, chan_sum = make_projector(
        gathered,
        (
            lax.all_gather(w_query, "sp", axis=0, tiled=True),
            lax.all_gather(w_key, "sp", axis=0, tiled=True),
            lax.all_gather(w_value, "sp", axis=0, tiled=True),
            lax.all_gather(w_pool_in, "sp", axis=0, tiled=True),
        ),
    )
    query = query_sum.astype(jnp.bfloat16)
    key_value = joined_sum.astype(jnp.bfloat16)
    chan = chan_sum.astype(jnp.bfloat16)
    keys_ext = padded(key_value, (("sp", 0),), WINDOW)
    attended = attend_local(query, keys_ext, sink, offset, seq_len, key_cols)
    rim_rows = 2 ** (POOL_GROUPS - 1)
    chan_ext = padded(chan, (("sp", 0),), rim_rows)
    running = jnp.concatenate(
        [jnp.zeros((1, chan_cols), jnp.float32), jnp.cumsum(chan_ext.astype(jnp.float32), axis=0)],
        axis=0,
    )
    chan_float = chan.astype(jnp.float32)
    positions = offset + jnp.arange(tok_rows, dtype=jnp.int32)
    group_count = w_pool.shape[0]
    level = lax.axis_index("tp") * group_count + 0
    half = jnp.left_shift(jnp.int32(1), level)
    upper = lax.dynamic_slice_in_dim(running, rim_rows + half, tok_rows, 0)
    lower = lax.dynamic_slice_in_dim(running, rim_rows - half, tok_rows, 0)
    count = (
        jnp.clip(positions + half, 0, seq_len) - jnp.clip(positions - half, 0, seq_len)
    ).astype(jnp.float32)
    spread = ((upper - lower) / count[:, None] - chan_float).astype(jnp.bfloat16)
    outputs = jnp.dot(spread, w_pool[0], preferred_element_type=jnp.float32)
    pooled = (outputs * pool_scale).astype(jnp.bfloat16)
    hidden = jnp.concatenate([attended, pooled], axis=1)
    terms = jnp.dot(
        hidden,
        lax.all_gather(out_both, "sp", axis=1, tiled=True),
        preferred_element_type=jnp.float32,
    )
    share_width = out_gain.shape[0]
    model_width = share_width * lax.axis_size("tp")
    share = lax.psum_scatter(
        terms.astype(jnp.bfloat16), "tp", scatter_dimension=1, tiled=True
    ).astype(jnp.float32)
    row_total, row_square = lax.psum((jnp.sum(share, axis=1), jnp.sum(share * share, axis=1)), "tp")
    row_mean = row_total / model_width
    variance = row_square / model_width - row_mean * row_mean
    normed = (share - row_mean[:, None]) * lax.rsqrt(variance + epsilon)[:, None] * out_gain
    return normed.astype(jnp.bfloat16)


MESH = pl.DeviceIdType.MESH
RIM = 16
QUARTERS = 4
SENDS = 6
RECVS = 10


def mixer_kernel(
    n,
    tp,
    tok_ref,
    wq_ref,
    wk_ref,
    wv_ref,
    wc_ref,
    sink_ref,
    wp_ref,
    ps_ref,
    woa_ref,
    wop_ref,
    gain_ref,
    out_ref,
    win,
    wout,
    tok,
    acc,
    query,
    kv,
    chan,
    hidden,
    part,
    mated,
    landed,
    own,
    stats,
    late,
    echo,
    sums,
    pair_in,
    sinks,
    wpool,
    scales,
    gains,
    ring_send,
    ring_recv,
    tok_send,
    tok_recv,
    rim_send,
    rim_recv,
    mate_send,
    mate_recv,
    part_send,
    part_recv,
    echo_send,
    echo_recv,
    load,
    stat_send,
    stat_recv,
    late_send,
    late_recv,
):
    f32, bf16 = jnp.float32, jnp.bfloat16
    me, t = lax.axis_index("sp"), lax.axis_index("tp")
    rows = tok_ref.shape[0]
    seq_len = rows * n
    half_n = n // 2
    column = me % 2
    pos = (me // 2) * (1 - column) + column * (n - 1 - me // 2)

    def at(p):
        p = lax.rem(p + n, n)
        back = p // half_n
        return (1 - back) * (2 * p) + back * (2 * (n - 1 - p) + 1)

    ring = (at(pos + 1), at(pos - 1))
    after, before = lax.rem(me + 1, n), lax.rem(me + n - 1, n)
    mate = t + 1 - 2 * lax.rem(t, 2)
    across = lax.rem(t + 2, tp)
    per = n // tp

    def rdma(src, dst, send, recv, sp, tpi):
        return pltpu.make_async_remote_copy(
            src_ref=src,
            dst_ref=dst,
            send_sem=send,
            recv_sem=recv,
            device_id={"sp": sp, "tp": tpi},
            device_id_type=MESH,
        )

    qc, kc = wq_ref.shape[2], wk_ref.shape[0]
    cc = wc_ref.shape[2]
    depth = QUARTERS * wq_ref.shape[1]
    quarter = depth // QUARTERS
    wide = woa_ref.shape[1]
    half = wide // 2
    barrier = pltpu.get_barrier_semaphore()
    peers = [(s, t) for s in ring]
    peers += [(me, mate), (me, across)]
    for s, p in peers:
        pl.semaphore_signal(barrier, inc=1, device_id={"sp": s, "tp": p}, device_id_type=MESH)

    loads = []

    def fetch(src, dst):
        copy = pltpu.make_async_copy(src, dst, load.at[len(loads)])
        copy.start()
        loads.append(copy)
        return copy

    pairs = [fetch(wk_ref, pair_in.at[pl.ds(0, kc)]), fetch(wv_ref, pair_in.at[pl.ds(kc, kc)])]
    first = [
        fetch(wq_ref, win.at[me, :, :, pl.ds(0, qc)]),
        fetch(wc_ref, win.at[me, :, :, pl.ds(qc + 2 * kc, cc)]),
    ]
    own_tok = [fetch(tok_ref.at[:, pl.ds(b * depth, depth)], tok.at[t * per + b]) for b in range(per)]
    later = []
    for h in range(2):
        later.append(fetch(woa_ref.at[:, pl.ds(h * half, half)], wout.at[me, h, 0]))
        later.append(fetch(wop_ref.at[:, pl.ds(h * half, half)], wout.at[me, h, 1]))
    later.append(fetch(sink_ref, sinks))
    later.append(fetch(wp_ref, wpool))
    later.append(fetch(ps_ref, scales))
    later.append(fetch(gain_ref, gains))
    for copy in pairs:
        copy.wait()
    pair = jnp.transpose(pair_in[...].astype(f32)).astype(bf16)
    for h in range(QUARTERS):
        win[me, h, :, qc : qc + 2 * kc] = pair[h * quarter : (h + 1) * quarter]
    for copy in first:
        copy.wait()
    pl.semaphore_wait(barrier, len(peers))

    count = QUARTERS * (n - 1) // 2
    last = count - 1

    def ring_copy(buf, way, k, hop, turn):
        sign = -1 if way == 0 else 1
        q = k % QUARTERS if way == 0 else QUARTERS - 1 - k % QUARTERS
        o = at(pos + sign * (k // QUARTERS + hop))
        slot = buf.at[o, q] if buf is win else buf.at[o, q // 2, q % 2]
        return rdma(slot, slot, ring_send.at[way, turn % SENDS], ring_recv.at[way, turn % RECVS], ring[way], t)

    def w_in(way, k, hop):
        return ring_copy(win, way, k, hop, k)

    def w_out(way, k, hop):
        return ring_copy(wout, way, k, hop, count + k)

    def launched(way, turn):
        return w_in(way, turn, 0) if turn < count else w_out(way, turn - count, 0)

    def launch(way, turn):
        if turn >= SENDS:
            launched(way, turn - SENDS).wait_send()
        launched(way, turn).start()

    def tok_copy(owner, b, i, dst):
        slot = tok.at[owner * per + b]
        return rdma(slot, slot, tok_send.at[i], tok_recv.at[i], me, dst)

    for k in range(QUARTERS):
        for way in range(2):
            launch(way, k)
    for copy in own_tok:
        copy.wait()
    for b in range(per):
        tok_copy(t, b, b, across).start()
    for b in range(per):
        tok_copy(t, b, per + b, mate).start()

    for copy in later:
        copy.wait()

    origin = [at(pos)]
    for d in range(1, half_n):
        origin += [at(pos - d), at(pos + d)]
    origin.append(at(pos + half_n))

    def project(i, first=False):
        o = origin[i]
        w = win[o].reshape(depth, qc + 2 * kc + cc)
        term = jnp.dot(tok[o], w, preferred_element_type=f32)
        if first:
            acc[...] = term
        else:
            acc[...] += term

    def relay(copy, k):
        for way in range(2):
            copy(way, k, 1).wait_recv()
            if k + QUARTERS <= last:
                launch(way, k + QUARTERS + (0 if copy is w_in else count))

    def start_out(k):
        for way in range(2):
            launch(way, count + k)

    done_blocks = 0
    for k in range(count):
        relay(w_in, k)
        if last - 3 <= k < last:
            start_out(k - (last - 3))
        if k in (3, 6):
            b = 0 if k == 3 else 1
            tok_copy(across, b, b, across).wait_recv()
            tok_copy(across, b, 2 * per + b, mate).start()
        if k == 8:
            for b in range(per):
                tok_copy(mate, b, per + b, mate).wait_recv()
                tok_copy(lax.rem(mate + 2, tp), b, 2 * per + b, mate).wait_recv()
        if k >= 8:
            ready = n if k == last else 1 + 2 * ((k + 1) // QUARTERS)
            upto = ready if k == last else min(ready, done_blocks + 2)
            while done_blocks < upto:
                project(done_blocks, done_blocks == 0)
                done_blocks += 1

    kv[WINDOW : WINDOW + rows, :] = acc[:, qc : qc + 2 * kc].astype(bf16)
    chan[RIM : RIM + rows, :] = acc[:, qc + 2 * kc :].astype(bf16)

    def rim(buf, width, down, i):
        if down:
            return rdma(buf.at[pl.ds(rows, width)], buf.at[pl.ds(0, width)], rim_send.at[i], rim_recv.at[i], after, t)
        return rdma(
            buf.at[pl.ds(width, width)], buf.at[pl.ds(rows + width, width)], rim_send.at[i], rim_recv.at[i], before, t
        )

    rims = [rim(kv, WINDOW, True, 0), rim(kv, WINDOW, False, 1), rim(chan, RIM, True, 2), rim(chan, RIM, False, 3)]
    for c in rims:
        c.start()
    start_out(3)
    query[...] = acc[:, 0:qc].astype(bf16)

    group = qc // kc

    def attend(b):
        band = kv[b * WINDOW : (b + 3) * WINDOW, :]
        q = query[b * WINDOW : (b + 1) * WINDOW, :]
        stacked = jnp.concatenate([q[:, g * HEAD_DIM : (g + 1) * HEAD_DIM] for g in range(group)], axis=0)
        scores = lax.dot_general(
            stacked, band[:, :HEAD_DIM], (((1,), (1,)), ((), ())), preferred_element_type=f32
        ) * HEAD_DIM ** (-0.5)
        scores = scores.reshape(group, WINDOW, 3 * WINDOW)
        r = lax.broadcasted_iota(jnp.int32, (WINDOW, 3 * WINDOW), 0)
        c = lax.broadcasted_iota(jnp.int32, (WINDOW, 3 * WINDOW), 1)
        keep = (c >= r) & (c <= r + 2 * WINDOW)
        key_pos = c + (me * rows + b * WINDOW - WINDOW)
        keep = keep & (key_pos >= 0) & (key_pos < seq_len)
        outs = []
        for g in range(group):
            s = jnp.where(keep, scores[g], masked_score)
            logit = sinks[0:1, g : g + 1]
            top = jnp.maximum(jnp.max(s, axis=1, keepdims=True), logit)
            raised = jnp.exp(s - top)
            total = jnp.sum(raised, axis=1, keepdims=True) + jnp.exp(logit - top)
            outs.append((raised * (1.0 / total)).astype(bf16))
        got = jnp.dot(jnp.concatenate(outs, axis=0), band, preferred_element_type=f32)
        got = got[:, HEAD_DIM : 2 * HEAD_DIM].astype(bf16)
        hidden[place(b) : place(b) + WINDOW, 0:qc] = jnp.concatenate(
            [got[g * WINDOW : (g + 1) * WINDOW] for g in range(group)], axis=1
        )

    blocks = rows // WINDOW
    order = list(range(1, blocks - 1)) + [0, blocks - 1]
    early = (blocks - 2) * WINDOW

    def place(b):
        return order.index(b) * WINDOW

    half_width = 1
    for level in range(1, POOL_GROUPS):
        half_width = jnp.where(t == level, 2**level, half_width)

    def spread_of(start, size):
        length = size + 2 * RIM
        e = chan[start : start + length].astype(f32)
        p = lax.broadcasted_iota(jnp.int32, (length, 1), 0) + (me * rows + start - RIM)
        e = jnp.where((p >= 0) & (p < seq_len), e, 0.0)
        total = e + pltpu.roll(e, 1, 0)
        pick = total
        for level in range(1, POOL_GROUPS):
            step = 2 ** (level - 1)
            total = pltpu.roll(total, step, 0) + pltpu.roll(total, length - step, 0)
            pick = jnp.where(t == level, total, pick)
        number = (jnp.clip(p + half_width, 0, seq_len) - jnp.clip(p - half_width, 0, seq_len)).astype(f32)
        return (pick[RIM : RIM + size] / number[RIM : RIM + size] - e[RIM : RIM + size]).astype(bf16)

    def pooled_of(spread):
        return (jnp.dot(spread, wpool[0], preferred_element_type=f32) * scales[...]).astype(bf16)

    def pool_inner():
        got = pooled_of(spread_of(RIM, rows - 2 * RIM))
        for b in range(blocks):
            low, high = max(b * WINDOW, RIM), min((b + 1) * WINDOW, rows - RIM)
            base = place(b) - b * WINDOW
            hidden[base + low : base + high, qc:] = got[low - RIM : high - RIM]

    def pool_edges():
        got = pooled_of(jnp.concatenate([spread_of(0, RIM), spread_of(rows - RIM, RIM)], axis=0))
        hidden[place(0) : place(0) + RIM, qc:] = got[0:RIM]
        end = place(blocks - 1) + WINDOW
        hidden[end - RIM : end, qc:] = got[RIM:]

    near = 3
    spans = (pl.ds(0, early), pl.ds(early, rows - early))

    def unit(buf, o, u, split):
        return buf.at[o, :, spans[u]] if split else buf.at[o, u]

    def to_mate(o, u, split):
        i = (o // (2 * per)) * per + lax.rem(o, per)
        return rdma(
            unit(part, o, u, split), unit(mated, o, u, split), mate_send.at[i, u], mate_recv.at[i, u], me, mate
        )

    def to_owner(o, u, split):
        i = lax.rem(o, per)
        return rdma(
            unit(part, o, u, split), unit(landed, i, u, split), part_send.at[i, u], part_recv.at[i, u], me, across
        )

    final = origin[n - 1]
    holder = final // per

    def to_echo(h):
        return rdma(part.at[final, h], echo.at[h], echo_send.at[h], echo_recv.at[h], me, across)

    def to_late():
        return rdma(late, late, late_send.at[0], late_recv.at[0], me, mate)

    pieces = [(0, 0), (0, 1)]
    for k in range(1, count, 2):
        d, h = k // QUARTERS, (k % QUARTERS) // 2
        pieces += [(min(2 * d + 1, n - 1), h), (min(2 * d + 2, n - 1), 1 - h)]

    def emit(places, span, split):
        side = jnp.concatenate([wout[origin[i], h].reshape(qc + cc, half) for i, h in places], axis=1)
        got = jnp.dot(hidden[span, :], side, preferred_element_type=f32).astype(bf16)
        for j, (i, h) in enumerate(places):
            part[origin[i], h, span] = got[:, j * half : (j + 1) * half]
        sent = [(i, spans.index(span)) for i, h in places if h == 0] if split else places
        for i, u in sent:
            o = origin[i]

            @pl.when(lax.rem(o // per, 2) != lax.rem(t, 2))
            def _(o=o, u=u):
                to_mate(o, u, split).start()

    def emit_near(u):
        emit([(i, h) for i in range(near) for h in range(2)], spans[u], True)

    def emit_far(ids):
        emit([pieces[i] for i in ids], pl.ds(0, rows), False)

    def combine(i, u, split):
        o = origin[i]
        where = (slice(None), spans[u]) if split else (u,)

        @pl.when(o // per == t)
        def _():
            to_mate(o, u, split).wait_recv()
            both = part[(o,) + where].astype(f32) + mated[(o,) + where].astype(f32)
            own[(lax.rem(o, per),) + where] = both
            if i == n - 1:
                part[(o,) + where] = both.astype(bf16)
                to_echo(u).start()

        @pl.when(o // per == across)
        def _():
            to_mate(o, u, split).wait_recv()
            both = part[(o,) + where].astype(f32) + mated[(o,) + where].astype(f32)
            part[(o,) + where] = both.astype(bf16)
            to_owner(o, u, split).start()

    def combine_near(u):
        for i in range(near):
            combine(i, u, True)

    def combine_far(ids):
        for i in ids:
            combine(pieces[i][0], pieces[i][1], False)

    def pack(one, two):
        one = jnp.sum(one, axis=1, keepdims=True)
        two = jnp.sum(two, axis=1, keepdims=True)
        lane = lax.broadcasted_iota(jnp.int32, (rows, 128), 1)
        return jnp.transpose(jnp.where(lane == 0, one, jnp.where(lane == 1, two, 0.0)))[0:8]

    sums[...] = jnp.zeros_like(sums)
    emits = {5: (6, 8), 7: (8, 10), 9: (10, 12), 11: (12, 14), 13: (14, 16)}
    combines = {7: (6, 8), 8: (8, 10), 10: (10, 12), 12: (12, 14), 13: (14, 16)}
    for k in range(count):
        relay(w_out, k)
        if k < 2:
            for b in order[: blocks - 2][k::2]:
                attend(b)
        elif k == 2:
            pool_inner()
        elif k == 3:
            emit_near(0)
            for c in rims:
                c.wait()
            attend(0)
        elif k == 4:
            attend(blocks - 1)
            combine_near(0)
            pool_edges()
            emit_near(1)
        elif k == 6:
            combine_near(1)
        if k in emits:
            emit_far(range(*emits[k]))
        combine_far(range(*combines.get(k, (0, 0))))

    def stat_copy(j):
        return rdma(stats.at[t], stats.at[t], stat_send.at[j], stat_recv.at[t], me, lax.rem(t + j, tp))

    for i in range(n - 1):
        o = origin[i]

        @pl.when(o // per == t)
        def _(o=o, i=i):
            for u in range(2):
                to_owner(o, u, i < near).wait_recv()

    for i in range(per):
        o = t * per + i

        @pl.when(o != final)
        def _(o=o, i=i):
            one = two = 0.0
            for h in range(2):
                mix = own[i, h] + landed[i, h].astype(f32)
                acc[:, (2 * i + h) * half : (2 * i + h + 1) * half] = mix
                one, two = one + mix, two + mix * mix
            sums[0] += one
            sums[1] += two

    stats[t] = pack(sums[0], sums[1])
    for j in range(1, tp):
        stat_copy(j).start()

    @pl.when(holder == t)
    def _():
        one = two = 0.0
        for h in range(2):
            i = lax.rem(final, per)
            to_owner(final, h, False).wait_recv()
            mix = own[i, h] + landed[i, h].astype(f32)
            acc[:, pl.ds(pl.multiple_of((2 * i + h) * half, 128), half)] = mix
            one, two = one + mix, two + mix * mix
        late[...] = pack(one, two)
        to_late().start()

    @pl.when(holder == across)
    def _():
        one = two = 0.0
        for h in range(2):
            to_echo(h).wait_recv()
            mix = part[final, h].astype(f32) + echo[h].astype(f32)
            one, two = one + mix, two + mix * mix
        late[...] = pack(one, two)
        to_late().start()

    for i in range(n):
        o = origin[i]

        @pl.when(lax.rem(o // per, 2) != lax.rem(t, 2))
        def _(o=o, i=i):
            for u in range(2):
                to_mate(o, u, i < near).wait_send()

        @pl.when(o // per == across)
        def _(o=o, i=i):
            for u in range(2):
                to_owner(o, u, i < near).wait_send()

    @pl.when(holder == t)
    def _():
        for h in range(2):
            to_echo(h).wait_send()

    for turn in range(2 * count - SENDS, 2 * count):
        for way in range(2):
            launched(way, turn).wait_send()
    for b in range(per):
        tok_copy(t, b, b, across).wait_send()
        tok_copy(t, b, per + b, mate).wait_send()
        tok_copy(across, b, 2 * per + b, mate).wait_send()
    for j in range(1, tp):
        src = lax.rem(t + j, tp)
        rdma(stats.at[src], stats.at[src], stat_send.at[j], stat_recv.at[src], me, src).wait_recv()
    paired = lax.rem(holder, 2) == lax.rem(t, 2)

    @pl.when(jnp.logical_not(paired))
    def _():
        to_late().wait_recv()

    totals = late[...] + stats[0]
    for i in range(1, tp):
        totals = totals + stats[i]
    tall = jnp.concatenate([totals, jnp.zeros((120, rows), f32)], axis=0)
    back = jnp.transpose(tall)
    width = gain_ref.shape[1] * tp
    row_mean = back[:, 0:1] / width
    variance = back[:, 1:2] / width - row_mean * row_mean
    scale = lax.rsqrt(variance + epsilon)
    normed = ((acc[:, 0 : gain_ref.shape[1]] - row_mean) * scale * gains[...]).astype(bf16)
    for b in range(blocks):
        out_ref[b * WINDOW : (b + 1) * WINDOW, :] = normed[place(b) : place(b) + WINDOW]
    for j in range(1, tp):
        stat_copy(j).wait_send()

    @pl.when(paired)
    def _():
        to_late().wait_send()


def fused(n, tp, tokens, w_query, w_key, w_value, w_pool_in, sink, w_pool, pool_scale, w_out_attn, w_out_pool, out_gain):
    rows, share = tokens.shape
    depth, qc = w_query.shape
    kc, cc = w_key.shape[1], w_pool_in.shape[1]
    wide = w_out_attn.shape[1]
    half = wide // 2
    per = n // tp
    count = QUARTERS * (n - 1) // 2
    bf16, f32 = jnp.bfloat16, jnp.float32
    dma = pltpu.SemaphoreType.DMA
    return pl.pallas_call(
        functools.partial(mixer_kernel, n, tp),
        out_shape=jax.ShapeDtypeStruct((rows, share), bf16),
        in_specs=[pl.BlockSpec(memory_space=pltpu.HBM)] * 11,
        out_specs=pl.BlockSpec(memory_space=pltpu.VMEM),
        scratch_shapes=[
            pltpu.VMEM((n, QUARTERS, depth // QUARTERS, qc + 2 * kc + cc), bf16),
            pltpu.VMEM((n, 2, 2, qc, half), bf16),
            pltpu.VMEM((n, rows, depth), bf16),
            pltpu.VMEM((rows, qc + 2 * kc + cc), f32),
            pltpu.VMEM((rows, qc), bf16),
            pltpu.VMEM((rows + 2 * WINDOW, 2 * kc), bf16),
            pltpu.VMEM((rows + 2 * RIM, cc), bf16),
            pltpu.VMEM((rows, qc + cc), bf16),
            pltpu.VMEM((n, 2, rows, half), bf16),
            pltpu.VMEM((n, 2, rows, half), bf16),
            pltpu.VMEM((per, 2, rows, half), bf16),
            pltpu.VMEM((per, 2, rows, half), f32),
            pltpu.VMEM((tp, 8, rows), f32),
            pltpu.VMEM((8, rows), f32),
            pltpu.VMEM((2, rows, half), bf16),
            pltpu.VMEM((2, rows, half), f32),
            pltpu.VMEM((2 * kc, depth), bf16),
            pltpu.VMEM((1, sink.shape[0]), f32),
            pltpu.VMEM(w_pool.shape, bf16),
            pltpu.VMEM((1, cc), f32),
            pltpu.VMEM((1, share), f32),
            dma((2, SENDS)),
            dma((2, RECVS)),
            dma((3 * per,)),
            dma((3 * per,)),
            dma((4,)),
            dma((4,)),
            dma((n // 2, 2)),
            dma((n // 2, 2)),
            dma((per, 2)),
            dma((per, 2)),
            dma((2,)),
            dma((2,)),
            dma((per + 12,)),
            dma((tp,)),
            dma((tp,)),
            dma((1,)),
            dma((1,)),
        ],
        compiler_params=pltpu.CompilerParams(
            collective_id=0, has_side_effects=True, vmem_limit_bytes=32 * 1024 * 1024
        ),
        name="mixer",
    )(
        pltpu.with_memory_space_constraint(tokens, pltpu.HBM),
        pltpu.with_memory_space_constraint(w_query.reshape(QUARTERS, -1, qc), pltpu.HBM),
        pltpu.with_memory_space_constraint(w_key.T, pltpu.HBM),
        pltpu.with_memory_space_constraint(w_value.T, pltpu.HBM),
        pltpu.with_memory_space_constraint(w_pool_in.reshape(QUARTERS, -1, cc), pltpu.HBM),
        pltpu.with_memory_space_constraint(sink.reshape(1, -1), pltpu.HBM),
        pltpu.with_memory_space_constraint(w_pool, pltpu.HBM),
        pltpu.with_memory_space_constraint(pool_scale.reshape(1, -1), pltpu.HBM),
        pltpu.with_memory_space_constraint(w_out_attn, pltpu.HBM),
        pltpu.with_memory_space_constraint(w_out_pool, pltpu.HBM),
        pltpu.with_memory_space_constraint(out_gain.reshape(1, -1), pltpu.HBM),
    )


def fits(n, tp, tokens, w_query, w_key, w_pool, w_out_attn):
    return (
        tp == 4
        and n == 2 * tp
        and w_query.shape[0] % 64 == 0
        and w_query.shape[1] % 128 == 0
        and w_key.shape[1] == HEAD_DIM
        and w_pool.shape[0] == 1
        and w_out_attn.shape[1] % 256 == 0
        and w_out_attn.shape[0] == w_query.shape[1]
        and tokens.shape[0] >= 3 * WINDOW
    )


def mixed_rows(*args):
    n, tp = lax.axis_size("sp"), lax.axis_size("tp")
    if fits(n, tp, args[0], args[1], args[2], args[6], args[8]):
        return fused(n, tp, *args)
    return local(*args)


def solution(mesh):
    return jax.shard_map(
        mixed_rows,
        mesh=mesh,
        in_specs=(
            P("sp", "tp"),
            P("sp", "tp"),
            P("sp", "tp"),
            P("sp", "tp"),
            P("sp", "tp"),
            P("tp"),
            P("tp", None, None),
            P("tp"),
            P("tp", "sp"),
            P("tp", "sp"),
            P("tp"),
        ),
        out_specs=P("sp", "tp"),
        check_vma=False,
    )
```

```python
import functools

import jax
import jax.numpy as jnp
from jax import lax
from jax.experimental import pallas as pl
from jax.experimental.pallas import tpu as pltpu
from jax.sharding import PartitionSpec as P

HEAD_DIM = 64
POOL_GROUPS = 4
WINDOW = 128


epsilon = 1e-05
masked_score = -1e30


def padded(cells, sides, width):
    for axis, dim in sides:
        count = lax.axis_size(axis)
        ends = count - 1
        head = lax.slice_in_dim(cells, 0, width, axis=dim)
        tail = lax.slice_in_dim(cells, cells.shape[dim] - width, cells.shape[dim], axis=dim)
        cells = jnp.concatenate(
            [
                lax.ppermute(tail, axis, [(i, (i + 1) % count) for i in range(ends)]),
                cells,
                lax.ppermute(head, axis, [((i + 1) % count, i) for i in range(ends)]),
            ],
            axis=dim,
        )
    return cells


def make_projector(gathered, pieces):
    piece_query, piece_key, piece_value, piece_chan = pieces
    joined = jnp.concatenate([piece_key, piece_value], axis=1)
    return (
        jnp.dot(gathered, piece_query, preferred_element_type=jnp.float32),
        jnp.dot(gathered, joined, preferred_element_type=jnp.float32),
        jnp.dot(gathered, piece_chan, preferred_element_type=jnp.float32),
    )


def attend_local(query, keys_ext, sinks, offset, seq_len, key_cols):
    tok_rows, query_cols = query.shape
    kv_local = key_cols // HEAD_DIM
    group = query_cols // key_cols
    block_count = tok_rows // WINDOW
    stacked = keys_ext.reshape(block_count + 2, WINDOW, 2 * key_cols)
    banded = jnp.concatenate([stacked[:-2], stacked[1:-1], stacked[2:]], axis=1)
    key_band = banded[:, :, :key_cols].reshape(block_count, 3 * WINDOW, kv_local, HEAD_DIM)
    value_band = banded[:, :, key_cols:].reshape(block_count, 3 * WINDOW, kv_local, HEAD_DIM)
    query_blocks = query.reshape(block_count, WINDOW, kv_local, group, HEAD_DIM)
    scores = jnp.einsum(
        "nqkgd,nskd->nkgqs", query_blocks, key_band, preferred_element_type=jnp.float32
    ) * HEAD_DIM ** (-0.5)
    starts = offset + jnp.arange(block_count, dtype=jnp.int32) * WINDOW
    query_pos = starts[:, None] + jnp.arange(WINDOW, dtype=jnp.int32)[None, :]
    key_pos = starts[:, None] + jnp.arange(3 * WINDOW, dtype=jnp.int32)[None, :] - WINDOW
    distance = key_pos[:, None, :] - query_pos[:, :, None]
    inside = (key_pos >= 0) & (key_pos < seq_len)
    keep = (jnp.abs(distance) <= WINDOW) & inside[:, None, :]
    scores = jnp.where(keep[:, None, None], scores, masked_score)
    sink_logit = sinks.reshape(kv_local, group)[None, :, :, None, None]
    top = jnp.maximum(jnp.max(scores, axis=-1, keepdims=True), sink_logit)
    raised = jnp.exp(scores - top)
    total = jnp.sum(raised, axis=-1, keepdims=True) + jnp.exp(sink_logit - top)
    probs = (raised / total).astype(jnp.bfloat16)
    attended = jnp.einsum(
        "nkgqs,nskd->nqkgd", probs, value_band, preferred_element_type=jnp.float32
    )
    return attended.astype(jnp.bfloat16).reshape(tok_rows, query_cols)


def local(
    tokens,
    w_query,
    w_key,
    w_value,
    w_pool_in,
    sink,
    w_pool,
    pool_scale,
    w_out_attn,
    w_out_pool,
    out_gain,
):
    tok_rows = tokens.shape[0]
    seq_len = tok_rows * lax.axis_size("sp")
    offset = lax.axis_index("sp") * tok_rows
    out_both = jnp.concatenate([w_out_attn, w_out_pool], axis=0)
    gathered = lax.all_gather(tokens, "tp", axis=1, tiled=True)
    key_cols = w_key.shape[1]
    chan_cols = w_pool_in.shape[1]
    query_sum, joined_sum, chan_sum = make_projector(
        gathered,
        (
            lax.all_gather(w_query, "sp", axis=0, tiled=True),
            lax.all_gather(w_key, "sp", axis=0, tiled=True),
            lax.all_gather(w_value, "sp", axis=0, tiled=True),
            lax.all_gather(w_pool_in, "sp", axis=0, tiled=True),
        ),
    )
    query = query_sum.astype(jnp.bfloat16)
    key_value = joined_sum.astype(jnp.bfloat16)
    chan = chan_sum.astype(jnp.bfloat16)
    keys_ext = padded(key_value, (("sp", 0),), WINDOW)
    attended = attend_local(query, keys_ext, sink, offset, seq_len, key_cols)
    rim_rows = 2 ** (POOL_GROUPS - 1)
    chan_ext = padded(chan, (("sp", 0),), rim_rows)
    running = jnp.concatenate(
        [jnp.zeros((1, chan_cols), jnp.float32), jnp.cumsum(chan_ext.astype(jnp.float32), axis=0)],
        axis=0,
    )
    chan_float = chan.astype(jnp.float32)
    positions = offset + jnp.arange(tok_rows, dtype=jnp.int32)
    group_count = w_pool.shape[0]
    level = lax.axis_index("tp") * group_count + 0
    half = jnp.left_shift(jnp.int32(1), level)
    upper = lax.dynamic_slice_in_dim(running, rim_rows + half, tok_rows, 0)
    lower = lax.dynamic_slice_in_dim(running, rim_rows - half, tok_rows, 0)
    count = (
        jnp.clip(positions + half, 0, seq_len) - jnp.clip(positions - half, 0, seq_len)
    ).astype(jnp.float32)
    spread = ((upper - lower) / count[:, None] - chan_float).astype(jnp.bfloat16)
    outputs = jnp.dot(spread, w_pool[0], preferred_element_type=jnp.float32)
    pooled = (outputs * pool_scale).astype(jnp.bfloat16)
    hidden = jnp.concatenate([attended, pooled], axis=1)
    terms = jnp.dot(
        hidden,
        lax.all_gather(out_both, "sp", axis=1, tiled=True),
        preferred_element_type=jnp.float32,
    )
    share_width = out_gain.shape[0]
    model_width = share_width * lax.axis_size("tp")
    share = lax.psum_scatter(
        terms.astype(jnp.bfloat16), "tp", scatter_dimension=1, tiled=True
    ).astype(jnp.float32)
    row_total, row_square = lax.psum((jnp.sum(share, axis=1), jnp.sum(share * share, axis=1)), "tp")
    row_mean = row_total / model_width
    variance = row_square / model_width - row_mean * row_mean
    normed = (share - row_mean[:, None]) * lax.rsqrt(variance + epsilon)[:, None] * out_gain
    return normed.astype(jnp.bfloat16)


MESH = pl.DeviceIdType.MESH
RIM = 16
QUARTERS = 4
SENDS = 6
RECVS = 10


def mixer_kernel(
    n,
    tp,
    tok_ref,
    wq_ref,
    wk_ref,
    wv_ref,
    wc_ref,
    sink_ref,
    wp_ref,
    ps_ref,
    woa_ref,
    wop_ref,
    gain_ref,
    out_ref,
    win,
    wout,
    tok,
    acc,
    query,
    kv,
    chan,
    hidden,
    part,
    mated,
    landed,
    own,
    stats,
    late,
    echo,
    sums,
    pair_in,
    sinks,
    wpool,
    scales,
    gains,
    ring_send,
    ring_recv,
    tok_send,
    tok_recv,
    rim_send,
    rim_recv,
    mate_send,
    mate_recv,
    part_send,
    part_recv,
    echo_send,
    echo_recv,
    load,
    stat_send,
    stat_recv,
    late_send,
    late_recv,
):
    f32, bf16 = jnp.float32, jnp.bfloat16
    me, t = lax.axis_index("sp"), lax.axis_index("tp")
    rows = tok_ref.shape[0]
    seq_len = rows * n
    half_n = n // 2
    column = me % 2
    pos = (me // 2) * (1 - column) + column * (n - 1 - me // 2)

    def at(p):
        p = lax.rem(p + n, n)
        back = p // half_n
        return (1 - back) * (2 * p) + back * (2 * (n - 1 - p) + 1)

    ring = (at(pos + 1), at(pos - 1))
    after, before = lax.rem(me + 1, n), lax.rem(me + n - 1, n)
    mate = t + 1 - 2 * lax.rem(t, 2)
    across = lax.rem(t + 2, tp)
    per = n // tp

    def rdma(src, dst, send, recv, sp, tpi):
        return pltpu.make_async_remote_copy(
            src_ref=src,
            dst_ref=dst,
            send_sem=send,
            recv_sem=recv,
            device_id={"sp": sp, "tp": tpi},
            device_id_type=MESH,
        )

    qc, kc = wq_ref.shape[2], wk_ref.shape[0]
    cc = wc_ref.shape[2]
    depth = QUARTERS * wq_ref.shape[1]
    quarter = depth // QUARTERS
    wide = woa_ref.shape[1]
    half = wide // 2
    barrier = pltpu.get_barrier_semaphore()
    peers = [(s, t) for s in ring]
    peers += [(me, mate), (me, across)]
    for s, p in peers:
        pl.semaphore_signal(barrier, inc=1, device_id={"sp": s, "tp": p}, device_id_type=MESH)

    loads = []

    def fetch(src, dst):
        copy = pltpu.make_async_copy(src, dst, load.at[len(loads)])
        copy.start()
        loads.append(copy)
        return copy

    pairs = [fetch(wk_ref, pair_in.at[pl.ds(0, kc)]), fetch(wv_ref, pair_in.at[pl.ds(kc, kc)])]
    first = [
        fetch(wq_ref, win.at[me, :, :, pl.ds(0, qc)]),
        fetch(wc_ref, win.at[me, :, :, pl.ds(qc + 2 * kc, cc)]),
    ]
    own_tok = [fetch(tok_ref.at[:, pl.ds(b * depth, depth)], tok.at[t * per + b]) for b in range(per)]
    later = []
    for h in range(2):
        later.append(fetch(woa_ref.at[:, pl.ds(h * half, half)], wout.at[me, h, 0]))
        later.append(fetch(wop_ref.at[:, pl.ds(h * half, half)], wout.at[me, h, 1]))
    later.append(fetch(sink_ref, sinks))
    later.append(fetch(wp_ref, wpool))
    later.append(fetch(ps_ref, scales))
    later.append(fetch(gain_ref, gains))
    for copy in pairs:
        copy.wait()
    pair = jnp.transpose(pair_in[...].astype(f32)).astype(bf16)
    for h in range(QUARTERS):
        win[me, h, :, qc : qc + 2 * kc] = pair[h * quarter : (h + 1) * quarter]
    for copy in first:
        copy.wait()
    pl.semaphore_wait(barrier, len(peers))

    count = QUARTERS * (n - 1) // 2
    last = count - 1

    def ring_copy(buf, way, k, hop, turn):
        sign = -1 if way == 0 else 1
        q = k % QUARTERS if way == 0 else QUARTERS - 1 - k % QUARTERS
        o = at(pos + sign * (k // QUARTERS + hop))
        slot = buf.at[o, q] if buf is win else buf.at[o, q // 2, q % 2]
        return rdma(slot, slot, ring_send.at[way, turn % SENDS], ring_recv.at[way, turn % RECVS], ring[way], t)

    def w_in(way, k, hop):
        return ring_copy(win, way, k, hop, k)

    def w_out(way, k, hop):
        return ring_copy(wout, way, k, hop, count + k)

    def launched(way, turn):
        return w_in(way, turn, 0) if turn < count else w_out(way, turn - count, 0)

    def launch(way, turn):
        if turn >= SENDS:
            launched(way, turn - SENDS).wait_send()
        launched(way, turn).start()

    def tok_copy(owner, b, i, dst):
        slot = tok.at[owner * per + b]
        return rdma(slot, slot, tok_send.at[0], tok_recv.at[i], me, dst)

    for k in range(QUARTERS):
        for way in range(2):
            launch(way, k)
    for copy in own_tok:
        copy.wait()
    for b in range(per):
        tok_copy(t, b, b, across).start()
    for b in range(per):
        tok_copy(t, b, per + b, mate).start()

    for copy in later:
        copy.wait()

    origin = [at(pos)]
    for d in range(1, half_n):
        origin += [at(pos - d), at(pos + d)]
    origin.append(at(pos + half_n))

    def project(i, first=False):
        o = origin[i]
        w = win[o].reshape(depth, qc + 2 * kc + cc)
        term = jnp.dot(tok[o], w, preferred_element_type=f32)
        if first:
            acc[...] = term
        else:
            acc[...] += term

    def relay(copy, k):
        for way in range(2):
            copy(way, k, 1).wait_recv()
            if k + QUARTERS <= last:
                launch(way, k + QUARTERS + (0 if copy is w_in else count))

    def start_out(k):
        for way in range(2):
            launch(way, count + k)

    done_blocks = 0
    for k in range(count):
        relay(w_in, k)
        if last - 3 <= k < last:
            start_out(k - (last - 3))
        if k in (3, 6):
            b = 0 if k == 3 else 1
            tok_copy(across, b, b, across).wait_recv()
            tok_copy(across, b, 2 * per + b, mate).start()
        if k == 8:
            for b in range(per):
                tok_copy(mate, b, per + b, mate).wait_recv()
                tok_copy(lax.rem(mate + 2, tp), b, 2 * per + b, mate).wait_recv()
        if k >= 8:
            ready = n if k == last else 1 + 2 * ((k + 1) // QUARTERS)
            upto = ready if k == last else min(ready, done_blocks + 2)
            while done_blocks < upto:
                project(done_blocks, done_blocks == 0)
                done_blocks += 1

    kv[WINDOW : WINDOW + rows, :] = acc[:, qc : qc + 2 * kc].astype(bf16)
    chan[RIM : RIM + rows, :] = acc[:, qc + 2 * kc :].astype(bf16)

    def rim(buf, width, down, i):
        if down:
            return rdma(buf.at[pl.ds(rows, width)], buf.at[pl.ds(0, width)], rim_send.at[i], rim_recv.at[i], after, t)
        return rdma(
            buf.at[pl.ds(width, width)], buf.at[pl.ds(rows + width, width)], rim_send.at[i], rim_recv.at[i], before, t
        )

    rims = [rim(kv, WINDOW, True, 0), rim(kv, WINDOW, False, 1), rim(chan, RIM, True, 2), rim(chan, RIM, False, 3)]
    for c in rims:
        c.start()
    start_out(3)
    query[...] = acc[:, 0:qc].astype(bf16)

    group = qc // kc

    def attend(b):
        band = kv[b * WINDOW : (b + 3) * WINDOW, :]
        q = query[b * WINDOW : (b + 1) * WINDOW, :]
        stacked = jnp.concatenate([q[:, g * HEAD_DIM : (g + 1) * HEAD_DIM] for g in range(group)], axis=0)
        scores = lax.dot_general(
            stacked, band[:, :HEAD_DIM], (((1,), (1,)), ((), ())), preferred_element_type=f32
        ) * HEAD_DIM ** (-0.5)
        scores = scores.reshape(group, WINDOW, 3 * WINDOW)
        r = lax.broadcasted_iota(jnp.int32, (WINDOW, 3 * WINDOW), 0)
        c = lax.broadcasted_iota(jnp.int32, (WINDOW, 3 * WINDOW), 1)
        keep = (c >= r) & (c <= r + 2 * WINDOW)
        key_pos = c + (me * rows + b * WINDOW - WINDOW)
        keep = keep & (key_pos >= 0) & (key_pos < seq_len)
        outs = []
        for g in range(group):
            s = jnp.where(keep, scores[g], masked_score)
            logit = sinks[0:1, g : g + 1]
            top = jnp.maximum(jnp.max(s, axis=1, keepdims=True), logit)
            raised = jnp.exp(s - top)
            total = jnp.sum(raised, axis=1, keepdims=True) + jnp.exp(logit - top)
            outs.append((raised * (1.0 / total)).astype(bf16))
        got = jnp.dot(jnp.concatenate(outs, axis=0), band, preferred_element_type=f32)
        got = got[:, HEAD_DIM : 2 * HEAD_DIM].astype(bf16)
        hidden[place(b) : place(b) + WINDOW, 0:qc] = jnp.concatenate(
            [got[g * WINDOW : (g + 1) * WINDOW] for g in range(group)], axis=1
        )

    blocks = rows // WINDOW
    order = list(range(1, blocks - 1)) + [0, blocks - 1]
    early = (blocks - 2) * WINDOW

    def place(b):
        return order.index(b) * WINDOW

    half_width = 1
    for level in range(1, POOL_GROUPS):
        half_width = jnp.where(t == level, 2**level, half_width)

    def spread_of(start, size):
        length = size + 2 * RIM
        e = chan[start : start + length].astype(f32)
        p = lax.broadcasted_iota(jnp.int32, (length, 1), 0) + (me * rows + start - RIM)
        e = jnp.where((p >= 0) & (p < seq_len), e, 0.0)
        total = e + pltpu.roll(e, 1, 0)
        pick = total
        for level in range(1, POOL_GROUPS):
            step = 2 ** (level - 1)
            total = pltpu.roll(total, step, 0) + pltpu.roll(total, length - step, 0)
            pick = jnp.where(t == level, total, pick)
        number = (jnp.clip(p + half_width, 0, seq_len) - jnp.clip(p - half_width, 0, seq_len)).astype(f32)
        return (pick[RIM : RIM + size] / number[RIM : RIM + size] - e[RIM : RIM + size]).astype(bf16)

    def pooled_of(spread):
        return (jnp.dot(spread, wpool[0], preferred_element_type=f32) * scales[...]).astype(bf16)

    def pool_inner():
        got = pooled_of(spread_of(RIM, rows - 2 * RIM))
        for b in range(blocks):
            low, high = max(b * WINDOW, RIM), min((b + 1) * WINDOW, rows - RIM)
            base = place(b) - b * WINDOW
            hidden[base + low : base + high, qc:] = got[low - RIM : high - RIM]

    def pool_edges():
        got = pooled_of(jnp.concatenate([spread_of(0, RIM), spread_of(rows - RIM, RIM)], axis=0))
        hidden[place(0) : place(0) + RIM, qc:] = got[0:RIM]
        end = place(blocks - 1) + WINDOW
        hidden[end - RIM : end, qc:] = got[RIM:]

    near = 3
    spans = (pl.ds(0, early), pl.ds(early, rows - early))

    def unit(buf, o, u, split):
        return buf.at[o, :, spans[u]] if split else buf.at[o, u]

    def to_mate(o, u, split):
        i = (o // (2 * per)) * per + lax.rem(o, per)
        return rdma(
            unit(part, o, u, split), unit(mated, o, u, split), mate_send.at[0], mate_recv.at[i, u], me, mate
        )

    def to_owner(o, u, split):
        i = lax.rem(o, per)
        return rdma(
            unit(part, o, u, split), unit(landed, i, u, split), part_send.at[0], part_recv.at[i, u], me, across
        )

    final = origin[n - 1]
    holder = final // per

    def to_echo(h):
        return rdma(part.at[final, h], echo.at[h], echo_send.at[0], echo_recv.at[h], me, across)

    def to_late():
        return rdma(late, late, late_send.at[0], late_recv.at[0], me, mate)

    pieces = [(0, 0), (0, 1)]
    for k in range(1, count, 2):
        d, h = k // QUARTERS, (k % QUARTERS) // 2
        pieces += [(min(2 * d + 1, n - 1), h), (min(2 * d + 2, n - 1), 1 - h)]

    def emit(places, span, split):
        side = jnp.concatenate([wout[origin[i], h].reshape(qc + cc, half) for i, h in places], axis=1)
        got = jnp.dot(hidden[span, :], side, preferred_element_type=f32).astype(bf16)
        for j, (i, h) in enumerate(places):
            part[origin[i], h, span] = got[:, j * half : (j + 1) * half]
        sent = [(i, spans.index(span)) for i, h in places if h == 0] if split else places
        for i, u in sent:
            o = origin[i]

            @pl.when(lax.rem(o // per, 2) != lax.rem(t, 2))
            def _(o=o, u=u):
                to_mate(o, u, split).start()

    def emit_near(u):
        emit([(i, h) for i in range(near) for h in range(2)], spans[u], True)

    def emit_far(ids):
        emit([pieces[i] for i in ids], pl.ds(0, rows), False)

    def combine(i, u, split):
        o = origin[i]
        where = (slice(None), spans[u]) if split else (u,)

        @pl.when(o // per == t)
        def _():
            to_mate(o, u, split).wait_recv()
            both = part[(o,) + where].astype(f32) + mated[(o,) + where].astype(f32)
            own[(lax.rem(o, per),) + where] = both
            if i == n - 1:
                part[(o,) + where] = both.astype(bf16)
                to_echo(u).start()

        @pl.when(o // per == across)
        def _():
            to_mate(o, u, split).wait_recv()
            both = part[(o,) + where].astype(f32) + mated[(o,) + where].astype(f32)
            part[(o,) + where] = both.astype(bf16)
            to_owner(o, u, split).start()

    def combine_near(u):
        for i in range(near):
            combine(i, u, True)

    def combine_far(ids):
        for i in ids:
            combine(pieces[i][0], pieces[i][1], False)

    def pack(one, two):
        one = jnp.sum(one, axis=1, keepdims=True)
        two = jnp.sum(two, axis=1, keepdims=True)
        lane = lax.broadcasted_iota(jnp.int32, (rows, 128), 1)
        return jnp.transpose(jnp.where(lane == 0, one, jnp.where(lane == 1, two, 0.0)))[0:8]

    sums[...] = jnp.zeros_like(sums)
    emits = {5: (6, 8), 7: (8, 10), 9: (10, 12), 11: (12, 14), 13: (14, 16)}
    odd = lax.rem(t, 2) == 1
    ahead = {6: (6, 8), 7: (8, 10), 9: (10, 12), 11: (12, 14)}
    behind = {7: (6, 8), 8: (8, 10), 10: (10, 12), 13: (12, 14)}

    def on(core, work, *args):
        @pl.when(odd == core)
        def _():
            work(*args)

    for k in range(count):
        relay(w_out, k)
        if k < 2:
            for b in order[: blocks - 2][k::2]:
                attend(b)
        elif k == 2:
            pool_inner()
        elif k == 3:
            emit_near(0)
            for c in rims:
                c.wait()
            attend(0)
            on(False, combine_near, 0)
        elif k == 4:
            attend(blocks - 1)
            on(True, combine_near, 0)
            pool_edges()
            emit_near(1)
        if k in emits:
            emit_far(range(*emits[k]))
        if k == 5:
            on(False, combine_near, 1)
        elif k == 6:
            on(True, combine_near, 1)
        if k in ahead:
            on(False, combine_far, range(*ahead[k]))
        if k in behind:
            on(True, combine_far, range(*behind[k]))
    combine_far(range(14, 16))

    def stat_copy(j):
        return rdma(stats.at[t], stats.at[t], stat_send.at[0], stat_recv.at[t], me, lax.rem(t + j, tp))

    for i in range(n - 1):
        o = origin[i]

        @pl.when(o // per == t)
        def _(o=o, i=i):
            for u in range(2):
                to_owner(o, u, i < near).wait_recv()

    for i in range(per):
        o = t * per + i

        @pl.when(o != final)
        def _(o=o, i=i):
            one = two = 0.0
            for h in range(2):
                mix = own[i, h] + landed[i, h].astype(f32)
                acc[:, (2 * i + h) * half : (2 * i + h + 1) * half] = mix
                one, two = one + mix, two + mix * mix
            sums[0] += one
            sums[1] += two

    stats[t] = pack(sums[0], sums[1])
    for j in range(1, tp):
        stat_copy(j).start()

    @pl.when(holder == t)
    def _():
        one = two = 0.0
        for h in range(2):
            i = lax.rem(final, per)
            to_owner(final, h, False).wait_recv()
            mix = own[i, h] + landed[i, h].astype(f32)
            acc[:, pl.ds(pl.multiple_of((2 * i + h) * half, 128), half)] = mix
            one, two = one + mix, two + mix * mix
        late[...] = pack(one, two)
        to_late().start()

    @pl.when(holder == across)
    def _():
        one = two = 0.0
        for h in range(2):
            to_echo(h).wait_recv()
            mix = part[final, h].astype(f32) + echo[h].astype(f32)
            one, two = one + mix, two + mix * mix
        late[...] = pack(one, two)
        to_late().start()

    def drain(buf, amount, sem):
        whole = buf.at[pl.ds(0, amount)]
        rdma(whole, whole, sem.at[0], mate_recv.at[0, 0], me, mate).wait_send()

    drain(part, n // 2, mate_send)
    drain(part, per, part_send)
    drain(tok, 3 * per, tok_send)

    @pl.when(holder == t)
    def _():
        drain(part, 1, echo_send)

    for turn in range(2 * count - SENDS, 2 * count):
        for way in range(2):
            launched(way, turn).wait_send()
    for j in range(1, tp):
        src = lax.rem(t + j, tp)
        rdma(stats.at[src], stats.at[src], stat_send.at[0], stat_recv.at[src], me, src).wait_recv()
    paired = lax.rem(holder, 2) == lax.rem(t, 2)

    @pl.when(jnp.logical_not(paired))
    def _():
        to_late().wait_recv()

    totals = late[...] + stats[0]
    for i in range(1, tp):
        totals = totals + stats[i]
    tall = jnp.concatenate([totals, jnp.zeros((120, rows), f32)], axis=0)
    back = jnp.transpose(tall)
    width = gain_ref.shape[1] * tp
    row_mean = back[:, 0:1] / width
    variance = back[:, 1:2] / width - row_mean * row_mean
    scale = lax.rsqrt(variance + epsilon)
    normed = ((acc[:, 0 : gain_ref.shape[1]] - row_mean) * scale * gains[...]).astype(bf16)
    for b in range(blocks):
        out_ref[b * WINDOW : (b + 1) * WINDOW, :] = normed[place(b) : place(b) + WINDOW]
    drain(stats, tp - 1, stat_send)

    @pl.when(paired)
    def _():
        to_late().wait_send()


def fused(n, tp, tokens, w_query, w_key, w_value, w_pool_in, sink, w_pool, pool_scale, w_out_attn, w_out_pool, out_gain):
    rows, share = tokens.shape
    depth, qc = w_query.shape
    kc, cc = w_key.shape[1], w_pool_in.shape[1]
    wide = w_out_attn.shape[1]
    half = wide // 2
    per = n // tp
    count = QUARTERS * (n - 1) // 2
    bf16, f32 = jnp.bfloat16, jnp.float32
    dma = pltpu.SemaphoreType.DMA
    return pl.pallas_call(
        functools.partial(mixer_kernel, n, tp),
        out_shape=jax.ShapeDtypeStruct((rows, share), bf16),
        in_specs=[pl.BlockSpec(memory_space=pltpu.HBM)] * 11,
        out_specs=pl.BlockSpec(memory_space=pltpu.VMEM),
        scratch_shapes=[
            pltpu.VMEM((n, QUARTERS, depth // QUARTERS, qc + 2 * kc + cc), bf16),
            pltpu.VMEM((n, 2, 2, qc, half), bf16),
            pltpu.VMEM((n, rows, depth), bf16),
            pltpu.VMEM((rows, qc + 2 * kc + cc), f32),
            pltpu.VMEM((rows, qc), bf16),
            pltpu.VMEM((rows + 2 * WINDOW, 2 * kc), bf16),
            pltpu.VMEM((rows + 2 * RIM, cc), bf16),
            pltpu.VMEM((rows, qc + cc), bf16),
            pltpu.VMEM((n, 2, rows, half), bf16),
            pltpu.VMEM((n, 2, rows, half), bf16),
            pltpu.VMEM((per, 2, rows, half), bf16),
            pltpu.VMEM((per, 2, rows, half), f32),
            pltpu.VMEM((tp, 8, rows), f32),
            pltpu.VMEM((8, rows), f32),
            pltpu.VMEM((2, rows, half), bf16),
            pltpu.VMEM((2, rows, half), f32),
            pltpu.VMEM((2 * kc, depth), bf16),
            pltpu.VMEM((1, sink.shape[0]), f32),
            pltpu.VMEM(w_pool.shape, bf16),
            pltpu.VMEM((1, cc), f32),
            pltpu.VMEM((1, share), f32),
            dma((2, SENDS)),
            dma((2, RECVS)),
            dma((1,)),
            dma((3 * per,)),
            dma((4,)),
            dma((4,)),
            dma((1,)),
            dma((n // 2, 2)),
            dma((1,)),
            dma((per, 2)),
            dma((1,)),
            dma((2,)),
            dma((per + 12,)),
            dma((1,)),
            dma((tp,)),
            dma((1,)),
            dma((1,)),
        ],
        compiler_params=pltpu.CompilerParams(
            collective_id=0, has_side_effects=True, vmem_limit_bytes=32 * 1024 * 1024
        ),
        name="mixer",
    )(
        pltpu.with_memory_space_constraint(tokens, pltpu.HBM),
        pltpu.with_memory_space_constraint(w_query.reshape(QUARTERS, -1, qc), pltpu.HBM),
        pltpu.with_memory_space_constraint(w_key.T, pltpu.HBM),
        pltpu.with_memory_space_constraint(w_value.T, pltpu.HBM),
        pltpu.with_memory_space_constraint(w_pool_in.reshape(QUARTERS, -1, cc), pltpu.HBM),
        pltpu.with_memory_space_constraint(sink.reshape(1, -1), pltpu.HBM),
        pltpu.with_memory_space_constraint(w_pool, pltpu.HBM),
        pltpu.with_memory_space_constraint(pool_scale.reshape(1, -1), pltpu.HBM),
        pltpu.with_memory_space_constraint(w_out_attn, pltpu.HBM),
        pltpu.with_memory_space_constraint(w_out_pool, pltpu.HBM),
        pltpu.with_memory_space_constraint(out_gain.reshape(1, -1), pltpu.HBM),
    )


def fits(n, tp, tokens, w_query, w_key, w_pool, w_out_attn):
    return (
        tp == 4
        and n == 2 * tp
        and w_query.shape[0] % 64 == 0
        and w_query.shape[1] % 128 == 0
        and w_key.shape[1] == HEAD_DIM
        and w_pool.shape[0] == 1
        and w_out_attn.shape[1] % 256 == 0
        and w_out_attn.shape[0] == w_query.shape[1]
        and tokens.shape[0] >= 3 * WINDOW
    )


def mixed_rows(*args):
    n, tp = lax.axis_size("sp"), lax.axis_size("tp")
    if fits(n, tp, args[0], args[1], args[2], args[6], args[8]):
        return fused(n, tp, *args)
    return local(*args)


def solution(mesh):
    return jax.shard_map(
        mixed_rows,
        mesh=mesh,
        in_specs=(
            P("sp", "tp"),
            P("sp", "tp"),
            P("sp", "tp"),
            P("sp", "tp"),
            P("sp", "tp"),
            P("tp"),
            P("tp", None, None),
            P("tp"),
            P("tp", "sp"),
            P("tp", "sp"),
            P("tp"),
        ),
        out_specs=P("sp", "tp"),
        check_vma=False,
    )
```

```python
import functools

import jax
import jax.numpy as jnp
from jax import lax
from jax.experimental import pallas as pl
from jax.experimental.pallas import tpu as pltpu
from jax.sharding import PartitionSpec as P

HEAD_DIM = 64
POOL_GROUPS = 4
WINDOW = 128


epsilon = 1e-05
masked_score = -1e30


def padded(cells, sides, width):
    for axis, dim in sides:
        count = lax.axis_size(axis)
        ends = count - 1
        head = lax.slice_in_dim(cells, 0, width, axis=dim)
        tail = lax.slice_in_dim(cells, cells.shape[dim] - width, cells.shape[dim], axis=dim)
        cells = jnp.concatenate(
            [
                lax.ppermute(tail, axis, [(i, (i + 1) % count) for i in range(ends)]),
                cells,
                lax.ppermute(head, axis, [((i + 1) % count, i) for i in range(ends)]),
            ],
            axis=dim,
        )
    return cells


def make_projector(gathered, pieces):
    piece_query, piece_key, piece_value, piece_chan = pieces
    joined = jnp.concatenate([piece_key, piece_value], axis=1)
    return (
        jnp.dot(gathered, piece_query, preferred_element_type=jnp.float32),
        jnp.dot(gathered, joined, preferred_element_type=jnp.float32),
        jnp.dot(gathered, piece_chan, preferred_element_type=jnp.float32),
    )


def attend_local(query, keys_ext, sinks, offset, seq_len, key_cols):
    tok_rows, query_cols = query.shape
    kv_local = key_cols // HEAD_DIM
    group = query_cols // key_cols
    block_count = tok_rows // WINDOW
    stacked = keys_ext.reshape(block_count + 2, WINDOW, 2 * key_cols)
    banded = jnp.concatenate([stacked[:-2], stacked[1:-1], stacked[2:]], axis=1)
    key_band = banded[:, :, :key_cols].reshape(block_count, 3 * WINDOW, kv_local, HEAD_DIM)
    value_band = banded[:, :, key_cols:].reshape(block_count, 3 * WINDOW, kv_local, HEAD_DIM)
    query_blocks = query.reshape(block_count, WINDOW, kv_local, group, HEAD_DIM)
    scores = jnp.einsum(
        "nqkgd,nskd->nkgqs", query_blocks, key_band, preferred_element_type=jnp.float32
    ) * HEAD_DIM ** (-0.5)
    starts = offset + jnp.arange(block_count, dtype=jnp.int32) * WINDOW
    query_pos = starts[:, None] + jnp.arange(WINDOW, dtype=jnp.int32)[None, :]
    key_pos = starts[:, None] + jnp.arange(3 * WINDOW, dtype=jnp.int32)[None, :] - WINDOW
    distance = key_pos[:, None, :] - query_pos[:, :, None]
    inside = (key_pos >= 0) & (key_pos < seq_len)
    keep = (jnp.abs(distance) <= WINDOW) & inside[:, None, :]
    scores = jnp.where(keep[:, None, None], scores, masked_score)
    sink_logit = sinks.reshape(kv_local, group)[None, :, :, None, None]
    top = jnp.maximum(jnp.max(scores, axis=-1, keepdims=True), sink_logit)
    raised = jnp.exp(scores - top)
    total = jnp.sum(raised, axis=-1, keepdims=True) + jnp.exp(sink_logit - top)
    probs = (raised / total).astype(jnp.bfloat16)
    attended = jnp.einsum(
        "nkgqs,nskd->nqkgd", probs, value_band, preferred_element_type=jnp.float32
    )
    return attended.astype(jnp.bfloat16).reshape(tok_rows, query_cols)


def local(
    tokens,
    w_query,
    w_key,
    w_value,
    w_pool_in,
    sink,
    w_pool,
    pool_scale,
    w_out_attn,
    w_out_pool,
    out_gain,
):
    tok_rows = tokens.shape[0]
    seq_len = tok_rows * lax.axis_size("sp")
    offset = lax.axis_index("sp") * tok_rows
    out_both = jnp.concatenate([w_out_attn, w_out_pool], axis=0)
    gathered = lax.all_gather(tokens, "tp", axis=1, tiled=True)
    key_cols = w_key.shape[1]
    chan_cols = w_pool_in.shape[1]
    query_sum, joined_sum, chan_sum = make_projector(
        gathered,
        (
            lax.all_gather(w_query, "sp", axis=0, tiled=True),
            lax.all_gather(w_key, "sp", axis=0, tiled=True),
            lax.all_gather(w_value, "sp", axis=0, tiled=True),
            lax.all_gather(w_pool_in, "sp", axis=0, tiled=True),
        ),
    )
    query = query_sum.astype(jnp.bfloat16)
    key_value = joined_sum.astype(jnp.bfloat16)
    chan = chan_sum.astype(jnp.bfloat16)
    keys_ext = padded(key_value, (("sp", 0),), WINDOW)
    attended = attend_local(query, keys_ext, sink, offset, seq_len, key_cols)
    rim_rows = 2 ** (POOL_GROUPS - 1)
    chan_ext = padded(chan, (("sp", 0),), rim_rows)
    running = jnp.concatenate(
        [jnp.zeros((1, chan_cols), jnp.float32), jnp.cumsum(chan_ext.astype(jnp.float32), axis=0)],
        axis=0,
    )
    chan_float = chan.astype(jnp.float32)
    positions = offset + jnp.arange(tok_rows, dtype=jnp.int32)
    group_count = w_pool.shape[0]
    level = lax.axis_index("tp") * group_count + 0
    half = jnp.left_shift(jnp.int32(1), level)
    upper = lax.dynamic_slice_in_dim(running, rim_rows + half, tok_rows, 0)
    lower = lax.dynamic_slice_in_dim(running, rim_rows - half, tok_rows, 0)
    count = (
        jnp.clip(positions + half, 0, seq_len) - jnp.clip(positions - half, 0, seq_len)
    ).astype(jnp.float32)
    spread = ((upper - lower) / count[:, None] - chan_float).astype(jnp.bfloat16)
    outputs = jnp.dot(spread, w_pool[0], preferred_element_type=jnp.float32)
    pooled = (outputs * pool_scale).astype(jnp.bfloat16)
    hidden = jnp.concatenate([attended, pooled], axis=1)
    terms = jnp.dot(
        hidden,
        lax.all_gather(out_both, "sp", axis=1, tiled=True),
        preferred_element_type=jnp.float32,
    )
    share_width = out_gain.shape[0]
    model_width = share_width * lax.axis_size("tp")
    share = lax.psum_scatter(
        terms.astype(jnp.bfloat16), "tp", scatter_dimension=1, tiled=True
    ).astype(jnp.float32)
    row_total, row_square = lax.psum((jnp.sum(share, axis=1), jnp.sum(share * share, axis=1)), "tp")
    row_mean = row_total / model_width
    variance = row_square / model_width - row_mean * row_mean
    normed = (share - row_mean[:, None]) * lax.rsqrt(variance + epsilon)[:, None] * out_gain
    return normed.astype(jnp.bfloat16)


MESH = pl.DeviceIdType.MESH
RIM = 16
QUARTERS = 4
SENDS = 6
RECVS = 10


def mixer_kernel(
    n,
    tp,
    tok_ref,
    wq_ref,
    wk_ref,
    wv_ref,
    wc_ref,
    sink_ref,
    wp_ref,
    ps_ref,
    woa_ref,
    wop_ref,
    gain_ref,
    out_ref,
    win,
    wout,
    tok,
    acc,
    query,
    kv,
    chan,
    hidden,
    part,
    mated,
    landed,
    own,
    stats,
    late,
    echo,
    sums,
    pair_in,
    sinks,
    wpool,
    scales,
    gains,
    ring_send,
    ring_recv,
    tok_send,
    tok_recv,
    rim_send,
    rim_recv,
    mate_send,
    mate_recv,
    part_send,
    part_recv,
    echo_send,
    echo_recv,
    load,
    stat_send,
    stat_recv,
    late_send,
    late_recv,
):
    f32, bf16 = jnp.float32, jnp.bfloat16
    me, t = lax.axis_index("sp"), lax.axis_index("tp")
    rows = tok_ref.shape[0]
    seq_len = rows * n
    half_n = n // 2
    column = me % 2
    pos = (me // 2) * (1 - column) + column * (n - 1 - me // 2)

    def at(p):
        p = lax.rem(p + n, n)
        back = p // half_n
        return (1 - back) * (2 * p) + back * (2 * (n - 1 - p) + 1)

    ring = (at(pos + 1), at(pos - 1))
    after, before = lax.rem(me + 1, n), lax.rem(me + n - 1, n)
    mate = t + 1 - 2 * lax.rem(t, 2)
    across = lax.rem(t + 2, tp)
    per = n // tp

    def rdma(src, dst, send, recv, sp, tpi):
        return pltpu.make_async_remote_copy(
            src_ref=src,
            dst_ref=dst,
            send_sem=send,
            recv_sem=recv,
            device_id={"sp": sp, "tp": tpi},
            device_id_type=MESH,
        )

    qc, kc = wq_ref.shape[2], wk_ref.shape[0]
    cc = wc_ref.shape[2]
    depth = QUARTERS * wq_ref.shape[1]
    quarter = depth // QUARTERS
    wide = woa_ref.shape[1]
    half = wide // 2
    barrier = pltpu.get_barrier_semaphore()
    peers = [(s, t) for s in ring]
    peers += [(me, mate), (me, across)]
    for s, p in peers:
        pl.semaphore_signal(barrier, inc=1, device_id={"sp": s, "tp": p}, device_id_type=MESH)

    loads = []

    def fetch(src, dst):
        copy = pltpu.make_async_copy(src, dst, load.at[len(loads)])
        copy.start()
        loads.append(copy)
        return copy

    pairs = [fetch(wk_ref, pair_in.at[pl.ds(0, kc)]), fetch(wv_ref, pair_in.at[pl.ds(kc, kc)])]
    first = [
        fetch(wq_ref, win.at[me, :, :, pl.ds(0, qc)]),
        fetch(wc_ref, win.at[me, :, :, pl.ds(qc + 2 * kc, cc)]),
    ]
    own_tok = [fetch(tok_ref.at[:, pl.ds(b * depth, depth)], tok.at[t * per + b]) for b in range(per)]
    later = []
    for h in range(2):
        later.append(fetch(woa_ref.at[:, pl.ds(h * half, half)], wout.at[me, h, 0]))
        later.append(fetch(wop_ref.at[:, pl.ds(h * half, half)], wout.at[me, h, 1]))
    later.append(fetch(sink_ref, sinks))
    later.append(fetch(wp_ref, wpool))
    later.append(fetch(ps_ref, scales))
    later.append(fetch(gain_ref, gains))
    for copy in pairs:
        copy.wait()
    pair = jnp.transpose(pair_in[...].astype(f32)).astype(bf16)
    for h in range(QUARTERS):
        win[me, h, :, qc : qc + 2 * kc] = pair[h * quarter : (h + 1) * quarter]
    for copy in first:
        copy.wait()
    pl.semaphore_wait(barrier, len(peers))

    count = QUARTERS * (n - 1) // 2
    last = count - 1

    def ring_copy(buf, way, k, hop, turn):
        sign = -1 if way == 0 else 1
        q = k % QUARTERS
        o = at(pos + sign * (k // QUARTERS + hop))
        if buf is win:
            slot = buf.at[o, q if way == 0 else QUARTERS - 1 - q]
        elif k >= last - 1:
            slot = buf.at[o, q, way]
        else:
            slot = buf.at[o, q // 2, (q + way) % 2]
        return rdma(slot, slot, ring_send.at[way, turn % SENDS], ring_recv.at[way, turn % RECVS], ring[way], t)

    def w_in(way, k, hop):
        return ring_copy(win, way, k, hop, k)

    def w_out(way, k, hop):
        return ring_copy(wout, way, k, hop, count + k)

    def launched(way, turn):
        return w_in(way, turn, 0) if turn < count else w_out(way, turn - count, 0)

    def launch(way, turn):
        if turn >= SENDS:
            launched(way, turn - SENDS).wait_send()
        launched(way, turn).start()

    def tok_copy(owner, b, i, dst):
        slot = tok.at[owner * per + b]
        return rdma(slot, slot, tok_send.at[0], tok_recv.at[i], me, dst)

    for k in range(QUARTERS):
        for way in range(2):
            launch(way, k)
    for copy in own_tok:
        copy.wait()
    for b in range(per):
        tok_copy(t, b, b, across).start()
    for b in range(per):
        tok_copy(t, b, per + b, mate).start()

    for copy in later:
        copy.wait()

    origin = [at(pos)]
    for d in range(1, half_n):
        origin += [at(pos - d), at(pos + d)]
    origin.append(at(pos + half_n))

    def project(i, first=False):
        o = origin[i]
        w = win[o].reshape(depth, qc + 2 * kc + cc)
        term = jnp.dot(tok[o], w, preferred_element_type=f32)
        if first:
            acc[...] = term
        else:
            acc[...] += term

    def relay(copy, k):
        for way in range(2):
            copy(way, k, 1).wait_recv()
            if copy is w_in:
                if k + QUARTERS <= last:
                    launch(way, k + QUARTERS)
            elif k + QUARTERS < last:
                launch(way, count + k + QUARTERS)
            elif k == last - 3:
                launch(way, count + last)

    def start_out(k):
        for way in range(2):
            launch(way, count + k)

    done_blocks = 0
    for k in range(count):
        relay(w_in, k)
        if last - 3 <= k < last:
            start_out(k - (last - 3))
        if k in (3, 6):
            b = 0 if k == 3 else 1
            tok_copy(across, b, b, across).wait_recv()
            tok_copy(across, b, 2 * per + b, mate).start()
        if k == 8:
            for b in range(per):
                tok_copy(mate, b, per + b, mate).wait_recv()
                tok_copy(lax.rem(mate + 2, tp), b, 2 * per + b, mate).wait_recv()
        if k >= 8:
            ready = n if k == last else 1 + 2 * ((k + 1) // QUARTERS)
            upto = ready if k == last else min(ready, done_blocks + 2)
            while done_blocks < upto:
                project(done_blocks, done_blocks == 0)
                done_blocks += 1

    kv[WINDOW : WINDOW + rows, :] = acc[:, qc : qc + 2 * kc].astype(bf16)
    chan[RIM : RIM + rows, :] = acc[:, qc + 2 * kc :].astype(bf16)

    def rim(buf, width, down, i):
        if down:
            return rdma(buf.at[pl.ds(rows, width)], buf.at[pl.ds(0, width)], rim_send.at[i], rim_recv.at[i], after, t)
        return rdma(
            buf.at[pl.ds(width, width)], buf.at[pl.ds(rows + width, width)], rim_send.at[i], rim_recv.at[i], before, t
        )

    rims = [rim(kv, WINDOW, True, 0), rim(kv, WINDOW, False, 1), rim(chan, RIM, True, 2), rim(chan, RIM, False, 3)]
    for c in rims:
        c.start()
    start_out(3)
    query[...] = acc[:, 0:qc].astype(bf16)

    group = qc // kc

    def attend(b):
        band = kv[b * WINDOW : (b + 3) * WINDOW, :]
        q = query[b * WINDOW : (b + 1) * WINDOW, :]
        stacked = jnp.concatenate([q[:, g * HEAD_DIM : (g + 1) * HEAD_DIM] for g in range(group)], axis=0)
        scores = lax.dot_general(
            stacked, band[:, :HEAD_DIM], (((1,), (1,)), ((), ())), preferred_element_type=f32
        ) * HEAD_DIM ** (-0.5)
        scores = scores.reshape(group, WINDOW, 3 * WINDOW)
        r = lax.broadcasted_iota(jnp.int32, (WINDOW, 3 * WINDOW), 0)
        c = lax.broadcasted_iota(jnp.int32, (WINDOW, 3 * WINDOW), 1)
        keep = (c >= r) & (c <= r + 2 * WINDOW)
        key_pos = c + (me * rows + b * WINDOW - WINDOW)
        keep = keep & (key_pos >= 0) & (key_pos < seq_len)
        outs = []
        for g in range(group):
            s = jnp.where(keep, scores[g], masked_score)
            logit = sinks[0:1, g : g + 1]
            top = jnp.maximum(jnp.max(s, axis=1, keepdims=True), logit)
            raised = jnp.exp(s - top)
            total = jnp.sum(raised, axis=1, keepdims=True) + jnp.exp(logit - top)
            outs.append((raised * (1.0 / total)).astype(bf16))
        got = jnp.dot(jnp.concatenate(outs, axis=0), band, preferred_element_type=f32)
        got = got[:, HEAD_DIM : 2 * HEAD_DIM].astype(bf16)
        hidden[place(b) : place(b) + WINDOW, 0:qc] = jnp.concatenate(
            [got[g * WINDOW : (g + 1) * WINDOW] for g in range(group)], axis=1
        )

    blocks = rows // WINDOW
    order = list(range(1, blocks - 1)) + [0, blocks - 1]
    early = (blocks - 2) * WINDOW

    def place(b):
        return order.index(b) * WINDOW

    half_width = 1
    for level in range(1, POOL_GROUPS):
        half_width = jnp.where(t == level, 2**level, half_width)

    def spread_of(start, size):
        length = size + 2 * RIM
        e = chan[start : start + length].astype(f32)
        p = lax.broadcasted_iota(jnp.int32, (length, 1), 0) + (me * rows + start - RIM)
        e = jnp.where((p >= 0) & (p < seq_len), e, 0.0)
        total = e + pltpu.roll(e, 1, 0)
        pick = total
        for level in range(1, POOL_GROUPS):
            step = 2 ** (level - 1)
            total = pltpu.roll(total, step, 0) + pltpu.roll(total, length - step, 0)
            pick = jnp.where(t == level, total, pick)
        number = (jnp.clip(p + half_width, 0, seq_len) - jnp.clip(p - half_width, 0, seq_len)).astype(f32)
        return (pick[RIM : RIM + size] / number[RIM : RIM + size] - e[RIM : RIM + size]).astype(bf16)

    def pooled_of(spread):
        return (jnp.dot(spread, wpool[0], preferred_element_type=f32) * scales[...]).astype(bf16)

    def pool_inner():
        got = pooled_of(spread_of(RIM, rows - 2 * RIM))
        for b in range(blocks):
            low, high = max(b * WINDOW, RIM), min((b + 1) * WINDOW, rows - RIM)
            base = place(b) - b * WINDOW
            hidden[base + low : base + high, qc:] = got[low - RIM : high - RIM]

    def pool_edges():
        got = pooled_of(jnp.concatenate([spread_of(0, RIM), spread_of(rows - RIM, RIM)], axis=0))
        hidden[place(0) : place(0) + RIM, qc:] = got[0:RIM]
        end = place(blocks - 1) + WINDOW
        hidden[end - RIM : end, qc:] = got[RIM:]

    near = 3
    spans = (pl.ds(0, early), pl.ds(early, rows - early))

    def unit(buf, o, u, split):
        return buf.at[o, :, spans[u]] if split else buf.at[o, u]

    def to_mate(o, u, split):
        i = (o // (2 * per)) * per + lax.rem(o, per)
        return rdma(
            unit(part, o, u, split), unit(mated, o, u, split), mate_send.at[0], mate_recv.at[i, u], me, mate
        )

    def to_owner(o, u, split):
        i = lax.rem(o, per)
        return rdma(
            unit(part, o, u, split), unit(landed, i, u, split), part_send.at[0], part_recv.at[i, u], me, across
        )

    final = origin[n - 1]
    holder = final // per

    def to_echo(h):
        return rdma(part.at[final, h], echo.at[h], echo_send.at[0], echo_recv.at[h], me, across)

    def to_late():
        return rdma(late, late, late_send.at[0], late_recv.at[0], me, mate)

    pieces = [(0, 0), (0, 1)]
    for k in range(1, count - 2, 2):
        d, h = k // QUARTERS, (k % QUARTERS) // 2
        pieces += [(2 * d + 1, h), (2 * d + 2, h)]
    pieces += [(n - 1, 0), (n - 1, 1)]

    def emit(places, span, split):
        side = jnp.concatenate([wout[origin[i], h].reshape(qc + cc, half) for i, h in places], axis=1)
        got = jnp.dot(hidden[span, :], side, preferred_element_type=f32).astype(bf16)
        for j, (i, h) in enumerate(places):
            part[origin[i], h, span] = got[:, j * half : (j + 1) * half]
        sent = [(i, spans.index(span)) for i, h in places if h == 0] if split else places
        for i, u in sent:
            o = origin[i]

            @pl.when(lax.rem(o // per, 2) != lax.rem(t, 2))
            def _(o=o, u=u):
                to_mate(o, u, split).start()

    def emit_near(u):
        emit([(i, h) for i in range(near) for h in range(2)], spans[u], True)

    def emit_far(ids):
        emit([pieces[i] for i in ids], pl.ds(0, rows), False)

    def combine(i, u, split):
        o = origin[i]
        where = (slice(None), spans[u]) if split else (u,)

        @pl.when(o // per == t)
        def _():
            to_mate(o, u, split).wait_recv()
            both = part[(o,) + where].astype(f32) + mated[(o,) + where].astype(f32)
            own[(lax.rem(o, per),) + where] = both
            if i == n - 1:
                part[(o,) + where] = both.astype(bf16)
                to_echo(u).start()

        @pl.when(o // per == across)
        def _():
            to_mate(o, u, split).wait_recv()
            both = part[(o,) + where].astype(f32) + mated[(o,) + where].astype(f32)
            part[(o,) + where] = both.astype(bf16)
            to_owner(o, u, split).start()

    def combine_near(u):
        for i in range(near):
            combine(i, u, True)

    def combine_far(ids):
        for i in ids:
            combine(pieces[i][0], pieces[i][1], False)

    def pack(one, two):
        one = jnp.sum(one, axis=1, keepdims=True)
        two = jnp.sum(two, axis=1, keepdims=True)
        lane = lax.broadcasted_iota(jnp.int32, (rows, 128), 1)
        return jnp.transpose(jnp.where(lane == 0, one, jnp.where(lane == 1, two, 0.0)))[0:8]

    sums[...] = jnp.zeros_like(sums)
    emits = {5: (6, 8), 7: (8, 10), 9: (10, 12), 11: (12, 14), 12: (14, 15), 13: (15, 16)}
    odd = lax.rem(t, 2) == 1
    ahead = {6: (6, 8), 7: (8, 10), 9: (10, 12), 11: (12, 14), 12: (14, 15), 13: (15, 16)}
    behind = {7: (6, 8), 8: (8, 10), 10: (10, 12), 13: (12, 16)}

    def on(core, work, *args):
        @pl.when(odd == core)
        def _():
            work(*args)

    for k in range(count):
        relay(w_out, k)
        if k < 2:
            for b in order[: blocks - 2][k::2]:
                attend(b)
        elif k == 2:
            pool_inner()
        elif k == 3:
            emit_near(0)
            for c in rims:
                c.wait()
            attend(0)
            on(False, combine_near, 0)
        elif k == 4:
            attend(blocks - 1)
            on(True, combine_near, 0)
            pool_edges()
            emit_near(1)
        if k in emits:
            emit_far(range(*emits[k]))
        if k == 5:
            on(False, combine_near, 1)
        elif k == 6:
            on(True, combine_near, 1)
        if k in ahead:
            on(False, combine_far, range(*ahead[k]))
        if k in behind:
            on(True, combine_far, range(*behind[k]))

    def stat_copy(j):
        return rdma(stats.at[t], stats.at[t], stat_send.at[0], stat_recv.at[t], me, lax.rem(t + j, tp))

    for i in range(n - 1):
        o = origin[i]

        @pl.when(o // per == t)
        def _(o=o, i=i):
            for u in range(2):
                to_owner(o, u, i < near).wait_recv()

    for i in range(per):
        o = t * per + i

        @pl.when(o != final)
        def _(o=o, i=i):
            one = two = 0.0
            for h in range(2):
                mix = own[i, h] + landed[i, h].astype(f32)
                acc[:, (2 * i + h) * half : (2 * i + h + 1) * half] = mix
                one, two = one + mix, two + mix * mix
            sums[0] += one
            sums[1] += two

    stats[t] = pack(sums[0], sums[1])
    for j in range(1, tp):
        stat_copy(j).start()

    @pl.when(holder == t)
    def _():
        one = two = 0.0
        for h in range(2):
            i = lax.rem(final, per)
            to_owner(final, h, False).wait_recv()
            mix = own[i, h] + landed[i, h].astype(f32)
            acc[:, pl.ds(pl.multiple_of((2 * i + h) * half, 128), half)] = mix
            one, two = one + mix, two + mix * mix
        late[...] = pack(one, two)
        to_late().start()

    @pl.when(holder == across)
    def _():
        one = two = 0.0
        for h in range(2):
            to_echo(h).wait_recv()
            mix = part[final, h].astype(f32) + echo[h].astype(f32)
            one, two = one + mix, two + mix * mix
        late[...] = pack(one, two)
        to_late().start()

    def drain(buf, amount, sem):
        whole = buf.at[pl.ds(0, amount)]
        rdma(whole, whole, sem.at[0], mate_recv.at[0, 0], me, mate).wait_send()

    drain(part, n // 2, mate_send)
    drain(part, per, part_send)
    drain(tok, 3 * per, tok_send)

    @pl.when(holder == t)
    def _():
        drain(part, 1, echo_send)

    for turn in range(2 * count - SENDS, 2 * count):
        for way in range(2):
            launched(way, turn).wait_send()
    for j in range(1, tp):
        src = lax.rem(t + j, tp)
        rdma(stats.at[src], stats.at[src], stat_send.at[0], stat_recv.at[src], me, src).wait_recv()
    paired = lax.rem(holder, 2) == lax.rem(t, 2)

    @pl.when(jnp.logical_not(paired))
    def _():
        to_late().wait_recv()

    totals = late[...] + stats[0]
    for i in range(1, tp):
        totals = totals + stats[i]
    tall = jnp.concatenate([totals, jnp.zeros((120, rows), f32)], axis=0)
    back = jnp.transpose(tall)
    width = gain_ref.shape[1] * tp
    row_mean = back[:, 0:1] / width
    variance = back[:, 1:2] / width - row_mean * row_mean
    scale = lax.rsqrt(variance + epsilon)
    normed = ((acc[:, 0 : gain_ref.shape[1]] - row_mean) * scale * gains[...]).astype(bf16)
    for b in range(blocks):
        out_ref[b * WINDOW : (b + 1) * WINDOW, :] = normed[place(b) : place(b) + WINDOW]
    drain(stats, tp - 1, stat_send)

    @pl.when(paired)
    def _():
        to_late().wait_send()


def fused(n, tp, tokens, w_query, w_key, w_value, w_pool_in, sink, w_pool, pool_scale, w_out_attn, w_out_pool, out_gain):
    rows, share = tokens.shape
    depth, qc = w_query.shape
    kc, cc = w_key.shape[1], w_pool_in.shape[1]
    wide = w_out_attn.shape[1]
    half = wide // 2
    per = n // tp
    count = QUARTERS * (n - 1) // 2
    bf16, f32 = jnp.bfloat16, jnp.float32
    dma = pltpu.SemaphoreType.DMA
    return pl.pallas_call(
        functools.partial(mixer_kernel, n, tp),
        out_shape=jax.ShapeDtypeStruct((rows, share), bf16),
        in_specs=[pl.BlockSpec(memory_space=pltpu.HBM)] * 11,
        out_specs=pl.BlockSpec(memory_space=pltpu.VMEM),
        scratch_shapes=[
            pltpu.VMEM((n, QUARTERS, depth // QUARTERS, qc + 2 * kc + cc), bf16),
            pltpu.VMEM((n, 2, 2, qc, half), bf16),
            pltpu.VMEM((n, rows, depth), bf16),
            pltpu.VMEM((rows, qc + 2 * kc + cc), f32),
            pltpu.VMEM((rows, qc), bf16),
            pltpu.VMEM((rows + 2 * WINDOW, 2 * kc), bf16),
            pltpu.VMEM((rows + 2 * RIM, cc), bf16),
            pltpu.VMEM((rows, qc + cc), bf16),
            pltpu.VMEM((n, 2, rows, half), bf16),
            pltpu.VMEM((n, 2, rows, half), bf16),
            pltpu.VMEM((per, 2, rows, half), bf16),
            pltpu.VMEM((per, 2, rows, half), f32),
            pltpu.VMEM((tp, 8, rows), f32),
            pltpu.VMEM((8, rows), f32),
            pltpu.VMEM((2, rows, half), bf16),
            pltpu.VMEM((2, rows, half), f32),
            pltpu.VMEM((2 * kc, depth), bf16),
            pltpu.VMEM((1, sink.shape[0]), f32),
            pltpu.VMEM(w_pool.shape, bf16),
            pltpu.VMEM((1, cc), f32),
            pltpu.VMEM((1, share), f32),
            dma((2, SENDS)),
            dma((2, RECVS)),
            dma((1,)),
            dma((3 * per,)),
            dma((4,)),
            dma((4,)),
            dma((1,)),
            dma((n // 2, 2)),
            dma((1,)),
            dma((per, 2)),
            dma((1,)),
            dma((2,)),
            dma((per + 12,)),
            dma((1,)),
            dma((tp,)),
            dma((1,)),
            dma((1,)),
        ],
        compiler_params=pltpu.CompilerParams(
            collective_id=0, has_side_effects=True, vmem_limit_bytes=32 * 1024 * 1024
        ),
        name="mixer",
    )(
        pltpu.with_memory_space_constraint(tokens, pltpu.HBM),
        pltpu.with_memory_space_constraint(w_query.reshape(QUARTERS, -1, qc), pltpu.HBM),
        pltpu.with_memory_space_constraint(w_key.T, pltpu.HBM),
        pltpu.with_memory_space_constraint(w_value.T, pltpu.HBM),
        pltpu.with_memory_space_constraint(w_pool_in.reshape(QUARTERS, -1, cc), pltpu.HBM),
        pltpu.with_memory_space_constraint(sink.reshape(1, -1), pltpu.HBM),
        pltpu.with_memory_space_constraint(w_pool, pltpu.HBM),
        pltpu.with_memory_space_constraint(pool_scale.reshape(1, -1), pltpu.HBM),
        pltpu.with_memory_space_constraint(w_out_attn, pltpu.HBM),
        pltpu.with_memory_space_constraint(w_out_pool, pltpu.HBM),
        pltpu.with_memory_space_constraint(out_gain.reshape(1, -1), pltpu.HBM),
    )


def fits(n, tp, tokens, w_query, w_key, w_pool, w_out_attn):
    return (
        tp == 4
        and n == 2 * tp
        and w_query.shape[0] % 64 == 0
        and w_query.shape[1] % 128 == 0
        and w_key.shape[1] == HEAD_DIM
        and w_pool.shape[0] == 1
        and w_out_attn.shape[1] % 256 == 0
        and w_out_attn.shape[0] == w_query.shape[1]
        and tokens.shape[0] >= 3 * WINDOW
    )


def mixed_rows(*args):
    n, tp = lax.axis_size("sp"), lax.axis_size("tp")
    if fits(n, tp, args[0], args[1], args[2], args[6], args[8]):
        return fused(n, tp, *args)
    return local(*args)


def solution(mesh):
    return jax.shard_map(
        mixed_rows,
        mesh=mesh,
        in_specs=(
            P("sp", "tp"),
            P("sp", "tp"),
            P("sp", "tp"),
            P("sp", "tp"),
            P("sp", "tp"),
            P("tp"),
            P("tp", None, None),
            P("tp"),
            P("tp", "sp"),
            P("tp", "sp"),
            P("tp"),
        ),
        out_specs=P("sp", "tp"),
        check_vma=False,
    )
```

```python
import functools

import jax
import jax.numpy as jnp
from jax import lax
from jax.experimental import pallas as pl
from jax.experimental.pallas import tpu as pltpu
from jax.sharding import PartitionSpec as P

HEAD_DIM = 64
POOL_GROUPS = 4
WINDOW = 128


epsilon = 1e-05
masked_score = -1e30


def padded(cells, sides, width):
    for axis, dim in sides:
        count = lax.axis_size(axis)
        ends = count - 1
        head = lax.slice_in_dim(cells, 0, width, axis=dim)
        tail = lax.slice_in_dim(cells, cells.shape[dim] - width, cells.shape[dim], axis=dim)
        cells = jnp.concatenate(
            [
                lax.ppermute(tail, axis, [(i, (i + 1) % count) for i in range(ends)]),
                cells,
                lax.ppermute(head, axis, [((i + 1) % count, i) for i in range(ends)]),
            ],
            axis=dim,
        )
    return cells


def make_projector(gathered, pieces):
    piece_query, piece_key, piece_value, piece_chan = pieces
    joined = jnp.concatenate([piece_key, piece_value], axis=1)
    return (
        jnp.dot(gathered, piece_query, preferred_element_type=jnp.float32),
        jnp.dot(gathered, joined, preferred_element_type=jnp.float32),
        jnp.dot(gathered, piece_chan, preferred_element_type=jnp.float32),
    )


def attend_local(query, keys_ext, sinks, offset, seq_len, key_cols):
    tok_rows, query_cols = query.shape
    kv_local = key_cols // HEAD_DIM
    group = query_cols // key_cols
    block_count = tok_rows // WINDOW
    stacked = keys_ext.reshape(block_count + 2, WINDOW, 2 * key_cols)
    banded = jnp.concatenate([stacked[:-2], stacked[1:-1], stacked[2:]], axis=1)
    key_band = banded[:, :, :key_cols].reshape(block_count, 3 * WINDOW, kv_local, HEAD_DIM)
    value_band = banded[:, :, key_cols:].reshape(block_count, 3 * WINDOW, kv_local, HEAD_DIM)
    query_blocks = query.reshape(block_count, WINDOW, kv_local, group, HEAD_DIM)
    scores = jnp.einsum(
        "nqkgd,nskd->nkgqs", query_blocks, key_band, preferred_element_type=jnp.float32
    ) * HEAD_DIM ** (-0.5)
    starts = offset + jnp.arange(block_count, dtype=jnp.int32) * WINDOW
    query_pos = starts[:, None] + jnp.arange(WINDOW, dtype=jnp.int32)[None, :]
    key_pos = starts[:, None] + jnp.arange(3 * WINDOW, dtype=jnp.int32)[None, :] - WINDOW
    distance = key_pos[:, None, :] - query_pos[:, :, None]
    inside = (key_pos >= 0) & (key_pos < seq_len)
    keep = (jnp.abs(distance) <= WINDOW) & inside[:, None, :]
    scores = jnp.where(keep[:, None, None], scores, masked_score)
    sink_logit = sinks.reshape(kv_local, group)[None, :, :, None, None]
    top = jnp.maximum(jnp.max(scores, axis=-1, keepdims=True), sink_logit)
    raised = jnp.exp(scores - top)
    total = jnp.sum(raised, axis=-1, keepdims=True) + jnp.exp(sink_logit - top)
    probs = (raised / total).astype(jnp.bfloat16)
    attended = jnp.einsum(
        "nkgqs,nskd->nqkgd", probs, value_band, preferred_element_type=jnp.float32
    )
    return attended.astype(jnp.bfloat16).reshape(tok_rows, query_cols)


def local(
    tokens,
    w_query,
    w_key,
    w_value,
    w_pool_in,
    sink,
    w_pool,
    pool_scale,
    w_out_attn,
    w_out_pool,
    out_gain,
):
    tok_rows = tokens.shape[0]
    seq_len = tok_rows * lax.axis_size("sp")
    offset = lax.axis_index("sp") * tok_rows
    out_both = jnp.concatenate([w_out_attn, w_out_pool], axis=0)
    gathered = lax.all_gather(tokens, "tp", axis=1, tiled=True)
    key_cols = w_key.shape[1]
    chan_cols = w_pool_in.shape[1]
    query_sum, joined_sum, chan_sum = make_projector(
        gathered,
        (
            lax.all_gather(w_query, "sp", axis=0, tiled=True),
            lax.all_gather(w_key, "sp", axis=0, tiled=True),
            lax.all_gather(w_value, "sp", axis=0, tiled=True),
            lax.all_gather(w_pool_in, "sp", axis=0, tiled=True),
        ),
    )
    query = query_sum.astype(jnp.bfloat16)
    key_value = joined_sum.astype(jnp.bfloat16)
    chan = chan_sum.astype(jnp.bfloat16)
    keys_ext = padded(key_value, (("sp", 0),), WINDOW)
    attended = attend_local(query, keys_ext, sink, offset, seq_len, key_cols)
    rim_rows = 2 ** (POOL_GROUPS - 1)
    chan_ext = padded(chan, (("sp", 0),), rim_rows)
    running = jnp.concatenate(
        [jnp.zeros((1, chan_cols), jnp.float32), jnp.cumsum(chan_ext.astype(jnp.float32), axis=0)],
        axis=0,
    )
    chan_float = chan.astype(jnp.float32)
    positions = offset + jnp.arange(tok_rows, dtype=jnp.int32)
    group_count = w_pool.shape[0]
    level = lax.axis_index("tp") * group_count + 0
    half = jnp.left_shift(jnp.int32(1), level)
    upper = lax.dynamic_slice_in_dim(running, rim_rows + half, tok_rows, 0)
    lower = lax.dynamic_slice_in_dim(running, rim_rows - half, tok_rows, 0)
    count = (
        jnp.clip(positions + half, 0, seq_len) - jnp.clip(positions - half, 0, seq_len)
    ).astype(jnp.float32)
    spread = ((upper - lower) / count[:, None] - chan_float).astype(jnp.bfloat16)
    outputs = jnp.dot(spread, w_pool[0], preferred_element_type=jnp.float32)
    pooled = (outputs * pool_scale).astype(jnp.bfloat16)
    hidden = jnp.concatenate([attended, pooled], axis=1)
    terms = jnp.dot(
        hidden,
        lax.all_gather(out_both, "sp", axis=1, tiled=True),
        preferred_element_type=jnp.float32,
    )
    share_width = out_gain.shape[0]
    model_width = share_width * lax.axis_size("tp")
    share = lax.psum_scatter(
        terms.astype(jnp.bfloat16), "tp", scatter_dimension=1, tiled=True
    ).astype(jnp.float32)
    row_total, row_square = lax.psum((jnp.sum(share, axis=1), jnp.sum(share * share, axis=1)), "tp")
    row_mean = row_total / model_width
    variance = row_square / model_width - row_mean * row_mean
    normed = (share - row_mean[:, None]) * lax.rsqrt(variance + epsilon)[:, None] * out_gain
    return normed.astype(jnp.bfloat16)


MESH = pl.DeviceIdType.MESH
RIM = 16
QUARTERS = 4
SENDS = 6
RECVS = 10


def mixer_kernel(
    n,
    tp,
    tok_ref,
    wq_ref,
    wk_ref,
    wv_ref,
    wc_ref,
    sink_ref,
    wp_ref,
    ps_ref,
    woa_ref,
    wop_ref,
    gain_ref,
    out_ref,
    win,
    wout,
    tok,
    acc,
    query,
    kv,
    chan,
    hidden,
    part,
    mated,
    landed,
    own,
    stats,
    late,
    echo,
    sums,
    pair_in,
    sinks,
    wpool,
    scales,
    gains,
    ring_send,
    ring_recv,
    tok_send,
    tok_recv,
    rim_send,
    rim_recv,
    mate_send,
    mate_recv,
    part_send,
    part_recv,
    echo_send,
    echo_recv,
    load,
    stat_send,
    stat_recv,
    late_send,
    late_recv,
):
    f32, bf16 = jnp.float32, jnp.bfloat16
    me, t = lax.axis_index("sp"), lax.axis_index("tp")
    rows = tok_ref.shape[0]
    seq_len = rows * n
    half_n = n // 2
    column = me % 2
    pos = (me // 2) * (1 - column) + column * (n - 1 - me // 2)

    def at(p):
        p = lax.rem(p + n, n)
        back = p // half_n
        return (1 - back) * (2 * p) + back * (2 * (n - 1 - p) + 1)

    ring = (at(pos + 1), at(pos - 1))
    after, before = lax.rem(me + 1, n), lax.rem(me + n - 1, n)
    mate = t + 1 - 2 * lax.rem(t, 2)
    across = lax.rem(t + 2, tp)
    per = n // tp

    def rdma(src, dst, send, recv, sp, tpi):
        return pltpu.make_async_remote_copy(
            src_ref=src,
            dst_ref=dst,
            send_sem=send,
            recv_sem=recv,
            device_id={"sp": sp, "tp": tpi},
            device_id_type=MESH,
        )

    qc, kc = wq_ref.shape[2], wk_ref.shape[0]
    cc = wc_ref.shape[2]
    depth = QUARTERS * wq_ref.shape[1]
    quarter = depth // QUARTERS
    wide = woa_ref.shape[1]
    half = wide // 2
    barrier = pltpu.get_barrier_semaphore()
    peers = [(s, t) for s in ring]
    peers += [(me, mate), (me, across)]
    for s, p in peers:
        pl.semaphore_signal(barrier, inc=1, device_id={"sp": s, "tp": p}, device_id_type=MESH)

    loads = []

    def fetch(src, dst):
        copy = pltpu.make_async_copy(src, dst, load.at[len(loads)])
        copy.start()
        loads.append(copy)
        return copy

    pairs = [fetch(wk_ref, pair_in.at[pl.ds(0, kc)]), fetch(wv_ref, pair_in.at[pl.ds(kc, kc)])]
    first = [
        fetch(wq_ref, win.at[me, :, :, pl.ds(0, qc)]),
        fetch(wc_ref, win.at[me, :, :, pl.ds(qc + 2 * kc, cc)]),
    ]
    own_tok = [fetch(tok_ref.at[:, pl.ds(b * depth, depth)], tok.at[t * per + b]) for b in range(per)]
    later = []
    for h in range(2):
        later.append(fetch(woa_ref.at[:, pl.ds(h * half, half)], wout.at[me, h, 0]))
        later.append(fetch(wop_ref.at[:, pl.ds(h * half, half)], wout.at[me, h, 1]))
    later.append(fetch(sink_ref, sinks))
    later.append(fetch(wp_ref, wpool))
    later.append(fetch(ps_ref, scales))
    later.append(fetch(gain_ref, gains))
    for copy in pairs:
        copy.wait()
    pair = jnp.transpose(pair_in[...].astype(f32)).astype(bf16)
    for h in range(QUARTERS):
        win[me, h, :, qc : qc + 2 * kc] = pair[h * quarter : (h + 1) * quarter]
    for copy in first:
        copy.wait()
    pl.semaphore_wait(barrier, len(peers))

    count = QUARTERS * (n - 1) // 2
    last = count - 1

    def ring_copy(buf, way, k, hop, turn):
        sign = -1 if way == 0 else 1
        q = k % QUARTERS
        o = at(pos + sign * (k // QUARTERS + hop))
        if buf is win:
            slot = buf.at[o, q if way == 0 else QUARTERS - 1 - q]
        elif k >= last - 1:
            slot = buf.at[o, q, way]
        else:
            slot = buf.at[o, q // 2, (q + way) % 2]
        return rdma(slot, slot, ring_send.at[way, turn % SENDS], ring_recv.at[way, turn % RECVS], ring[way], t)

    def w_in(way, k, hop):
        return ring_copy(win, way, k, hop, k)

    def w_out(way, k, hop):
        return ring_copy(wout, way, k, hop, count + k)

    def launched(way, turn):
        return w_in(way, turn, 0) if turn < count else w_out(way, turn - count, 0)

    def launch(way, turn):
        if turn >= SENDS:
            launched(way, turn - SENDS).wait_send()
        launched(way, turn).start()

    def tok_copy(owner, b, i, dst):
        slot = tok.at[owner * per + b]
        return rdma(slot, slot, tok_send.at[0], tok_recv.at[i], me, dst)

    for k in range(QUARTERS):
        for way in range(2):
            launch(way, k)
    for copy in own_tok:
        copy.wait()
    for b in range(per):
        tok_copy(t, b, b, across).start()
    for b in range(per):
        tok_copy(t, b, per + b, mate).start()

    for copy in later:
        copy.wait()

    origin = [at(pos)]
    for d in range(1, half_n):
        origin += [at(pos - d), at(pos + d)]
    origin.append(at(pos + half_n))

    def project(i, first=False):
        o = origin[i]
        w = win[o].reshape(depth, qc + 2 * kc + cc)
        term = jnp.dot(tok[o], w, preferred_element_type=f32)
        if first:
            acc[...] = term
        else:
            acc[...] += term

    def relay(copy, k):
        for way in range(2):
            copy(way, k, 1).wait_recv()
            if copy is w_in:
                if k + QUARTERS <= last:
                    launch(way, k + QUARTERS)
            elif k + QUARTERS < last:
                launch(way, count + k + QUARTERS)
            elif k == last - 3:
                launch(way, count + last)

    def start_out(k):
        for way in range(2):
            launch(way, count + k)

    done_blocks = 0
    for k in range(count):
        relay(w_in, k)
        if last - 3 <= k < last:
            start_out(k - (last - 3))
        if k in (3, 6):
            b = 0 if k == 3 else 1
            tok_copy(across, b, b, across).wait_recv()
            tok_copy(across, b, 2 * per + b, mate).start()
        if k == 8:
            for b in range(per):
                tok_copy(mate, b, per + b, mate).wait_recv()
                tok_copy(lax.rem(mate + 2, tp), b, 2 * per + b, mate).wait_recv()
        if k >= 8:
            ready = n if k == last else 1 + 2 * ((k + 1) // QUARTERS)
            upto = ready if k == last else min(ready, done_blocks + 2)
            while done_blocks < upto:
                project(done_blocks, done_blocks == 0)
                done_blocks += 1

    kv[WINDOW : WINDOW + rows, :] = acc[:, qc : qc + 2 * kc].astype(bf16)
    chan[RIM : RIM + rows, :] = acc[:, qc + 2 * kc :].astype(bf16)

    def rim(buf, width, down, i):
        if down:
            return rdma(buf.at[pl.ds(rows, width)], buf.at[pl.ds(0, width)], rim_send.at[i], rim_recv.at[i], after, t)
        return rdma(
            buf.at[pl.ds(width, width)], buf.at[pl.ds(rows + width, width)], rim_send.at[i], rim_recv.at[i], before, t
        )

    rims = [rim(kv, WINDOW, True, 0), rim(kv, WINDOW, False, 1), rim(chan, RIM, True, 2), rim(chan, RIM, False, 3)]
    for c in rims:
        c.start()
    start_out(3)
    query[...] = acc[:, 0:qc].astype(bf16)

    group = qc // kc

    def attend(b):
        band = kv[b * WINDOW : (b + 3) * WINDOW, :]
        q = query[b * WINDOW : (b + 1) * WINDOW, :]
        stacked = jnp.concatenate([q[:, g * HEAD_DIM : (g + 1) * HEAD_DIM] for g in range(group)], axis=0)
        scores = lax.dot_general(
            stacked, band[:, :HEAD_DIM], (((1,), (1,)), ((), ())), preferred_element_type=f32
        ) * HEAD_DIM ** (-0.5)
        scores = scores.reshape(group, WINDOW, 3 * WINDOW)
        r = lax.broadcasted_iota(jnp.int32, (WINDOW, 3 * WINDOW), 0)
        c = lax.broadcasted_iota(jnp.int32, (WINDOW, 3 * WINDOW), 1)
        keep = (c >= r) & (c <= r + 2 * WINDOW)
        key_pos = c + (me * rows + b * WINDOW - WINDOW)
        keep = keep & (key_pos >= 0) & (key_pos < seq_len)
        outs = []
        for g in range(group):
            s = jnp.where(keep, scores[g], masked_score)
            logit = sinks[0:1, g : g + 1]
            top = jnp.maximum(jnp.max(s, axis=1, keepdims=True), logit)
            raised = jnp.exp(s - top)
            total = jnp.sum(raised, axis=1, keepdims=True) + jnp.exp(logit - top)
            outs.append((raised * (1.0 / total)).astype(bf16))
        got = jnp.dot(jnp.concatenate(outs, axis=0), band, preferred_element_type=f32)
        got = got[:, HEAD_DIM : 2 * HEAD_DIM].astype(bf16)
        hidden[place(b) : place(b) + WINDOW, 0:qc] = jnp.concatenate(
            [got[g * WINDOW : (g + 1) * WINDOW] for g in range(group)], axis=1
        )

    blocks = rows // WINDOW
    order = list(range(1, blocks - 1)) + [0, blocks - 1]
    early = (blocks - 2) * WINDOW

    def place(b):
        return order.index(b) * WINDOW

    half_width = 1
    for level in range(1, POOL_GROUPS):
        half_width = jnp.where(t == level, 2**level, half_width)

    def spread_of(start, size):
        length = size + 2 * RIM
        e = chan[start : start + length].astype(f32)
        p = lax.broadcasted_iota(jnp.int32, (length, 1), 0) + (me * rows + start - RIM)
        e = jnp.where((p >= 0) & (p < seq_len), e, 0.0)
        total = e + pltpu.roll(e, 1, 0)
        pick = total
        for level in range(1, POOL_GROUPS):
            step = 2 ** (level - 1)
            total = pltpu.roll(total, step, 0) + pltpu.roll(total, length - step, 0)
            pick = jnp.where(t == level, total, pick)
        number = (jnp.clip(p + half_width, 0, seq_len) - jnp.clip(p - half_width, 0, seq_len)).astype(f32)
        return (pick[RIM : RIM + size] / number[RIM : RIM + size] - e[RIM : RIM + size]).astype(bf16)

    def pooled_of(spread):
        return (jnp.dot(spread, wpool[0], preferred_element_type=f32) * scales[...]).astype(bf16)

    def pool_inner():
        got = pooled_of(spread_of(RIM, rows - 2 * RIM))
        for b in range(blocks):
            low, high = max(b * WINDOW, RIM), min((b + 1) * WINDOW, rows - RIM)
            base = place(b) - b * WINDOW
            hidden[base + low : base + high, qc:] = got[low - RIM : high - RIM]

    def pool_edges():
        got = pooled_of(jnp.concatenate([spread_of(0, RIM), spread_of(rows - RIM, RIM)], axis=0))
        hidden[place(0) : place(0) + RIM, qc:] = got[0:RIM]
        end = place(blocks - 1) + WINDOW
        hidden[end - RIM : end, qc:] = got[RIM:]

    near = 3
    spans = (pl.ds(0, early), pl.ds(early, rows - early))

    def unit(buf, o, u, split):
        return buf.at[o, :, spans[u]] if split else buf.at[o, u]

    def to_mate(o, u, split):
        i = (o // (2 * per)) * per + lax.rem(o, per)
        return rdma(
            unit(part, o, u, split), unit(mated, o, u, split), mate_send.at[0], mate_recv.at[i, u], me, mate
        )

    def to_owner(o, u, split):
        i = lax.rem(o, per)
        return rdma(
            unit(part, o, u, split), unit(landed, i, u, split), part_send.at[0], part_recv.at[i, u], me, across
        )

    final = origin[n - 1]
    holder = final // per

    def to_echo(h):
        return rdma(part.at[final, h], echo.at[h], echo_send.at[0], echo_recv.at[h], me, across)

    def to_late():
        return rdma(late, late, late_send.at[0], late_recv.at[0], me, mate)

    pieces = [(0, 0), (0, 1)]
    for k in range(1, count - 2, 2):
        d, h = k // QUARTERS, (k % QUARTERS) // 2
        pieces += [(2 * d + 1, h), (2 * d + 2, h)]
    pieces += [(n - 1, 0), (n - 1, 1)]

    def emit(places, span, split):
        side = jnp.concatenate([wout[origin[i], h].reshape(qc + cc, half) for i, h in places], axis=1)
        got = jnp.dot(hidden[span, :], side, preferred_element_type=f32).astype(bf16)
        for j, (i, h) in enumerate(places):
            part[origin[i], h, span] = got[:, j * half : (j + 1) * half]
        sent = [(i, spans.index(span)) for i, h in places if h == 0] if split else places
        for i, u in sent:
            o = origin[i]

            @pl.when(lax.rem(o // per, 2) != lax.rem(t, 2))
            def _(o=o, u=u):
                to_mate(o, u, split).start()

    def emit_near(u):
        emit([(i, h) for i in range(near) for h in range(2)], spans[u], True)

    def emit_far(ids):
        emit([pieces[i] for i in ids], pl.ds(0, rows), False)

    def combine(i, u, split):
        o = origin[i]
        where = (slice(None), spans[u]) if split else (u,)

        @pl.when(o // per == t)
        def _():
            to_mate(o, u, split).wait_recv()
            both = part[(o,) + where].astype(f32) + mated[(o,) + where].astype(f32)
            own[(lax.rem(o, per),) + where] = both
            if i == n - 1:
                part[(o,) + where] = both.astype(bf16)
                to_echo(u).start()

        @pl.when(o // per == across)
        def _():
            to_mate(o, u, split).wait_recv()
            both = part[(o,) + where].astype(f32) + mated[(o,) + where].astype(f32)
            part[(o,) + where] = both.astype(bf16)
            to_owner(o, u, split).start()

    def combine_near(u):
        for i in range(near):
            combine(i, u, True)

    def combine_far(ids):
        for i in ids:
            combine(pieces[i][0], pieces[i][1], False)

    def pack(one, two):
        one = jnp.sum(jnp.transpose(one), axis=0, keepdims=True)
        two = jnp.sum(jnp.transpose(two), axis=0, keepdims=True)
        return jnp.concatenate([one, two, jnp.zeros((6, rows), f32)], axis=0)

    sums[...] = jnp.zeros_like(sums)
    emits = {5: (6, 8), 7: (8, 10), 9: (10, 12), 11: (12, 14), 12: (14, 15), 13: (15, 16)}
    odd = lax.rem(t, 2) == 1
    ahead = {6: (6, 8), 7: (8, 10), 9: (10, 12), 11: (12, 14), 12: (14, 15), 13: (15, 16)}
    behind = {7: (6, 8), 8: (8, 10), 10: (10, 12), 12: (12, 14), 13: (14, 16)}

    def on(core, work, *args):
        @pl.when(odd == core)
        def _():
            work(*args)

    for k in range(count):
        relay(w_out, k)
        if k < 2:
            for b in order[: blocks - 2][k::2]:
                attend(b)
        elif k == 2:
            pool_inner()
        elif k == 3:
            emit_near(0)
            for c in rims:
                c.wait()
            attend(0)
            on(False, combine_near, 0)
        elif k == 4:
            attend(blocks - 1)
            on(True, combine_near, 0)
            pool_edges()
            emit_near(1)
        if k in emits:
            emit_far(range(*emits[k]))
        if k == 5:
            on(False, combine_near, 1)
        elif k == 6:
            on(True, combine_near, 1)
        if k in ahead:
            on(False, combine_far, range(*ahead[k]))
        if k in behind:
            on(True, combine_far, range(*behind[k]))

    def stat_copy(j):
        return rdma(stats.at[t], stats.at[t], stat_send.at[0], stat_recv.at[t], me, lax.rem(t + j, tp))

    for i in range(n - 1):
        o = origin[i]

        @pl.when(o // per == t)
        def _(o=o, i=i):
            for u in range(2):
                to_owner(o, u, i < near).wait_recv()

    for i in range(per):
        o = t * per + i

        @pl.when(o != final)
        def _(o=o, i=i):
            one = two = 0.0
            for h in range(2):
                mix = own[i, h] + landed[i, h].astype(f32)
                acc[:, (2 * i + h) * half : (2 * i + h + 1) * half] = mix
                one, two = one + mix, two + mix * mix
            sums[0] += one
            sums[1] += two

    stats[t] = pack(sums[0], sums[1])
    for j in range(1, tp):
        stat_copy(j).start()

    @pl.when(holder == t)
    def _():
        one = two = 0.0
        for h in range(2):
            i = lax.rem(final, per)
            to_owner(final, h, False).wait_recv()
            mix = own[i, h] + landed[i, h].astype(f32)
            acc[:, pl.ds(pl.multiple_of((2 * i + h) * half, 128), half)] = mix
            one, two = one + mix, two + mix * mix
        late[...] = pack(one, two)
        to_late().start()

    @pl.when(holder == across)
    def _():
        one = two = 0.0
        for h in range(2):
            to_echo(h).wait_recv()
            mix = part[final, h].astype(f32) + echo[h].astype(f32)
            one, two = one + mix, two + mix * mix
        late[...] = pack(one, two)
        to_late().start()

    def drain(buf, amount, sem):
        whole = buf.at[pl.ds(0, amount)]
        rdma(whole, whole, sem.at[0], mate_recv.at[0, 0], me, mate).wait_send()

    drain(part, n // 2, mate_send)
    drain(part, per, part_send)
    drain(tok, 3 * per, tok_send)

    @pl.when(holder == t)
    def _():
        drain(part, 1, echo_send)

    for turn in range(2 * count - SENDS, 2 * count):
        for way in range(2):
            launched(way, turn).wait_send()
    for j in range(1, tp):
        src = lax.rem(t + j, tp)
        rdma(stats.at[src], stats.at[src], stat_send.at[0], stat_recv.at[src], me, src).wait_recv()
    paired = lax.rem(holder, 2) == lax.rem(t, 2)

    @pl.when(jnp.logical_not(paired))
    def _():
        to_late().wait_recv()

    totals = late[...] + stats[0]
    for i in range(1, tp):
        totals = totals + stats[i]
    width = gain_ref.shape[1] * tp
    line_mean = totals[0:1] / width
    line_scale = lax.rsqrt(totals[1:2] / width - line_mean * line_mean + epsilon)
    tall = jnp.concatenate([line_mean, line_scale, jnp.zeros((126, rows), f32)], axis=0)
    back = jnp.transpose(tall)
    row_mean, scale = back[:, 0:1], back[:, 1:2]
    normed = ((acc[:, 0 : gain_ref.shape[1]] - row_mean) * scale * gains[...]).astype(bf16)
    for b in range(blocks):
        out_ref[b * WINDOW : (b + 1) * WINDOW, :] = normed[place(b) : place(b) + WINDOW]
    drain(stats, tp - 1, stat_send)

    @pl.when(paired)
    def _():
        to_late().wait_send()


def fused(n, tp, tokens, w_query, w_key, w_value, w_pool_in, sink, w_pool, pool_scale, w_out_attn, w_out_pool, out_gain):
    rows, share = tokens.shape
    depth, qc = w_query.shape
    kc, cc = w_key.shape[1], w_pool_in.shape[1]
    wide = w_out_attn.shape[1]
    half = wide // 2
    per = n // tp
    count = QUARTERS * (n - 1) // 2
    bf16, f32 = jnp.bfloat16, jnp.float32
    dma = pltpu.SemaphoreType.DMA
    return pl.pallas_call(
        functools.partial(mixer_kernel, n, tp),
        out_shape=jax.ShapeDtypeStruct((rows, share), bf16),
        in_specs=[pl.BlockSpec(memory_space=pltpu.HBM)] * 11,
        out_specs=pl.BlockSpec(memory_space=pltpu.VMEM),
        scratch_shapes=[
            pltpu.VMEM((n, QUARTERS, depth // QUARTERS, qc + 2 * kc + cc), bf16),
            pltpu.VMEM((n, 2, 2, qc, half), bf16),
            pltpu.VMEM((n, rows, depth), bf16),
            pltpu.VMEM((rows, qc + 2 * kc + cc), f32),
            pltpu.VMEM((rows, qc), bf16),
            pltpu.VMEM((rows + 2 * WINDOW, 2 * kc), bf16),
            pltpu.VMEM((rows + 2 * RIM, cc), bf16),
            pltpu.VMEM((rows, qc + cc), bf16),
            pltpu.VMEM((n, 2, rows, half), bf16),
            pltpu.VMEM((n, 2, rows, half), bf16),
            pltpu.VMEM((per, 2, rows, half), bf16),
            pltpu.VMEM((per, 2, rows, half), f32),
            pltpu.VMEM((tp, 8, rows), f32),
            pltpu.VMEM((8, rows), f32),
            pltpu.VMEM((2, rows, half), bf16),
            pltpu.VMEM((2, rows, half), f32),
            pltpu.VMEM((2 * kc, depth), bf16),
            pltpu.VMEM((1, sink.shape[0]), f32),
            pltpu.VMEM(w_pool.shape, bf16),
            pltpu.VMEM((1, cc), f32),
            pltpu.VMEM((1, share), f32),
            dma((2, SENDS)),
            dma((2, RECVS)),
            dma((1,)),
            dma((3 * per,)),
            dma((4,)),
            dma((4,)),
            dma((1,)),
            dma((n // 2, 2)),
            dma((1,)),
            dma((per, 2)),
            dma((1,)),
            dma((2,)),
            dma((per + 12,)),
            dma((1,)),
            dma((tp,)),
            dma((1,)),
            dma((1,)),
        ],
        compiler_params=pltpu.CompilerParams(
            collective_id=0, has_side_effects=True, vmem_limit_bytes=32 * 1024 * 1024
        ),
        name="mixer",
    )(
        pltpu.with_memory_space_constraint(tokens, pltpu.HBM),
        pltpu.with_memory_space_constraint(w_query.reshape(QUARTERS, -1, qc), pltpu.HBM),
        pltpu.with_memory_space_constraint(w_key.T, pltpu.HBM),
        pltpu.with_memory_space_constraint(w_value.T, pltpu.HBM),
        pltpu.with_memory_space_constraint(w_pool_in.reshape(QUARTERS, -1, cc), pltpu.HBM),
        pltpu.with_memory_space_constraint(sink.reshape(1, -1), pltpu.HBM),
        pltpu.with_memory_space_constraint(w_pool, pltpu.HBM),
        pltpu.with_memory_space_constraint(pool_scale.reshape(1, -1), pltpu.HBM),
        pltpu.with_memory_space_constraint(w_out_attn, pltpu.HBM),
        pltpu.with_memory_space_constraint(w_out_pool, pltpu.HBM),
        pltpu.with_memory_space_constraint(out_gain.reshape(1, -1), pltpu.HBM),
    )


def fits(n, tp, tokens, w_query, w_key, w_pool, w_out_attn):
    return (
        tp == 4
        and n == 2 * tp
        and w_query.shape[0] % 64 == 0
        and w_query.shape[1] % 128 == 0
        and w_key.shape[1] == HEAD_DIM
        and w_pool.shape[0] == 1
        and w_out_attn.shape[1] % 256 == 0
        and w_out_attn.shape[0] == w_query.shape[1]
        and tokens.shape[0] >= 3 * WINDOW
    )


def mixed_rows(*args):
    n, tp = lax.axis_size("sp"), lax.axis_size("tp")
    if fits(n, tp, args[0], args[1], args[2], args[6], args[8]):
        return fused(n, tp, *args)
    return local(*args)


def solution(mesh):
    return jax.shard_map(
        mixed_rows,
        mesh=mesh,
        in_specs=(
            P("sp", "tp"),
            P("sp", "tp"),
            P("sp", "tp"),
            P("sp", "tp"),
            P("sp", "tp"),
            P("tp"),
            P("tp", None, None),
            P("tp"),
            P("tp", "sp"),
            P("tp", "sp"),
            P("tp"),
        ),
        out_specs=P("sp", "tp"),
        check_vma=False,
    )
```

```python
import functools

import jax
import jax.numpy as jnp
from jax import lax
from jax.experimental import pallas as pl
from jax.experimental.pallas import tpu as pltpu
from jax.sharding import PartitionSpec as P

HEAD_DIM = 64
POOL_GROUPS = 4
WINDOW = 128


epsilon = 1e-05
masked_score = -1e30


def padded(cells, sides, width):
    for axis, dim in sides:
        count = lax.axis_size(axis)
        ends = count - 1
        head = lax.slice_in_dim(cells, 0, width, axis=dim)
        tail = lax.slice_in_dim(cells, cells.shape[dim] - width, cells.shape[dim], axis=dim)
        cells = jnp.concatenate(
            [
                lax.ppermute(tail, axis, [(i, (i + 1) % count) for i in range(ends)]),
                cells,
                lax.ppermute(head, axis, [((i + 1) % count, i) for i in range(ends)]),
            ],
            axis=dim,
        )
    return cells


def make_projector(gathered, pieces):
    piece_query, piece_key, piece_value, piece_chan = pieces
    joined = jnp.concatenate([piece_key, piece_value], axis=1)
    return (
        jnp.dot(gathered, piece_query, preferred_element_type=jnp.float32),
        jnp.dot(gathered, joined, preferred_element_type=jnp.float32),
        jnp.dot(gathered, piece_chan, preferred_element_type=jnp.float32),
    )


def attend_local(query, keys_ext, sinks, offset, seq_len, key_cols):
    tok_rows, query_cols = query.shape
    kv_local = key_cols // HEAD_DIM
    group = query_cols // key_cols
    block_count = tok_rows // WINDOW
    stacked = keys_ext.reshape(block_count + 2, WINDOW, 2 * key_cols)
    banded = jnp.concatenate([stacked[:-2], stacked[1:-1], stacked[2:]], axis=1)
    key_band = banded[:, :, :key_cols].reshape(block_count, 3 * WINDOW, kv_local, HEAD_DIM)
    value_band = banded[:, :, key_cols:].reshape(block_count, 3 * WINDOW, kv_local, HEAD_DIM)
    query_blocks = query.reshape(block_count, WINDOW, kv_local, group, HEAD_DIM)
    scores = jnp.einsum(
        "nqkgd,nskd->nkgqs", query_blocks, key_band, preferred_element_type=jnp.float32
    ) * HEAD_DIM ** (-0.5)
    starts = offset + jnp.arange(block_count, dtype=jnp.int32) * WINDOW
    query_pos = starts[:, None] + jnp.arange(WINDOW, dtype=jnp.int32)[None, :]
    key_pos = starts[:, None] + jnp.arange(3 * WINDOW, dtype=jnp.int32)[None, :] - WINDOW
    distance = key_pos[:, None, :] - query_pos[:, :, None]
    inside = (key_pos >= 0) & (key_pos < seq_len)
    keep = (jnp.abs(distance) <= WINDOW) & inside[:, None, :]
    scores = jnp.where(keep[:, None, None], scores, masked_score)
    sink_logit = sinks.reshape(kv_local, group)[None, :, :, None, None]
    top = jnp.maximum(jnp.max(scores, axis=-1, keepdims=True), sink_logit)
    raised = jnp.exp(scores - top)
    total = jnp.sum(raised, axis=-1, keepdims=True) + jnp.exp(sink_logit - top)
    probs = (raised / total).astype(jnp.bfloat16)
    attended = jnp.einsum(
        "nkgqs,nskd->nqkgd", probs, value_band, preferred_element_type=jnp.float32
    )
    return attended.astype(jnp.bfloat16).reshape(tok_rows, query_cols)


def local(
    tokens,
    w_query,
    w_key,
    w_value,
    w_pool_in,
    sink,
    w_pool,
    pool_scale,
    w_out_attn,
    w_out_pool,
    out_gain,
):
    tok_rows = tokens.shape[0]
    seq_len = tok_rows * lax.axis_size("sp")
    offset = lax.axis_index("sp") * tok_rows
    out_both = jnp.concatenate([w_out_attn, w_out_pool], axis=0)
    gathered = lax.all_gather(tokens, "tp", axis=1, tiled=True)
    key_cols = w_key.shape[1]
    chan_cols = w_pool_in.shape[1]
    query_sum, joined_sum, chan_sum = make_projector(
        gathered,
        (
            lax.all_gather(w_query, "sp", axis=0, tiled=True),
            lax.all_gather(w_key, "sp", axis=0, tiled=True),
            lax.all_gather(w_value, "sp", axis=0, tiled=True),
            lax.all_gather(w_pool_in, "sp", axis=0, tiled=True),
        ),
    )
    query = query_sum.astype(jnp.bfloat16)
    key_value = joined_sum.astype(jnp.bfloat16)
    chan = chan_sum.astype(jnp.bfloat16)
    keys_ext = padded(key_value, (("sp", 0),), WINDOW)
    attended = attend_local(query, keys_ext, sink, offset, seq_len, key_cols)
    rim_rows = 2 ** (POOL_GROUPS - 1)
    chan_ext = padded(chan, (("sp", 0),), rim_rows)
    running = jnp.concatenate(
        [jnp.zeros((1, chan_cols), jnp.float32), jnp.cumsum(chan_ext.astype(jnp.float32), axis=0)],
        axis=0,
    )
    chan_float = chan.astype(jnp.float32)
    positions = offset + jnp.arange(tok_rows, dtype=jnp.int32)
    group_count = w_pool.shape[0]
    level = lax.axis_index("tp") * group_count + 0
    half = jnp.left_shift(jnp.int32(1), level)
    upper = lax.dynamic_slice_in_dim(running, rim_rows + half, tok_rows, 0)
    lower = lax.dynamic_slice_in_dim(running, rim_rows - half, tok_rows, 0)
    count = (
        jnp.clip(positions + half, 0, seq_len) - jnp.clip(positions - half, 0, seq_len)
    ).astype(jnp.float32)
    spread = ((upper - lower) / count[:, None] - chan_float).astype(jnp.bfloat16)
    outputs = jnp.dot(spread, w_pool[0], preferred_element_type=jnp.float32)
    pooled = (outputs * pool_scale).astype(jnp.bfloat16)
    hidden = jnp.concatenate([attended, pooled], axis=1)
    terms = jnp.dot(
        hidden,
        lax.all_gather(out_both, "sp", axis=1, tiled=True),
        preferred_element_type=jnp.float32,
    )
    share_width = out_gain.shape[0]
    model_width = share_width * lax.axis_size("tp")
    share = lax.psum_scatter(
        terms.astype(jnp.bfloat16), "tp", scatter_dimension=1, tiled=True
    ).astype(jnp.float32)
    row_total, row_square = lax.psum((jnp.sum(share, axis=1), jnp.sum(share * share, axis=1)), "tp")
    row_mean = row_total / model_width
    variance = row_square / model_width - row_mean * row_mean
    normed = (share - row_mean[:, None]) * lax.rsqrt(variance + epsilon)[:, None] * out_gain
    return normed.astype(jnp.bfloat16)


MESH = pl.DeviceIdType.MESH
RIM = 16
QUARTERS = 4
SENDS = 6
RECVS = 10


def mixer_kernel(
    n,
    tp,
    tok_ref,
    wq_ref,
    wk_ref,
    wv_ref,
    wc_ref,
    sink_ref,
    wp_ref,
    ps_ref,
    woa_ref,
    wop_ref,
    gain_ref,
    out_ref,
    win,
    wout,
    tok,
    acc,
    query,
    kv,
    chan,
    hidden,
    part,
    mated,
    landed,
    own,
    stats,
    late,
    echo,
    sums,
    pair_in,
    sinks,
    wpool,
    scales,
    gains,
    ring_send,
    ring_recv,
    tok_send,
    tok_recv,
    rim_send,
    rim_recv,
    mate_send,
    mate_recv,
    part_send,
    part_recv,
    echo_send,
    echo_recv,
    load,
    stat_send,
    stat_recv,
    late_send,
    late_recv,
):
    f32, bf16 = jnp.float32, jnp.bfloat16
    me, t = lax.axis_index("sp"), lax.axis_index("tp")
    rows = tok_ref.shape[0]
    seq_len = rows * n
    half_n = n // 2
    column = me % 2
    pos = (me // 2) * (1 - column) + column * (n - 1 - me // 2)

    def at(p):
        p = lax.rem(p + n, n)
        back = p // half_n
        return (1 - back) * (2 * p) + back * (2 * (n - 1 - p) + 1)

    ring = (at(pos + 1), at(pos - 1))
    after, before = lax.rem(me + 1, n), lax.rem(me + n - 1, n)
    mate = t + 1 - 2 * lax.rem(t, 2)
    across = lax.rem(t + 2, tp)
    per = n // tp

    def rdma(src, dst, send, recv, sp, tpi):
        return pltpu.make_async_remote_copy(
            src_ref=src,
            dst_ref=dst,
            send_sem=send,
            recv_sem=recv,
            device_id={"sp": sp, "tp": tpi},
            device_id_type=MESH,
        )

    qc, kc = wq_ref.shape[2], wk_ref.shape[0]
    cc = wc_ref.shape[2]
    depth = QUARTERS * wq_ref.shape[1]
    quarter = depth // QUARTERS
    wide = woa_ref.shape[1]
    half = wide // 2
    barrier = pltpu.get_barrier_semaphore()
    peers = [(s, t) for s in ring]
    peers += [(me, mate), (me, across)]
    for s, p in peers:
        pl.semaphore_signal(barrier, inc=1, device_id={"sp": s, "tp": p}, device_id_type=MESH)

    loads = []

    def fetch(src, dst, sem=None):
        copy = pltpu.make_async_copy(src, dst, load.at[len(loads)] if sem is None else load.at[sem])
        copy.start()
        if sem is None:
            loads.append(copy)
        return copy

    fetch(wk_ref, pair_in.at[pl.ds(0, kc)])
    fetch(wv_ref, pair_in.at[pl.ds(kc, kc)], 0)
    pairs = [pltpu.make_async_copy(pair_in, pair_in, load.at[0])]
    first = [
        fetch(wq_ref, win.at[me, :, :, pl.ds(0, qc)]),
        fetch(wc_ref, win.at[me, :, :, pl.ds(qc + 2 * kc, cc)]),
    ]
    mine = tok.at[pl.ds(t * per, per)]
    own_sem = len(loads)
    for b in range(per):
        fetch(tok_ref.at[:, pl.ds(b * depth, depth)], tok.at[t * per + b], own_sem if b else None)
    own_tok = [pltpu.make_async_copy(mine, mine, load.at[own_sem])]
    wout_sem = len(loads)
    for h in range(2):
        fetch(woa_ref.at[:, pl.ds(h * half, half)], wout.at[me, h, 0], wout_sem if h else None)
        fetch(wop_ref.at[:, pl.ds(h * half, half)], wout.at[me, h, 1], wout_sem)
    later = [pltpu.make_async_copy(wout.at[me], wout.at[me], load.at[wout_sem])]
    later.append(fetch(sink_ref, sinks))
    later.append(fetch(wp_ref, wpool))
    later.append(fetch(ps_ref, scales))
    later.append(fetch(gain_ref, gains))
    for copy in pairs:
        copy.wait()
    pair = jnp.transpose(pair_in[...].astype(f32)).astype(bf16)
    for h in range(QUARTERS):
        win[me, h, :, qc : qc + 2 * kc] = pair[h * quarter : (h + 1) * quarter]
    for copy in first:
        copy.wait()
    pl.semaphore_wait(barrier, len(peers))

    count = QUARTERS * (n - 1) // 2
    last = count - 1

    def ring_copy(buf, way, k, hop, turn):
        sign = -1 if way == 0 else 1
        q = k % QUARTERS
        o = at(pos + sign * (k // QUARTERS + hop))
        if buf is win:
            slot = buf.at[o, q if way == 0 else QUARTERS - 1 - q]
        elif k >= last - 1:
            slot = buf.at[o, q, way]
        else:
            slot = buf.at[o, q // 2, (q + way) % 2]
        return rdma(slot, slot, ring_send.at[way, turn % SENDS], ring_recv.at[way, turn % RECVS], ring[way], t)

    def w_in(way, k, hop):
        return ring_copy(win, way, k, hop, k)

    def w_out(way, k, hop):
        return ring_copy(wout, way, k, hop, count + k)

    def launched(way, turn):
        return w_in(way, turn, 0) if turn < count else w_out(way, turn - count, 0)

    def launch(way, turn):
        if turn >= SENDS:
            launched(way, turn - SENDS).wait_send()
        launched(way, turn).start()

    def tok_copy(owner, b, i, dst):
        slot = tok.at[owner * per + b]
        return rdma(slot, slot, tok_send.at[0], tok_recv.at[i], me, dst)

    for k in range(QUARTERS):
        for way in range(2):
            launch(way, k)
    for copy in own_tok:
        copy.wait()
    for b in range(per):
        tok_copy(t, b, b, across).start()
    for b in range(per):
        tok_copy(t, b, per + b, mate).start()

    for copy in later:
        copy.wait()

    origin = [at(pos)]
    for d in range(1, half_n):
        origin += [at(pos - d), at(pos + d)]
    origin.append(at(pos + half_n))

    def project(i, first=False):
        o = origin[i]
        w = win[o].reshape(depth, qc + 2 * kc + cc)
        term = jnp.dot(tok[o], w, preferred_element_type=f32)
        if first:
            acc[...] = term
        else:
            acc[...] += term

    def relay(copy, k):
        for way in range(2):
            copy(way, k, 1).wait_recv()
            if copy is w_in:
                if k + QUARTERS <= last:
                    launch(way, k + QUARTERS)
            elif k + QUARTERS < last:
                launch(way, count + k + QUARTERS)
            elif k == last - 3:
                launch(way, count + last)

    def start_out(k):
        for way in range(2):
            launch(way, count + k)

    done_blocks = 0
    for k in range(count):
        relay(w_in, k)
        if last - 3 <= k < last:
            start_out(k - (last - 3))
        if k in (3, 6):
            b = 0 if k == 3 else 1
            tok_copy(across, b, b, across).wait_recv()
            tok_copy(across, b, 2 * per + b, mate).start()
        if k == 8:
            for b in range(per):
                tok_copy(mate, b, per + b, mate).wait_recv()
                tok_copy(lax.rem(mate + 2, tp), b, 2 * per + b, mate).wait_recv()
        if k >= 8:
            ready = n if k == last else 1 + 2 * ((k + 1) // QUARTERS)
            upto = ready if k == last else min(ready, done_blocks + 2)
            while done_blocks < upto:
                project(done_blocks, done_blocks == 0)
                done_blocks += 1

    kv[WINDOW : WINDOW + rows, :] = acc[:, qc : qc + 2 * kc].astype(bf16)
    chan[RIM : RIM + rows, :] = acc[:, qc + 2 * kc :].astype(bf16)

    def rim(buf, width, down, i):
        if down:
            return rdma(buf.at[pl.ds(rows, width)], buf.at[pl.ds(0, width)], rim_send.at[i], rim_recv.at[i], after, t)
        return rdma(
            buf.at[pl.ds(width, width)], buf.at[pl.ds(rows + width, width)], rim_send.at[i], rim_recv.at[i], before, t
        )

    rims = [rim(kv, WINDOW, True, 0), rim(kv, WINDOW, False, 1), rim(chan, RIM, True, 2), rim(chan, RIM, False, 3)]
    for c in rims:
        c.start()
    start_out(3)
    query[...] = acc[:, 0:qc].astype(bf16)

    group = qc // kc

    def attend(b):
        band = kv[b * WINDOW : (b + 3) * WINDOW, :]
        q = query[b * WINDOW : (b + 1) * WINDOW, :]
        stacked = jnp.concatenate([q[:, g * HEAD_DIM : (g + 1) * HEAD_DIM] for g in range(group)], axis=0)
        scores = lax.dot_general(
            stacked, band[:, :HEAD_DIM], (((1,), (1,)), ((), ())), preferred_element_type=f32
        ) * HEAD_DIM ** (-0.5)
        scores = scores.reshape(group, WINDOW, 3 * WINDOW)
        r = lax.broadcasted_iota(jnp.int32, (WINDOW, 3 * WINDOW), 0)
        c = lax.broadcasted_iota(jnp.int32, (WINDOW, 3 * WINDOW), 1)
        keep = (c >= r) & (c <= r + 2 * WINDOW)
        key_pos = c + (me * rows + b * WINDOW - WINDOW)
        keep = keep & (key_pos >= 0) & (key_pos < seq_len)
        outs = []
        for g in range(group):
            s = jnp.where(keep, scores[g], masked_score)
            logit = sinks[0:1, g : g + 1]
            top = jnp.maximum(jnp.max(s, axis=1, keepdims=True), logit)
            raised = jnp.exp(s - top)
            total = jnp.sum(raised, axis=1, keepdims=True) + jnp.exp(logit - top)
            outs.append((raised * (1.0 / total)).astype(bf16))
        got = jnp.dot(jnp.concatenate(outs, axis=0), band, preferred_element_type=f32)
        got = got[:, HEAD_DIM : 2 * HEAD_DIM].astype(bf16)
        hidden[place(b) : place(b) + WINDOW, 0:qc] = jnp.concatenate(
            [got[g * WINDOW : (g + 1) * WINDOW] for g in range(group)], axis=1
        )

    blocks = rows // WINDOW
    order = list(range(1, blocks - 1)) + [0, blocks - 1]
    early = (blocks - 2) * WINDOW

    def place(b):
        return order.index(b) * WINDOW

    half_width = 1
    for level in range(1, POOL_GROUPS):
        half_width = jnp.where(t == level, 2**level, half_width)

    def spread_of(start, size):
        length = size + 2 * RIM
        e = chan[start : start + length].astype(f32)
        p = lax.broadcasted_iota(jnp.int32, (length, 1), 0) + (me * rows + start - RIM)
        e = jnp.where((p >= 0) & (p < seq_len), e, 0.0)
        total = e + pltpu.roll(e, 1, 0)
        pick = total
        for level in range(1, POOL_GROUPS):
            step = 2 ** (level - 1)
            total = pltpu.roll(total, step, 0) + pltpu.roll(total, length - step, 0)
            pick = jnp.where(t == level, total, pick)
        number = (jnp.clip(p + half_width, 0, seq_len) - jnp.clip(p - half_width, 0, seq_len)).astype(f32)
        return (pick[RIM : RIM + size] / number[RIM : RIM + size] - e[RIM : RIM + size]).astype(bf16)

    def pooled_of(spread):
        return (jnp.dot(spread, wpool[0], preferred_element_type=f32) * scales[...]).astype(bf16)

    def pool_inner():
        got = pooled_of(spread_of(RIM, rows - 2 * RIM))
        for b in range(blocks):
            low, high = max(b * WINDOW, RIM), min((b + 1) * WINDOW, rows - RIM)
            base = place(b) - b * WINDOW
            hidden[base + low : base + high, qc:] = got[low - RIM : high - RIM]

    def pool_edges():
        got = pooled_of(jnp.concatenate([spread_of(0, RIM), spread_of(rows - RIM, RIM)], axis=0))
        hidden[place(0) : place(0) + RIM, qc:] = got[0:RIM]
        end = place(blocks - 1) + WINDOW
        hidden[end - RIM : end, qc:] = got[RIM:]

    near = 3
    spans = (pl.ds(0, early), pl.ds(early, rows - early))

    def unit(buf, o, u, split):
        return buf.at[o, :, spans[u]] if split else buf.at[o, u]

    def to_mate(o, u, split):
        i = (o // (2 * per)) * per + lax.rem(o, per)
        return rdma(
            unit(part, o, u, split), unit(mated, o, u, split), mate_send.at[0], mate_recv.at[i, u], me, mate
        )

    def to_owner(o, u, split):
        i = lax.rem(o, per)
        return rdma(
            unit(part, o, u, split), unit(landed, i, u, split), part_send.at[0], part_recv.at[i, u], me, across
        )

    final = origin[n - 1]
    holder = final // per

    def to_echo(h):
        return rdma(part.at[final, h], echo.at[h], echo_send.at[0], echo_recv.at[h], me, across)

    def to_late():
        return rdma(late, late, late_send.at[0], late_recv.at[0], me, mate)

    def to_far():
        return rdma(late, late, late_send.at[1], late_recv.at[0], me, lax.rem(mate + 2, tp))

    detour = holder == 0
    tells = jnp.logical_or(holder == across, jnp.logical_and(holder == t, jnp.logical_not(detour)))
    tells_far = jnp.logical_and(holder == across, detour)

    pieces = [(0, 0), (0, 1)]
    for k in range(1, count - 2, 2):
        d, h = k // QUARTERS, (k % QUARTERS) // 2
        pieces += [(2 * d + 1, h), (2 * d + 2, h)]
    pieces += [(n - 1, 0), (n - 1, 1)]

    def emit(places, span, split):
        side = jnp.concatenate([wout[origin[i], h].reshape(qc + cc, half) for i, h in places], axis=1)
        got = jnp.dot(hidden[span, :], side, preferred_element_type=f32).astype(bf16)
        for j, (i, h) in enumerate(places):
            part[origin[i], h, span] = got[:, j * half : (j + 1) * half]
        sent = [(i, spans.index(span)) for i, h in places if h == 0] if split else places
        for i, u in sent:
            o = origin[i]

            @pl.when(lax.rem(o // per, 2) != lax.rem(t, 2))
            def _(o=o, u=u):
                to_mate(o, u, split).start()

    def emit_near(u):
        emit([(i, h) for i in range(near) for h in range(2)], spans[u], True)

    def emit_far(ids):
        emit([pieces[i] for i in ids], pl.ds(0, rows), False)

    def combine(i, u, split):
        o = origin[i]
        where = (slice(None), spans[u]) if split else (u,)

        @pl.when(o // per == t)
        def _():
            to_mate(o, u, split).wait_recv()
            both = part[(o,) + where].astype(f32) + mated[(o,) + where].astype(f32)
            own[(lax.rem(o, per),) + where] = both
            if i == n - 1:
                part[(o,) + where] = both.astype(bf16)
                to_echo(u).start()

        @pl.when(o // per == across)
        def _():
            to_mate(o, u, split).wait_recv()
            both = part[(o,) + where].astype(f32) + mated[(o,) + where].astype(f32)
            part[(o,) + where] = both.astype(bf16)
            to_owner(o, u, split).start()

    def combine_near(u):
        for i in range(near):
            combine(i, u, True)

    def combine_far(ids):
        for i in ids:
            combine(pieces[i][0], pieces[i][1], False)

    def pack(one, two):
        one = jnp.sum(jnp.transpose(one), axis=0, keepdims=True)
        two = jnp.sum(jnp.transpose(two), axis=0, keepdims=True)
        return jnp.concatenate([one, two, jnp.zeros((6, rows), f32)], axis=0)

    sums[...] = jnp.zeros_like(sums)
    emits = {5: (6, 8), 7: (8, 10), 9: (10, 12), 11: (12, 14), 12: (14, 15), 13: (15, 16)}
    odd = lax.rem(t, 2) == 1
    ahead = {6: (6, 8), 7: (8, 10), 9: (10, 12), 11: (12, 14), 12: (14, 15), 13: (15, 16)}
    behind = {7: (6, 8), 8: (8, 10), 10: (10, 12), 12: (12, 14), 13: (14, 16)}

    def on(core, work, *args):
        @pl.when(odd == core)
        def _():
            work(*args)

    for k in range(count):
        relay(w_out, k)
        if k < 2:
            for b in order[: blocks - 2][k::2]:
                attend(b)
        elif k == 2:
            pool_inner()
        elif k == 3:
            emit_near(0)
            for c in rims:
                c.wait()
            attend(0)
            on(False, combine_near, 0)
        elif k == 4:
            attend(blocks - 1)
            on(True, combine_near, 0)
            pool_edges()
            emit_near(1)
        if k in emits:
            emit_far(range(*emits[k]))
        if k == 5:
            on(False, combine_near, 1)
        elif k == 6:
            on(True, combine_near, 1)
        if k in ahead:
            on(False, combine_far, range(*ahead[k]))
        if k in behind:
            on(True, combine_far, range(*behind[k]))

    def stat_copy(j):
        return rdma(stats.at[t], stats.at[t], stat_send.at[0], stat_recv.at[t], me, lax.rem(t + j, tp))

    for i in range(n - 1):
        o = origin[i]

        @pl.when(o // per == t)
        def _(o=o, i=i):
            for u in range(2):
                to_owner(o, u, i < near).wait_recv()

    for i in range(per):
        o = t * per + i

        @pl.when(o != final)
        def _(o=o, i=i):
            one = two = 0.0
            for h in range(2):
                mix = own[i, h] + landed[i, h].astype(f32)
                acc[:, (2 * i + h) * half : (2 * i + h + 1) * half] = mix
                one, two = one + mix, two + mix * mix
            sums[0] += one
            sums[1] += two

    stats[t] = pack(sums[0], sums[1])
    for j in range(1, tp):
        stat_copy(j).start()

    @pl.when(holder == t)
    def _():
        one = two = 0.0
        for h in range(2):
            i = lax.rem(final, per)
            to_owner(final, h, False).wait_recv()
            mix = own[i, h] + landed[i, h].astype(f32)
            acc[:, pl.ds(pl.multiple_of((2 * i + h) * half, 128), half)] = mix
            one, two = one + mix, two + mix * mix
        late[...] = pack(one, two)

        @pl.when(tells)
        def _():
            to_late().start()

    @pl.when(holder == across)
    def _():
        one = two = 0.0
        for h in range(2):
            to_echo(h).wait_recv()
            mix = part[final, h].astype(f32) + echo[h].astype(f32)
            one, two = one + mix, two + mix * mix
        late[...] = pack(one, two)

        @pl.when(tells_far)
        def _():
            to_far().start()

        to_late().start()

    def drain(buf, amount, sem):
        whole = buf.at[pl.ds(0, amount)]
        rdma(whole, whole, sem.at[0], mate_recv.at[0, 0], me, mate).wait_send()

    for j in range(1, tp):
        src = lax.rem(t + j, tp)
        rdma(stats.at[src], stats.at[src], stat_send.at[0], stat_recv.at[src], me, src).wait_recv()
    paired = lax.rem(holder, 2) == lax.rem(t, 2)

    @pl.when(jnp.logical_not(paired))
    def _():
        to_late().wait_recv()

    totals = late[...] + stats[0]
    for i in range(1, tp):
        totals = totals + stats[i]
    width = gain_ref.shape[1] * tp
    line_mean = totals[0:1] / width
    line_scale = lax.rsqrt(totals[1:2] / width - line_mean * line_mean + epsilon)
    tall = jnp.concatenate([line_mean, line_scale, jnp.zeros((6, rows), f32)], axis=0)
    back = jnp.transpose(tall)
    row_mean, scale = back[:, 0:1], back[:, 1:2]
    normed = ((acc[:, 0 : gain_ref.shape[1]] - row_mean) * scale * gains[...]).astype(bf16)
    for b in range(blocks):
        out_ref[b * WINDOW : (b + 1) * WINDOW, :] = normed[place(b) : place(b) + WINDOW]
    drain(part, n // 2, mate_send)
    drain(part, per, part_send)
    drain(tok, 3 * per, tok_send)

    @pl.when(holder == t)
    def _():
        drain(part, 1, echo_send)

    for turn in range(2 * count - SENDS, 2 * count):
        for way in range(2):
            launched(way, turn).wait_send()
    drain(stats, tp - 1, stat_send)

    @pl.when(tells)
    def _():
        to_late().wait_send()

    @pl.when(tells_far)
    def _():
        to_far().wait_send()


def fused(n, tp, tokens, w_query, w_key, w_value, w_pool_in, sink, w_pool, pool_scale, w_out_attn, w_out_pool, out_gain):
    rows, share = tokens.shape
    depth, qc = w_query.shape
    kc, cc = w_key.shape[1], w_pool_in.shape[1]
    wide = w_out_attn.shape[1]
    half = wide // 2
    per = n // tp
    count = QUARTERS * (n - 1) // 2
    bf16, f32 = jnp.bfloat16, jnp.float32
    dma = pltpu.SemaphoreType.DMA
    return pl.pallas_call(
        functools.partial(mixer_kernel, n, tp),
        out_shape=jax.ShapeDtypeStruct((rows, share), bf16),
        in_specs=[pl.BlockSpec(memory_space=pltpu.HBM)] * 11,
        out_specs=pl.BlockSpec(memory_space=pltpu.VMEM),
        scratch_shapes=[
            pltpu.VMEM((n, QUARTERS, depth // QUARTERS, qc + 2 * kc + cc), bf16),
            pltpu.VMEM((n, 2, 2, qc, half), bf16),
            pltpu.VMEM((n, rows, depth), bf16),
            pltpu.VMEM((rows, qc + 2 * kc + cc), f32),
            pltpu.VMEM((rows, qc), bf16),
            pltpu.VMEM((rows + 2 * WINDOW, 2 * kc), bf16),
            pltpu.VMEM((rows + 2 * RIM, cc), bf16),
            pltpu.VMEM((rows, qc + cc), bf16),
            pltpu.VMEM((n, 2, rows, half), bf16),
            pltpu.VMEM((n, 2, rows, half), bf16),
            pltpu.VMEM((per, 2, rows, half), bf16),
            pltpu.VMEM((per, 2, rows, half), f32),
            pltpu.VMEM((tp, 8, rows), f32),
            pltpu.VMEM((8, rows), f32),
            pltpu.VMEM((2, rows, half), bf16),
            pltpu.VMEM((2, rows, half), f32),
            pltpu.VMEM((2 * kc, depth), bf16),
            pltpu.VMEM((1, sink.shape[0]), f32),
            pltpu.VMEM(w_pool.shape, bf16),
            pltpu.VMEM((1, cc), f32),
            pltpu.VMEM((1, share), f32),
            dma((2, SENDS)),
            dma((2, RECVS)),
            dma((1,)),
            dma((3 * per,)),
            dma((4,)),
            dma((4,)),
            dma((1,)),
            dma((n // 2, 2)),
            dma((1,)),
            dma((per, 2)),
            dma((1,)),
            dma((2,)),
            dma((9,)),
            dma((1,)),
            dma((tp,)),
            dma((2,)),
            dma((1,)),
        ],
        compiler_params=pltpu.CompilerParams(
            collective_id=0, has_side_effects=True, vmem_limit_bytes=32 * 1024 * 1024
        ),
        name="mixer",
    )(
        pltpu.with_memory_space_constraint(tokens, pltpu.HBM),
        pltpu.with_memory_space_constraint(w_query.reshape(QUARTERS, -1, qc), pltpu.HBM),
        pltpu.with_memory_space_constraint(w_key.T, pltpu.HBM),
        pltpu.with_memory_space_constraint(w_value.T, pltpu.HBM),
        pltpu.with_memory_space_constraint(w_pool_in.reshape(QUARTERS, -1, cc), pltpu.HBM),
        pltpu.with_memory_space_constraint(sink.reshape(1, -1), pltpu.HBM),
        pltpu.with_memory_space_constraint(w_pool, pltpu.HBM),
        pltpu.with_memory_space_constraint(pool_scale.reshape(1, -1), pltpu.HBM),
        pltpu.with_memory_space_constraint(w_out_attn, pltpu.HBM),
        pltpu.with_memory_space_constraint(w_out_pool, pltpu.HBM),
        pltpu.with_memory_space_constraint(out_gain.reshape(1, -1), pltpu.HBM),
    )


def fits(n, tp, tokens, w_query, w_key, w_pool, w_out_attn):
    return (
        tp == 4
        and n == 2 * tp
        and w_query.shape[0] % 64 == 0
        and w_query.shape[1] % 128 == 0
        and w_key.shape[1] == HEAD_DIM
        and w_pool.shape[0] == 1
        and w_out_attn.shape[1] % 256 == 0
        and w_out_attn.shape[0] == w_query.shape[1]
        and tokens.shape[0] >= 3 * WINDOW
    )


def mixed_rows(*args):
    n, tp = lax.axis_size("sp"), lax.axis_size("tp")
    if fits(n, tp, args[0], args[1], args[2], args[6], args[8]):
        return fused(n, tp, *args)
    return local(*args)


def solution(mesh):
    return jax.shard_map(
        mixed_rows,
        mesh=mesh,
        in_specs=(
            P("sp", "tp"),
            P("sp", "tp"),
            P("sp", "tp"),
            P("sp", "tp"),
            P("sp", "tp"),
            P("tp"),
            P("tp", None, None),
            P("tp"),
            P("tp", "sp"),
            P("tp", "sp"),
            P("tp"),
        ),
        out_specs=P("sp", "tp"),
        check_vma=False,
    )
```

```python
import functools

import jax
import jax.numpy as jnp
from jax import lax
from jax.experimental import pallas as pl
from jax.experimental.pallas import tpu as pltpu
from jax.sharding import PartitionSpec as P

HEAD_DIM = 64
POOL_GROUPS = 4
WINDOW = 128


epsilon = 1e-05
masked_score = -1e30


def padded(cells, sides, width):
    for axis, dim in sides:
        count = lax.axis_size(axis)
        ends = count - 1
        head = lax.slice_in_dim(cells, 0, width, axis=dim)
        tail = lax.slice_in_dim(cells, cells.shape[dim] - width, cells.shape[dim], axis=dim)
        cells = jnp.concatenate(
            [
                lax.ppermute(tail, axis, [(i, (i + 1) % count) for i in range(ends)]),
                cells,
                lax.ppermute(head, axis, [((i + 1) % count, i) for i in range(ends)]),
            ],
            axis=dim,
        )
    return cells


def make_projector(gathered, pieces):
    piece_query, piece_key, piece_value, piece_chan = pieces
    joined = jnp.concatenate([piece_key, piece_value], axis=1)
    return (
        jnp.dot(gathered, piece_query, preferred_element_type=jnp.float32),
        jnp.dot(gathered, joined, preferred_element_type=jnp.float32),
        jnp.dot(gathered, piece_chan, preferred_element_type=jnp.float32),
    )


def attend_local(query, keys_ext, sinks, offset, seq_len, key_cols):
    tok_rows, query_cols = query.shape
    kv_local = key_cols // HEAD_DIM
    group = query_cols // key_cols
    block_count = tok_rows // WINDOW
    stacked = keys_ext.reshape(block_count + 2, WINDOW, 2 * key_cols)
    banded = jnp.concatenate([stacked[:-2], stacked[1:-1], stacked[2:]], axis=1)
    key_band = banded[:, :, :key_cols].reshape(block_count, 3 * WINDOW, kv_local, HEAD_DIM)
    value_band = banded[:, :, key_cols:].reshape(block_count, 3 * WINDOW, kv_local, HEAD_DIM)
    query_blocks = query.reshape(block_count, WINDOW, kv_local, group, HEAD_DIM)
    scores = jnp.einsum(
        "nqkgd,nskd->nkgqs", query_blocks, key_band, preferred_element_type=jnp.float32
    ) * HEAD_DIM ** (-0.5)
    starts = offset + jnp.arange(block_count, dtype=jnp.int32) * WINDOW
    query_pos = starts[:, None] + jnp.arange(WINDOW, dtype=jnp.int32)[None, :]
    key_pos = starts[:, None] + jnp.arange(3 * WINDOW, dtype=jnp.int32)[None, :] - WINDOW
    distance = key_pos[:, None, :] - query_pos[:, :, None]
    inside = (key_pos >= 0) & (key_pos < seq_len)
    keep = (jnp.abs(distance) <= WINDOW) & inside[:, None, :]
    scores = jnp.where(keep[:, None, None], scores, masked_score)
    sink_logit = sinks.reshape(kv_local, group)[None, :, :, None, None]
    top = jnp.maximum(jnp.max(scores, axis=-1, keepdims=True), sink_logit)
    raised = jnp.exp(scores - top)
    total = jnp.sum(raised, axis=-1, keepdims=True) + jnp.exp(sink_logit - top)
    probs = (raised / total).astype(jnp.bfloat16)
    attended = jnp.einsum(
        "nkgqs,nskd->nqkgd", probs, value_band, preferred_element_type=jnp.float32
    )
    return attended.astype(jnp.bfloat16).reshape(tok_rows, query_cols)


def local(
    tokens,
    w_query,
    w_key,
    w_value,
    w_pool_in,
    sink,
    w_pool,
    pool_scale,
    w_out_attn,
    w_out_pool,
    out_gain,
):
    tok_rows = tokens.shape[0]
    seq_len = tok_rows * lax.axis_size("sp")
    offset = lax.axis_index("sp") * tok_rows
    out_both = jnp.concatenate([w_out_attn, w_out_pool], axis=0)
    gathered = lax.all_gather(tokens, "tp", axis=1, tiled=True)
    key_cols = w_key.shape[1]
    chan_cols = w_pool_in.shape[1]
    query_sum, joined_sum, chan_sum = make_projector(
        gathered,
        (
            lax.all_gather(w_query, "sp", axis=0, tiled=True),
            lax.all_gather(w_key, "sp", axis=0, tiled=True),
            lax.all_gather(w_value, "sp", axis=0, tiled=True),
            lax.all_gather(w_pool_in, "sp", axis=0, tiled=True),
        ),
    )
    query = query_sum.astype(jnp.bfloat16)
    key_value = joined_sum.astype(jnp.bfloat16)
    chan = chan_sum.astype(jnp.bfloat16)
    keys_ext = padded(key_value, (("sp", 0),), WINDOW)
    attended = attend_local(query, keys_ext, sink, offset, seq_len, key_cols)
    rim_rows = 2 ** (POOL_GROUPS - 1)
    chan_ext = padded(chan, (("sp", 0),), rim_rows)
    running = jnp.concatenate(
        [jnp.zeros((1, chan_cols), jnp.float32), jnp.cumsum(chan_ext.astype(jnp.float32), axis=0)],
        axis=0,
    )
    chan_float = chan.astype(jnp.float32)
    positions = offset + jnp.arange(tok_rows, dtype=jnp.int32)
    group_count = w_pool.shape[0]
    level = lax.axis_index("tp") * group_count + 0
    half = jnp.left_shift(jnp.int32(1), level)
    upper = lax.dynamic_slice_in_dim(running, rim_rows + half, tok_rows, 0)
    lower = lax.dynamic_slice_in_dim(running, rim_rows - half, tok_rows, 0)
    count = (
        jnp.clip(positions + half, 0, seq_len) - jnp.clip(positions - half, 0, seq_len)
    ).astype(jnp.float32)
    spread = ((upper - lower) / count[:, None] - chan_float).astype(jnp.bfloat16)
    outputs = jnp.dot(spread, w_pool[0], preferred_element_type=jnp.float32)
    pooled = (outputs * pool_scale).astype(jnp.bfloat16)
    hidden = jnp.concatenate([attended, pooled], axis=1)
    terms = jnp.dot(
        hidden,
        lax.all_gather(out_both, "sp", axis=1, tiled=True),
        preferred_element_type=jnp.float32,
    )
    share_width = out_gain.shape[0]
    model_width = share_width * lax.axis_size("tp")
    share = lax.psum_scatter(
        terms.astype(jnp.bfloat16), "tp", scatter_dimension=1, tiled=True
    ).astype(jnp.float32)
    row_total, row_square = lax.psum((jnp.sum(share, axis=1), jnp.sum(share * share, axis=1)), "tp")
    row_mean = row_total / model_width
    variance = row_square / model_width - row_mean * row_mean
    normed = (share - row_mean[:, None]) * lax.rsqrt(variance + epsilon)[:, None] * out_gain
    return normed.astype(jnp.bfloat16)


MESH = pl.DeviceIdType.MESH
RIM = 16
QUARTERS = 4
SENDS = 6
RECVS = 10


def mixer_kernel(
    n,
    tp,
    tok_ref,
    wq_ref,
    wk_ref,
    wv_ref,
    wc_ref,
    sink_ref,
    wp_ref,
    ps_ref,
    woa_ref,
    wop_ref,
    gain_ref,
    out_ref,
    win,
    wout,
    tok,
    acc,
    query,
    kv,
    chan,
    hidden,
    part,
    mated,
    landed,
    own,
    stats,
    late,
    echo,
    sums,
    pair_in,
    sinks,
    wpool,
    scales,
    gains,
    ring_send,
    ring_recv,
    tok_send,
    tok_recv,
    rim_send,
    rim_recv,
    mate_send,
    mate_recv,
    part_send,
    part_recv,
    echo_send,
    echo_recv,
    load,
    stat_send,
    stat_recv,
    late_send,
    late_recv,
):
    f32, bf16 = jnp.float32, jnp.bfloat16
    me, t = lax.axis_index("sp"), lax.axis_index("tp")
    rows = tok_ref.shape[0]
    seq_len = rows * n
    half_n = n // 2
    column = me % 2
    pos = (me // 2) * (1 - column) + column * (n - 1 - me // 2)

    def at(p):
        p = lax.rem(p + n, n)
        back = p // half_n
        return (1 - back) * (2 * p) + back * (2 * (n - 1 - p) + 1)

    ring = (at(pos + 1), at(pos - 1))
    after, before = lax.rem(me + 1, n), lax.rem(me + n - 1, n)
    mate = t + 1 - 2 * lax.rem(t, 2)
    across = lax.rem(t + 2, tp)
    per = n // tp

    def rdma(src, dst, send, recv, sp, tpi):
        return pltpu.make_async_remote_copy(
            src_ref=src,
            dst_ref=dst,
            send_sem=send,
            recv_sem=recv,
            device_id={"sp": sp, "tp": tpi},
            device_id_type=MESH,
        )

    qc, kc = wq_ref.shape[2], wk_ref.shape[0]
    cc = wc_ref.shape[2]
    depth = QUARTERS * wq_ref.shape[1]
    quarter = depth // QUARTERS
    wide = woa_ref.shape[1]
    half = wide // 2
    barrier = pltpu.get_barrier_semaphore()
    peers = [(s, t) for s in ring]
    peers += [(me, mate), (me, across)]
    for s, p in peers:
        pl.semaphore_signal(barrier, inc=1, device_id={"sp": s, "tp": p}, device_id_type=MESH)

    loads = []

    def fetch(src, dst, sem=None):
        copy = pltpu.make_async_copy(src, dst, load.at[len(loads)] if sem is None else load.at[sem])
        copy.start()
        if sem is None:
            loads.append(copy)
        return copy

    fetch(wk_ref, pair_in.at[pl.ds(0, kc)])
    fetch(wv_ref, pair_in.at[pl.ds(kc, kc)], 0)
    pairs = [pltpu.make_async_copy(pair_in, pair_in, load.at[0])]
    first = [
        fetch(wq_ref, win.at[me, :, :, pl.ds(0, qc)]),
        fetch(wc_ref, win.at[me, :, :, pl.ds(qc + 2 * kc, cc)]),
    ]
    mine = tok.at[pl.ds(t * per, per)]
    own_sem = len(loads)
    for b in range(per):
        fetch(tok_ref.at[:, pl.ds(b * depth, depth)], tok.at[t * per + b], own_sem if b else None)
    own_tok = [pltpu.make_async_copy(mine, mine, load.at[own_sem])]
    wout_sem = len(loads)
    for h in range(2):
        fetch(woa_ref.at[:, pl.ds(h * half, half)], wout.at[me, h, 0], wout_sem if h else None)
        fetch(wop_ref.at[:, pl.ds(h * half, half)], wout.at[me, h, 1], wout_sem)
    later = [pltpu.make_async_copy(wout.at[me], wout.at[me], load.at[wout_sem])]
    later.append(fetch(sink_ref, sinks))
    later.append(fetch(wp_ref, wpool))
    later.append(fetch(ps_ref, scales))
    later.append(fetch(gain_ref, gains))
    for copy in pairs:
        copy.wait()
    pair = jnp.transpose(pair_in[...].astype(f32)).astype(bf16)
    for h in range(QUARTERS):
        win[me, h, :, qc : qc + 2 * kc] = pair[h * quarter : (h + 1) * quarter]
    for copy in first:
        copy.wait()
    pl.semaphore_wait(barrier, len(peers))

    count = QUARTERS * (n - 1) // 2
    last = count - 1

    def ring_copy(buf, way, k, hop, turn):
        sign = -1 if way == 0 else 1
        q = k % QUARTERS
        o = at(pos + sign * (k // QUARTERS + hop))
        if buf is win:
            slot = buf.at[o, q if way == 0 else QUARTERS - 1 - q]
        elif k >= last - 1:
            slot = buf.at[o, q, way]
        else:
            slot = buf.at[o, q // 2, (q + way) % 2]
        return rdma(slot, slot, ring_send.at[way, turn % SENDS], ring_recv.at[way, turn % RECVS], ring[way], t)

    def w_in(way, k, hop):
        return ring_copy(win, way, k, hop, k)

    def w_out(way, k, hop):
        return ring_copy(wout, way, k, hop, count + k)

    def launched(way, turn):
        return w_in(way, turn, 0) if turn < count else w_out(way, turn - count, 0)

    def launch(way, turn):
        if turn >= SENDS:
            launched(way, turn - SENDS).wait_send()
        launched(way, turn).start()

    def tok_copy(owner, b, i, dst):
        slot = tok.at[owner * per + b]
        return rdma(slot, slot, tok_send.at[0], tok_recv.at[i], me, dst)

    for k in range(QUARTERS):
        for way in range(2):
            launch(way, k)
    for copy in own_tok:
        copy.wait()
    for b in range(per):
        tok_copy(t, b, b, across).start()
    for b in range(per):
        tok_copy(t, b, per + b, mate).start()

    for copy in later:
        copy.wait()

    origin = [at(pos)]
    for d in range(1, half_n):
        origin += [at(pos - d), at(pos + d)]
    origin.append(at(pos + half_n))

    def project(i, first=False):
        o = origin[i]
        w = win[o].reshape(depth, qc + 2 * kc + cc)
        term = jnp.dot(tok[o], w, preferred_element_type=f32)
        if first:
            acc[...] = term
        else:
            acc[...] += term

    def relay(copy, k):
        for way in range(2):
            copy(way, k, 1).wait_recv()
            if copy is w_in:
                if k + QUARTERS <= last:
                    launch(way, k + QUARTERS)
            elif k + QUARTERS < last:
                launch(way, count + k + QUARTERS)
            elif k == last - 3:
                launch(way, count + last)

    def start_out(k):
        for way in range(2):
            launch(way, count + k)

    done_blocks = 0
    for k in range(count):
        relay(w_in, k)
        if last - 3 <= k < last:
            start_out(k - (last - 3))
        if k in (3, 6):
            b = 0 if k == 3 else 1
            tok_copy(across, b, b, across).wait_recv()
            tok_copy(across, b, 2 * per + b, mate).start()
        if k == 8:
            for b in range(per):
                tok_copy(mate, b, per + b, mate).wait_recv()
                tok_copy(lax.rem(mate + 2, tp), b, 2 * per + b, mate).wait_recv()
        if k >= 8:
            ready = n if k == last else 1 + 2 * ((k + 1) // QUARTERS)
            upto = ready if k == last else min(ready, done_blocks + 2)
            while done_blocks < upto:
                project(done_blocks, done_blocks == 0)
                done_blocks += 1

    kv[WINDOW : WINDOW + rows, :] = acc[:, qc : qc + 2 * kc].astype(bf16)
    chan[RIM : RIM + rows, :] = acc[:, qc + 2 * kc :].astype(bf16)

    def rim(buf, width, down, i):
        if down:
            return rdma(buf.at[pl.ds(rows, width)], buf.at[pl.ds(0, width)], rim_send.at[i], rim_recv.at[i], after, t)
        return rdma(
            buf.at[pl.ds(width, width)], buf.at[pl.ds(rows + width, width)], rim_send.at[i], rim_recv.at[i], before, t
        )

    rims = [rim(kv, WINDOW, True, 0), rim(kv, WINDOW, False, 1), rim(chan, RIM, True, 2), rim(chan, RIM, False, 3)]
    for c in rims:
        c.start()
    start_out(3)
    query[...] = acc[:, 0:qc].astype(bf16)

    group = qc // kc

    def attend(b):
        band = kv[b * WINDOW : (b + 3) * WINDOW, :]
        q = query[b * WINDOW : (b + 1) * WINDOW, :]
        stacked = jnp.concatenate([q[:, g * HEAD_DIM : (g + 1) * HEAD_DIM] for g in range(group)], axis=0)
        scores = lax.dot_general(
            stacked, band[:, :HEAD_DIM], (((1,), (1,)), ((), ())), preferred_element_type=f32
        ) * HEAD_DIM ** (-0.5)
        scores = scores.reshape(group, WINDOW, 3 * WINDOW)
        r = lax.broadcasted_iota(jnp.int32, (WINDOW, 3 * WINDOW), 0)
        c = lax.broadcasted_iota(jnp.int32, (WINDOW, 3 * WINDOW), 1)
        keep = (c >= r) & (c <= r + 2 * WINDOW)
        key_pos = c + (me * rows + b * WINDOW - WINDOW)
        keep = keep & (key_pos >= 0) & (key_pos < seq_len)
        outs = []
        for g in range(group):
            s = jnp.where(keep, scores[g], masked_score)
            logit = sinks[0:1, g : g + 1]
            top = jnp.maximum(jnp.max(s, axis=1, keepdims=True), logit)
            raised = jnp.exp(s - top)
            total = jnp.sum(raised, axis=1, keepdims=True) + jnp.exp(logit - top)
            outs.append((raised * (1.0 / total)).astype(bf16))
        got = jnp.dot(jnp.concatenate(outs, axis=0), band, preferred_element_type=f32)
        got = got[:, HEAD_DIM : 2 * HEAD_DIM].astype(bf16)
        hidden[place(b) : place(b) + WINDOW, 0:qc] = jnp.concatenate(
            [got[g * WINDOW : (g + 1) * WINDOW] for g in range(group)], axis=1
        )

    blocks = rows // WINDOW
    order = list(range(1, blocks - 1)) + [0, blocks - 1]
    early = (blocks - 2) * WINDOW

    def place(b):
        return order.index(b) * WINDOW

    half_width = 1
    for level in range(1, POOL_GROUPS):
        half_width = jnp.where(t == level, 2**level, half_width)

    def spread_of(start, size):
        length = size + 2 * RIM
        e = chan[start : start + length].astype(f32)
        p = lax.broadcasted_iota(jnp.int32, (length, 1), 0) + (me * rows + start - RIM)
        e = jnp.where((p >= 0) & (p < seq_len), e, 0.0)
        total = e + pltpu.roll(e, 1, 0)
        pick = total
        for level in range(1, POOL_GROUPS):
            step = 2 ** (level - 1)
            total = pltpu.roll(total, step, 0) + pltpu.roll(total, length - step, 0)
            pick = jnp.where(t == level, total, pick)
        number = (jnp.clip(p + half_width, 0, seq_len) - jnp.clip(p - half_width, 0, seq_len)).astype(f32)
        return (pick[RIM : RIM + size] / number[RIM : RIM + size] - e[RIM : RIM + size]).astype(bf16)

    def pooled_of(spread):
        return (jnp.dot(spread, wpool[0], preferred_element_type=f32) * scales[...]).astype(bf16)

    def pool_inner():
        got = pooled_of(spread_of(RIM, rows - 2 * RIM))
        for b in range(blocks):
            low, high = max(b * WINDOW, RIM), min((b + 1) * WINDOW, rows - RIM)
            base = place(b) - b * WINDOW
            hidden[base + low : base + high, qc:] = got[low - RIM : high - RIM]

    def pool_edges():
        got = pooled_of(jnp.concatenate([spread_of(0, RIM), spread_of(rows - RIM, RIM)], axis=0))
        hidden[place(0) : place(0) + RIM, qc:] = got[0:RIM]
        end = place(blocks - 1) + WINDOW
        hidden[end - RIM : end, qc:] = got[RIM:]

    near = 3
    spans = (pl.ds(0, early), pl.ds(early, rows - early))

    def unit(buf, o, u, split):
        return buf.at[o, :, spans[u]] if split else buf.at[o, u]

    def to_mate(o, u, split):
        i = (o // (2 * per)) * per + lax.rem(o, per)
        return rdma(
            unit(part, o, u, split), unit(mated, o, u, split), mate_send.at[0], mate_recv.at[i, u], me, mate
        )

    def to_owner(o, u, split):
        i = lax.rem(o, per)
        return rdma(
            unit(part, o, u, split), unit(landed, i, u, split), part_send.at[0], part_recv.at[i, u], me, across
        )

    final = origin[n - 1]
    holder = final // per

    def to_echo(h):
        return rdma(part.at[final, h], echo.at[h], echo_send.at[0], echo_recv.at[h], me, across)

    def to_late():
        return rdma(late, late, late_send.at[0], late_recv.at[0], me, mate)

    def to_far():
        return rdma(late, late, late_send.at[1], late_recv.at[0], me, lax.rem(mate + 2, tp))

    detour = holder == 0
    tells = jnp.logical_or(holder == across, jnp.logical_and(holder == t, jnp.logical_not(detour)))
    tells_far = jnp.logical_and(holder == across, detour)

    pieces = [(0, 0), (0, 1)]
    for k in range(1, count - 2, 2):
        d, h = k // QUARTERS, (k % QUARTERS) // 2
        pieces += [(2 * d + 1, h), (2 * d + 2, h)]
    pieces += [(n - 1, 0), (n - 1, 1)]

    def emit(places, span, split):
        side = jnp.concatenate([wout[origin[i], h].reshape(qc + cc, half) for i, h in places], axis=1)
        got = jnp.dot(hidden[span, :], side, preferred_element_type=f32).astype(bf16)
        for j, (i, h) in enumerate(places):
            part[origin[i], h, span] = got[:, j * half : (j + 1) * half]
        sent = [(i, spans.index(span)) for i, h in places if h == 0] if split else places
        for i, u in sent:
            o = origin[i]

            @pl.when(lax.rem(o // per, 2) != lax.rem(t, 2))
            def _(o=o, u=u):
                to_mate(o, u, split).start()

    def emit_near(u):
        emit([(i, h) for i in range(near) for h in range(2)], spans[u], True)

    def emit_far(ids):
        emit([pieces[i] for i in ids], pl.ds(0, rows), False)

    def combine(i, u, split):
        o = origin[i]
        where = (slice(None), spans[u]) if split else (u,)

        @pl.when(o // per == t)
        def _():
            to_mate(o, u, split).wait_recv()
            both = part[(o,) + where].astype(f32) + mated[(o,) + where].astype(f32)
            own[(lax.rem(o, per),) + where] = both
            if i == n - 1:
                part[(o,) + where] = both.astype(bf16)
                to_echo(u).start()

        @pl.when(o // per == across)
        def _():
            to_mate(o, u, split).wait_recv()
            both = part[(o,) + where].astype(f32) + mated[(o,) + where].astype(f32)
            part[(o,) + where] = both.astype(bf16)
            to_owner(o, u, split).start()

    def combine_near(u):
        for i in range(near):
            combine(i, u, True)

    def combine_far(ids):
        for i in ids:
            combine(pieces[i][0], pieces[i][1], False)

    def pack(one, two):
        one = jnp.sum(jnp.transpose(one), axis=0, keepdims=True)
        two = jnp.sum(jnp.transpose(two), axis=0, keepdims=True)
        return jnp.concatenate([one, two, jnp.zeros((6, rows), f32)], axis=0)

    sums[...] = jnp.zeros_like(sums)
    emits = {5: (6, 8), 7: (8, 10), 9: (10, 12), 11: (12, 14), 12: (14, 15), 13: (15, 16)}
    odd = lax.rem(t, 2) == 1
    ahead = {6: (6, 8), 7: (8, 10), 9: (10, 12), 11: (12, 14), 12: (14, 15), 13: (15, 16)}
    behind = {7: (6, 8), 8: (8, 10), 10: (10, 12), 13: (14, 16)}
    soon = lax.rem(holder, 2) == 1

    def on(core, work, *args):
        @pl.when(odd == core)
        def _():
            work(*args)

    for k in range(count):
        relay(w_out, k)
        if k < 2:
            for b in order[: blocks - 2][k::2]:
                attend(b)
        elif k == 2:
            pool_inner()
        elif k == 3:
            emit_near(0)
            for c in rims:
                c.wait()
            attend(0)
            on(False, combine_near, 0)
        elif k == 4:
            attend(blocks - 1)
            on(True, combine_near, 0)
            pool_edges()
            emit_near(1)
        if k in emits:
            emit_far(range(*emits[k]))
        if k == 5:
            on(False, combine_near, 1)
        elif k == 6:
            on(True, combine_near, 1)
        if k in ahead:
            on(False, combine_far, range(*ahead[k]))
        if k >= last - 1:

            @pl.when(jnp.logical_and(odd, soon == (k == last - 1)))
            def _():
                combine_far(range(12, 14))

        if k in behind:
            on(True, combine_far, range(*behind[k]))

    def stat_copy(j):
        return rdma(stats.at[t], stats.at[t], stat_send.at[0], stat_recv.at[t], me, lax.rem(t + j, tp))

    for i in range(n - 1):
        o = origin[i]

        @pl.when(o // per == t)
        def _(o=o, i=i):
            for u in range(2):
                to_owner(o, u, i < near).wait_recv()

    for i in range(per):
        o = t * per + i

        @pl.when(o != final)
        def _(o=o, i=i):
            one = two = 0.0
            for h in range(2):
                mix = own[i, h] + landed[i, h].astype(f32)
                acc[:, (2 * i + h) * half : (2 * i + h + 1) * half] = mix
                one, two = one + mix, two + mix * mix
            sums[0] += one
            sums[1] += two

    stats[t] = pack(sums[0], sums[1])
    for j in range(1, tp):
        stat_copy(j).start()

    @pl.when(holder == t)
    def _():
        one = two = 0.0
        for h in range(2):
            i = lax.rem(final, per)
            to_owner(final, h, False).wait_recv()
            mix = own[i, h] + landed[i, h].astype(f32)
            acc[:, pl.ds(pl.multiple_of((2 * i + h) * half, 128), half)] = mix
            one, two = one + mix, two + mix * mix
        late[...] = pack(one, two)

        @pl.when(tells)
        def _():
            to_late().start()

    @pl.when(holder == across)
    def _():
        one = two = 0.0
        for h in range(2):
            to_echo(h).wait_recv()
            mix = part[final, h].astype(f32) + echo[h].astype(f32)
            one, two = one + mix, two + mix * mix
        late[...] = pack(one, two)

        @pl.when(tells_far)
        def _():
            to_far().start()

        to_late().start()

    def drain(buf, amount, sem):
        whole = buf.at[pl.ds(0, amount)]
        rdma(whole, whole, sem.at[0], mate_recv.at[0, 0], me, mate).wait_send()

    for j in range(1, tp):
        src = lax.rem(t + j, tp)
        rdma(stats.at[src], stats.at[src], stat_send.at[0], stat_recv.at[src], me, src).wait_recv()
    paired = lax.rem(holder, 2) == lax.rem(t, 2)

    @pl.when(jnp.logical_not(paired))
    def _():
        to_late().wait_recv()

    totals = late[...] + stats[0]
    for i in range(1, tp):
        totals = totals + stats[i]
    width = gain_ref.shape[1] * tp
    line_mean = totals[0:1] / width
    line_scale = lax.rsqrt(totals[1:2] / width - line_mean * line_mean + epsilon)
    tall = jnp.concatenate([line_mean, line_scale, jnp.zeros((6, rows), f32)], axis=0)
    back = jnp.transpose(tall)
    row_mean, scale = back[:, 0:1], back[:, 1:2]
    normed = ((acc[:, 0 : gain_ref.shape[1]] - row_mean) * scale * gains[...]).astype(bf16)
    for b in range(blocks):
        out_ref[b * WINDOW : (b + 1) * WINDOW, :] = normed[place(b) : place(b) + WINDOW]
    drain(part, n // 2, mate_send)
    drain(part, per, part_send)
    drain(tok, 3 * per, tok_send)

    @pl.when(holder == t)
    def _():
        drain(part, 1, echo_send)

    for turn in range(2 * count - SENDS, 2 * count):
        for way in range(2):
            launched(way, turn).wait_send()
    drain(stats, tp - 1, stat_send)

    @pl.when(tells)
    def _():
        to_late().wait_send()

    @pl.when(tells_far)
    def _():
        to_far().wait_send()


def fused(n, tp, tokens, w_query, w_key, w_value, w_pool_in, sink, w_pool, pool_scale, w_out_attn, w_out_pool, out_gain):
    rows, share = tokens.shape
    depth, qc = w_query.shape
    kc, cc = w_key.shape[1], w_pool_in.shape[1]
    wide = w_out_attn.shape[1]
    half = wide // 2
    per = n // tp
    count = QUARTERS * (n - 1) // 2
    bf16, f32 = jnp.bfloat16, jnp.float32
    dma = pltpu.SemaphoreType.DMA
    return pl.pallas_call(
        functools.partial(mixer_kernel, n, tp),
        out_shape=jax.ShapeDtypeStruct((rows, share), bf16),
        in_specs=[pl.BlockSpec(memory_space=pltpu.HBM)] * 11,
        out_specs=pl.BlockSpec(memory_space=pltpu.VMEM),
        scratch_shapes=[
            pltpu.VMEM((n, QUARTERS, depth // QUARTERS, qc + 2 * kc + cc), bf16),
            pltpu.VMEM((n, 2, 2, qc, half), bf16),
            pltpu.VMEM((n, rows, depth), bf16),
            pltpu.VMEM((rows, qc + 2 * kc + cc), f32),
            pltpu.VMEM((rows, qc), bf16),
            pltpu.VMEM((rows + 2 * WINDOW, 2 * kc), bf16),
            pltpu.VMEM((rows + 2 * RIM, cc), bf16),
            pltpu.VMEM((rows, qc + cc), bf16),
            pltpu.VMEM((n, 2, rows, half), bf16),
            pltpu.VMEM((n, 2, rows, half), bf16),
            pltpu.VMEM((per, 2, rows, half), bf16),
            pltpu.VMEM((per, 2, rows, half), f32),
            pltpu.VMEM((tp, 8, rows), f32),
            pltpu.VMEM((8, rows), f32),
            pltpu.VMEM((2, rows, half), bf16),
            pltpu.VMEM((2, rows, half), f32),
            pltpu.VMEM((2 * kc, depth), bf16),
            pltpu.VMEM((1, sink.shape[0]), f32),
            pltpu.VMEM(w_pool.shape, bf16),
            pltpu.VMEM((1, cc), f32),
            pltpu.VMEM((1, share), f32),
            dma((2, SENDS)),
            dma((2, RECVS)),
            dma((1,)),
            dma((3 * per,)),
            dma((4,)),
            dma((4,)),
            dma((1,)),
            dma((n // 2, 2)),
            dma((1,)),
            dma((per, 2)),
            dma((1,)),
            dma((2,)),
            dma((9,)),
            dma((1,)),
            dma((tp,)),
            dma((2,)),
            dma((1,)),
        ],
        compiler_params=pltpu.CompilerParams(
            collective_id=0, has_side_effects=True, vmem_limit_bytes=32 * 1024 * 1024
        ),
        name="mixer",
    )(
        pltpu.with_memory_space_constraint(tokens, pltpu.HBM),
        pltpu.with_memory_space_constraint(w_query.reshape(QUARTERS, -1, qc), pltpu.HBM),
        pltpu.with_memory_space_constraint(w_key.T, pltpu.HBM),
        pltpu.with_memory_space_constraint(w_value.T, pltpu.HBM),
        pltpu.with_memory_space_constraint(w_pool_in.reshape(QUARTERS, -1, cc), pltpu.HBM),
        pltpu.with_memory_space_constraint(sink.reshape(1, -1), pltpu.HBM),
        pltpu.with_memory_space_constraint(w_pool, pltpu.HBM),
        pltpu.with_memory_space_constraint(pool_scale.reshape(1, -1), pltpu.HBM),
        pltpu.with_memory_space_constraint(w_out_attn, pltpu.HBM),
        pltpu.with_memory_space_constraint(w_out_pool, pltpu.HBM),
        pltpu.with_memory_space_constraint(out_gain.reshape(1, -1), pltpu.HBM),
    )


def fits(n, tp, tokens, w_query, w_key, w_pool, w_out_attn):
    return (
        tp == 4
        and n == 2 * tp
        and w_query.shape[0] % 64 == 0
        and w_query.shape[1] % 128 == 0
        and w_key.shape[1] == HEAD_DIM
        and w_pool.shape[0] == 1
        and w_out_attn.shape[1] % 256 == 0
        and w_out_attn.shape[0] == w_query.shape[1]
        and tokens.shape[0] >= 3 * WINDOW
    )


def mixed_rows(*args):
    n, tp = lax.axis_size("sp"), lax.axis_size("tp")
    if fits(n, tp, args[0], args[1], args[2], args[6], args[8]):
        return fused(n, tp, *args)
    return local(*args)


def solution(mesh):
    return jax.shard_map(
        mixed_rows,
        mesh=mesh,
        in_specs=(
            P("sp", "tp"),
            P("sp", "tp"),
            P("sp", "tp"),
            P("sp", "tp"),
            P("sp", "tp"),
            P("tp"),
            P("tp", None, None),
            P("tp"),
            P("tp", "sp"),
            P("tp", "sp"),
            P("tp"),
        ),
        out_specs=P("sp", "tp"),
        check_vma=False,
    )
```
